512 devices in a mesh: grp: 2 (over y), kv: 32 (over z), tp: 8 (over x, core).
Axes of the slice: x: 4, y: 2, z: 32, core: 2. Of those that a mesh axis runs over, the one named last changes fastest.
The devices are a block of a 4x8x32 slice.
Arguments:
- tokens: bfloat16 [256, 2048], P('grp', ('kv', 'tp')), parts along dimension 0, may hold values from -13 to 13, as said below
- state: float32 [256, 16, 128, 128], P(('grp', 'kv'), 'tp'), parts along dimension 0, may hold values from -0.6 to 0.6
- norm_gain: bfloat16 [2048], P('kv'), may hold values from 0.099609375 to 1.8984375
- w_query: bfloat16 [2048, 2048], P('kv', 'tp'), may hold values from -0.125 to 0.125
- w_key: bfloat16 [2048, 2048], P('kv', 'tp'), may hold values from -0.125 to 0.125
- w_value: bfloat16 [2048, 2048], P('kv', 'tp'), may hold values from -0.125 to 0.125
- w_beta: bfloat16 [2048, 16], replicated, may hold values from -0.125 to 0.125
- w_decay: bfloat16 [2048, 16], replicated, may hold values from -0.125 to 0.125
- a_log: float32 [16], P('tp'), may hold values from -3 to 1
- dt_bias: float32 [16], P('tp'), may hold values from -2 to 1
- head_gain: float32 [128], replicated, may hold values from 0.1 to 1.9
- w_out: bfloat16 [2048, 2048], P('tp', 'kv'), may hold values from -0.125 to 0.125
- mixer_gain: bfloat16 [2048], P('kv'), may hold values from 0.099609375 to 1.8984375
- w_up: bfloat16 [2048, 8192], P('kv', 'tp'), may hold values from -0.125 to 0.125
- w_down: bfloat16 [8192, 2048], P('tp', 'kv'), may hold values from -0.0625 to 0.0625
Outputs:
- mixed: bfloat16 [256, 2048], P('grp', ('kv', 'tp')), parts along dimension 0
- new_state: float32 [256, 16, 128, 128], P(('grp', 'kv'), 'tp'), parts along dimension 0
The draws below stay inside these ranges and needn't reach their ends.
There are 2 independent parts, one for each index of `grp`. The reference program is written for one: setup_inputs(seed, part) draws one part's arguments, and reference() takes and returns one part's arrays. A program takes and returns all parts, laid end to end along the dimension named above; an argument that names none is the same for every part. Nothing has to cross between parts.
Inputs may be any that keep to these rules, and one draw needn't show every extreme that they name: `tokens`: activations of order one.
All inputs are finite; a program needn't handle non-finite values.
Results may differ from the reference program's by a relative error of at most 0.019.
Values may be sent and summed in bfloat16 or wider, within the bound.
A program may use at most 64 MiB of HBM per device.

```python
import jax
import jax.numpy as jnp
from jax import lax

D = 2048
HEADS = 16
HEAD = 128
FF = 8192
BATCH = 128
N_TP = 8


def draw_tokens(key, part):
    first_key, second_key = jax.random.split(jax.random.fold_in(key, 17), 2)
    ramp = jnp.exp(jnp.linspace(jnp.log(0.5), jnp.log(1.5), D)).astype(jnp.float32)
    rough = jnp.exp(jax.random.uniform(second_key, (1, D), jnp.float32, -0.35, 0.35))
    base = jnp.clip(jax.random.normal(first_key, (BATCH, D), jnp.float32), -6.0, 6.0)
    return (base * ramp * rough).astype(jnp.bfloat16)


def steps_of(rng, extent, shards, low, top_value):
    def one(dim, blocks):
        heights = jax.random.uniform(jax.random.fold_in(jax.random.fold_in(rng, 6), dim), (blocks,), jnp.float32, low / len(shards), top_value / len(shards))
        return jnp.repeat(jnp.exp(heights), extent[dim] // blocks).reshape((-1,) + (1,) * (len(extent) - dim - 1))

    loudness = one(*shards[0])
    for cut in shards[1:]:
        loudness = loudness * one(*cut)
    return loudness


def scatter_about(key, shape, spread, limit, cuts=(), held_as=jnp.bfloat16):
    array = spread * jax.random.normal(key, shape, jnp.float32)
    if cuts:
        array = array * steps_of(key, shape, cuts, -0.22, 0.18)
    return jnp.clip(array, -limit, limit).astype(held_as)


def setup_inputs(seed: int = 0, part: int = 0) -> dict:
    splits = jax.random.split(jax.random.key(seed), 16)
    own_keys = jax.random.split(jax.random.fold_in(splits[15], part), 16)
    tokens = draw_tokens(jax.random.fold_in(jax.random.fold_in(splits[15], part), 71), part)
    state = scatter_about(own_keys[1], (BATCH, HEADS, HEAD, HEAD), 0.1, 0.6, ((0, 32), (1, 8)), jnp.float32)
    norm_gain = jnp.clip(1.0 + 0.18 * jax.random.normal(splits[2], (D,), jnp.float32), 0.099609375, 1.8984375).astype(jnp.bfloat16)
    w_query = scatter_about(splits[3], (D, HEADS * HEAD), D ** -0.5, 0.125, ((0, 32), (1, 8)))
    w_key = scatter_about(splits[4], (D, HEADS * HEAD), D ** -0.5, 0.125, ((0, 32), (1, 8)))
    w_value = scatter_about(splits[5], (D, HEADS * HEAD), D ** -0.5, 0.125, ((0, 32), (1, 8)))
    w_beta = scatter_about(splits[6], (D, HEADS), D ** -0.5, 0.125)
    w_decay = scatter_about(splits[7], (D, HEADS), D ** -0.5, 0.125)
    a_log = jnp.clip(-3.0 + 4.0 * jax.random.uniform(splits[8], (HEADS,), jnp.float32) ** steps_of(splits[8], (HEADS,), ((0, 8),), -0.2, 0.2), -3.0, 1.0)
    dt_bias = jnp.clip(-2.0 + 3.0 * jax.random.uniform(splits[9], (HEADS,), jnp.float32) ** steps_of(splits[9], (HEADS,), ((0, 8),), -0.2, 0.2), -2.0, 1.0)
    head_gain = jnp.clip(1.0 + 0.18 * jax.random.normal(splits[10], (HEAD,), jnp.float32), 0.1, 1.9)
    w_out = scatter_about(splits[11], (HEADS * HEAD, D), (HEADS * HEAD) ** -0.5, 0.125, ((0, 8), (1, 32)))
    mixer_gain = jnp.clip(1.0 + 0.18 * jax.random.normal(splits[12], (D,), jnp.float32), 0.099609375, 1.8984375).astype(jnp.bfloat16)
    w_up = scatter_about(splits[13], (D, FF), D ** -0.5, 0.125, ((0, 32), (1, 8)))
    w_down = scatter_about(splits[14], (FF, D), FF ** -0.5, 0.0625, ((0, 8), (1, 32)))
    return {"tokens": tokens, "state": state, "norm_gain": norm_gain, "w_query": w_query, "w_key": w_key, "w_value": w_value, "w_beta": w_beta, "w_decay": w_decay, "a_log": a_log, "dt_bias": dt_bias, "head_gain": head_gain, "w_out": w_out, "mixer_gain": mixer_gain, "w_up": w_up, "w_down": w_down}


epsilon = 1e-06

def dotted(left, right):
    return jnp.dot(left, right, preferred_element_type=jnp.float32)

def delta_update(query_pre, key_pre, value_pre, beta_pre, decay_pre, state, a_log, dt_bias, head_gain):
    query = query_pre * lax.rsqrt(lax.optimization_barrier(jnp.sum(query_pre * query_pre, axis=-1, keepdims=True)) + epsilon)
    keyed = key_pre * lax.rsqrt(lax.optimization_barrier(jnp.sum(key_pre * key_pre, axis=-1, keepdims=True)) + epsilon)
    beta = jax.nn.sigmoid(beta_pre)
    decay = jnp.exp(-jnp.exp(a_log) * jax.nn.softplus(decay_pre + dt_bias))
    key_read = jnp.einsum('bhk,bhkv->bhv', keyed, state)
    query_read = jnp.einsum('bhk,bhkv->bhv', query, state)
    fresh = beta[..., None] * (value_pre - decay[..., None] * key_read)
    new_state = decay[..., None, None] * state + keyed[..., :, None] * fresh[..., None, :]
    intersection = lax.optimization_barrier(jnp.sum(query * keyed, axis=-1))
    reading = decay[..., None] * query_read + intersection[..., None] * fresh
    normed = reading * lax.rsqrt(lax.optimization_barrier(jnp.mean(reading * reading, axis=-1, keepdims=True)) + epsilon) * head_gain
    return (normed.astype(jnp.bfloat16), new_state)

def grouped_sum(left, weight, groups):
    rows = left.shape[0]
    width = left.shape[1] // groups
    left_g = left.reshape(rows, groups, width).astype(jnp.float32)
    weight_g = weight.reshape(groups, width, weight.shape[1]).astype(jnp.float32)
    partial_g = jnp.einsum('bgi,gio->bgo', left_g, weight_g)
    return lax.optimization_barrier(jnp.sum(partial_g.astype(jnp.bfloat16).astype(jnp.float32), axis=1))

def reference(tokens, state, norm_gain, w_query, w_key, w_value, w_beta, w_decay, a_log, dt_bias, head_gain, w_out, mixer_gain, w_up, w_down):
    rows = tokens.shape[0]
    inputs = tokens.astype(jnp.float32)
    first = lax.rsqrt(lax.optimization_barrier(jnp.mean(inputs * inputs, axis=-1, keepdims=True)) + epsilon)
    scaled = (inputs * norm_gain.astype(jnp.float32)).astype(jnp.bfloat16)
    query_pre = (first * dotted(scaled, w_query)).reshape(rows, HEADS, HEAD)
    key_pre = (first * dotted(scaled, w_key)).reshape(rows, HEADS, HEAD)
    value_pre = (first * dotted(scaled, w_value)).reshape(rows, HEADS, HEAD)
    beta_pre = first * dotted(scaled, w_beta)
    decay_pre = first * dotted(scaled, w_decay)
    normed, new_state = delta_update(query_pre, key_pre, value_pre, beta_pre, decay_pre, state, a_log, dt_bias, head_gain)
    attended = grouped_sum(normed.reshape(rows, HEADS * HEAD), w_out, N_TP)
    middle = (inputs + attended).astype(jnp.bfloat16)
    middle_f = middle.astype(jnp.float32)
    second = lax.rsqrt(lax.optimization_barrier(jnp.mean(middle_f * middle_f, axis=-1, keepdims=True)) + epsilon)
    scaled_two = (middle_f * mixer_gain.astype(jnp.float32)).astype(jnp.bfloat16)
    hidden = jnp.square(jax.nn.relu(second * dotted(scaled_two, w_up))).astype(jnp.bfloat16)
    lowered = grouped_sum(hidden, w_down, N_TP)
    mixed = (middle_f + lowered).astype(jnp.bfloat16)
    return (mixed, new_state)
```

```python
import functools

import jax
import jax.numpy as jnp
from jax import lax
from jax.experimental import pallas as pl
from jax.experimental.pallas import tpu as pltpu
from jax.sharding import PartitionSpec as P

MESH = pl.DeviceIdType.MESH
epsilon = 1e-06
f32 = jnp.float32
bf16 = jnp.bfloat16


def nn(a, b):
    return jnp.dot(a, b, preferred_element_type=f32)


def nt(a, b):
    return lax.dot_general(a, b, (((1,), (1,)), ((), ())), preferred_element_type=f32)


def exact_nn(a, onehot):
    high = a.astype(bf16)
    low = (a - high.astype(f32)).astype(bf16)
    return nn(high, onehot) + nn(low, onehot)


def lanes_of(x, lane):
    at = lax.broadcasted_iota(jnp.int32, x.shape, 1)
    return jnp.sum(jnp.where(at == lane, x, 0.0), axis=1, keepdims=True)


def column_of(row):
    n = row.shape[1]
    eye = lax.broadcasted_iota(jnp.int32, (n, n), 0) == lax.broadcasted_iota(
        jnp.int32, (n, n), 1
    )
    return jnp.sum(jnp.where(eye, row, 0.0), axis=1, keepdims=True)


class Exchange:
    def __init__(self, n_kv, g, z, t):
        self.n_kv, self.g, self.z, self.t = n_kv, g, z, t
        self.half = n_kv // 8
        up = [2 + 4 * i for i in range(self.half)]
        self.reach = up + [-u for u in up]
        self.count = 2 * self.half
        self.steps = [(0, 1), (1, -1)]
        self.farthest_first = [
            k * self.half + i for i in reversed(range(self.half)) for k in (0, 1)
        ]
        self.nearest_first = list(reversed(self.farthest_first))

    def device(self, offset):
        return (self.g, lax.rem(self.z + offset + self.n_kv, self.n_kv), self.t)

    def near(self, i):
        last = () if i == self.count - 1 else ((3, 2 if i < self.half else -2),)
        return self.steps + list(last)

    def copy(self, src, dst, send, recv, offset):
        return pltpu.make_async_remote_copy(
            src_ref=src,
            dst_ref=dst,
            send_sem=send,
            recv_sem=recv,
            device_id=self.device(offset),
            device_id_type=MESH,
        )


def placing(per_slot, n_kv, seq, z):
    count = n_kv // 4
    half = count // 2
    shape = (n_kv * per_slot, n_kv * seq)
    m = lax.broadcasted_iota(jnp.int32, shape, 0)
    slot = m // per_slot
    i = slot % count
    group = slot // count
    reach = jnp.where(i < half, 2 + 4 * i, 4 * half - 2 - 4 * i)
    side = jnp.where(i < half, 2, -2)
    step = jnp.where(group == 0, 1, jnp.where(group == 1, -1, jnp.where(group == 2, 0, side)))
    offset = jnp.where(slot == n_kv - 1, 0, reach + step)
    owner = (z - offset + n_kv) % n_kv
    row = owner * seq + m % seq
    return (row == lax.broadcasted_iota(jnp.int32, shape, 1)).astype(bf16)


def kernel(
    dims,
    tok_ref,
    state_hbm,
    gain_ref,
    wq_hbm,
    wk_hbm,
    wv_hbm,
    wb_hbm,
    wd_hbm,
    alog_ref,
    dt_ref,
    hgain_ref,
    wo_hbm,
    mgain_ref,
    wu_hbm,
    wdn_hbm,
    out_ref,
    state_out,
    tok_all,
    state_v,
    rhs1,
    wext,
    wo_v,
    wu_v,
    wdn_v,
    rs1,
    rs1_near,
    rs1_far_src,
    rs1_far,
    ag2,
    att,
    mid,
    rs3,
    rs3_near,
    rs3_far_src,
    rs3_far,
    sq_src,
    sq_near,
    sq_far_src,
    sq_far,
    ag4,
    low_src,
    low,
    loc,
    tok_s,
    tok_r,
    rs1_ns,
    rs1_nr,
    rs1_fs,
    rs1_fr,
    ag2_ns,
    ag2_nr,
    ag2_fs,
    ag2_fr,
    att_s,
    att_r,
    rs3_ns,
    rs3_nr,
    rs3_fs,
    rs3_fr,
    sq_ns,
    sq_nr,
    sq_fs,
    sq_fr,
    ag4_ns,
    ag4_nr,
    ag4_fs,
    ag4_fr,
    low_s,
    low_r,
    sem_a,
    sem_b,
    sem_c,
):
    n_kv, n_tp, seq, heads, width = dims
    g, z, t = lax.axis_index("grp"), lax.axis_index("kv"), lax.axis_index("tp")
    ex = Exchange(n_kv, g, z, t)
    count, half = ex.count, ex.half
    block = tok_all.shape[0] * tok_all.shape[1]
    mine = tok_all.shape[1]
    head = hgain_ref.shape[1]
    own = n_kv - 1

    def tp_peer(k):
        return (g, z, lax.rem(t + k, n_tp))

    barrier = pltpu.get_barrier_semaphore()
    for k in range(1, n_tp):
        pl.semaphore_signal(barrier, inc=1, device_id=tp_peer(k), device_id_type=MESH)
    for offset in (1, -1, 2, -2):
        pl.semaphore_signal(barrier, inc=1, device_id=ex.device(offset), device_id_type=MESH)

    local = []

    def fetch(src, dst):
        copy = pltpu.make_async_copy(src, dst, loc.at[len(local)])
        copy.start()
        local.append(copy)

    for i, w in enumerate((wq_hbm, wk_hbm)):
        for h in range(heads):
            at = (i * heads + h) * block
            fetch(w.at[:, h * head : (h + 1) * head], rhs1.at[at : at + block, 0:head])
    for h in range(heads):
        fetch(
            wv_hbm.at[:, h * head : (h + 1) * head],
            rhs1.at[h * block : (h + 1) * block, head : 2 * head],
        )
    lanes = wext.shape[2]
    at = pl.multiple_of((z * block // lanes) * lanes, lanes)
    fetch(wb_hbm.at[:, pl.ds(at, lanes)], wext.at[0])
    fetch(wd_hbm.at[:, pl.ds(at, lanes)], wext.at[1])
    first_fetch = len(local)
    fetch(state_hbm, state_v)
    second_fetch = len(local)
    for h in range(heads):
        fetch(wo_hbm.at[:, h * head : (h + 1) * head], wo_v.at[h * block : (h + 1) * block])
    third_fetch = len(local)
    parts = wu_v.shape[0] // block
    wide = wu_v.shape[1]
    for j in range(parts):
        fetch(wu_hbm.at[:, j * wide : (j + 1) * wide], wu_v.at[j * block : (j + 1) * block])
    for j in range(parts):
        fetch(wdn_hbm.at[:, j * wide : (j + 1) * wide], wdn_v.at[j * block : (j + 1) * block])
    all_fetch = len(local)

    tok_all[t] = tok_ref[...].astype(f32)
    rhs1[heads * block :, head:] = jnp.zeros((heads * block, head), bf16)
    spread16 = placing(parts * seq, n_kv, seq, z)
    part_of_row = (
        lax.broadcasted_iota(jnp.int32, (n_kv * parts * seq, parts * block), 0) // seq
    ) % parts
    part_mask = part_of_row == (
        lax.broadcasted_iota(jnp.int32, (n_kv * parts * seq, parts * block), 1) // block
    )
    gain = column_of(gain_ref[...])
    mixer_gain = column_of(mgain_ref[...])

    pl.semaphore_wait(barrier, n_tp - 1 + 4)
    for offset in (2, -2):
        pl.semaphore_signal(sem_a, inc=1, device_id=ex.device(offset), device_id_type=MESH)

    def to_tp(src_of, dst, send, recv):
        copies = []
        for k in range(1, n_tp):
            peer = lax.rem(t + k, n_tp)
            copy = pltpu.make_async_remote_copy(
                src_ref=src_of(peer),
                dst_ref=dst.at[t],
                send_sem=send.at[k - 1],
                recv_sem=recv.at[k - 1],
                device_id=(g, z, peer),
                device_id_type=MESH,
            )
            copy.start()
            copies.append(copy)
        return copies

    pending = []
    copies = to_tp(lambda peer: tok_all.at[t], tok_all, tok_s, tok_r)
    pending += copies
    for k in range(first_fetch):
        local[k].wait()
    odd = lax.rem(z, lanes // block) if lanes // block > 1 else 0
    pieces = []
    for i in range(2):
        piece = wext[i][:, 0:block]
        for k in range(1, lanes // block):
            piece = jnp.where(odd == k, wext[i][:, k * block : (k + 1) * block], piece)
        pieces.append(piece)
    n_heads = pieces[0].shape[0]
    wext_t = jnp.concatenate(
        pieces + [jnp.zeros((head - 2 * n_heads, block), bf16)], axis=0
    )
    at_row = lax.broadcasted_iota(jnp.int32, (head, block), 0)
    square_t = (at_row == 2 * n_heads).astype(bf16)
    ext_t = jnp.concatenate([wext_t, square_t], axis=1)

    pl.semaphore_wait(sem_a, 2)
    for offset in (4, -4):
        pl.semaphore_signal(sem_b, inc=1, device_id=ex.device(offset), device_id_type=MESH)
    for copy in copies:
        copy.wait_recv()

    def spread(x_t):
        stacked = jnp.concatenate([x_t] * parts, axis=0)
        rows = nt(spread16, stacked)
        return jnp.where(part_mask, rows, 0.0).astype(bf16)

    tok_t = tok_all[...].reshape(block, tok_all.shape[2])
    scaled_t = (tok_t * gain).astype(bf16)
    left = spread(scaled_t)
    both = jnp.concatenate([scaled_t, (tok_t * tok_t).astype(bf16)], axis=0)
    left2 = nt(spread16, both)
    left2 = jnp.where(part_of_row[:, 0 : 2 * block] >= heads, left2, 0.0).astype(bf16)
    product = nn(left, rhs1[...])
    extra = nt(left2, ext_t)
    product = jnp.concatenate([product[:, :head], product[:, head:] + extra], axis=1)
    rs1[...] = product.astype(bf16).reshape(rs1.shape)

    def reduce_near(buf, near_buf, send, recv, order):
        started = {}
        for i in order:
            for group, step in ex.near(i):
                k = group * count + i if group < 2 else 2 * count + i
                copy = ex.copy(
                    buf.at[group * count + i],
                    near_buf.at[k],
                    send.at[k],
                    recv.at[k],
                    -step,
                )
                copy.start()
                started[k] = copy
        return started

    def near_sum(i, buf, near_buf, started):
        total = buf[2 * count + i].astype(f32)
        for group, step in ex.near(i):
            k = group * count + i if group < 2 else 2 * count + i
            started[k].wait_recv()
            total += near_buf[k].astype(f32)
        return total

    def reduce_far(i, total, far_src, far_buf, send, recv):
        far_src[i] = total.astype(far_src.dtype)
        copy = ex.copy(far_src.at[i], far_buf.at[i], send.at[i], recv.at[i], -ex.reach[i])
        copy.start()
        return copy

    def far_sum(buf, far_buf, copies):
        total = buf[own].astype(f32)
        for i, copy in copies:
            copy.wait_recv()
            total += far_buf[i].astype(f32)
        return total

    close = [i for i in ex.nearest_first if abs(ex.reach[i]) <= 8]
    distant = [i for i in ex.farthest_first if abs(ex.reach[i]) > 8]
    started = reduce_near(rs1, rs1_near, rs1_ns, rs1_nr, distant + close)
    pending += list(started.values())
    pl.semaphore_wait(sem_b, 2)
    for offset in (8, -8):
        pl.semaphore_signal(sem_c, inc=1, device_id=ex.device(offset), device_id_type=MESH)
    copies = []
    for i in close:
        total = near_sum(i, rs1, rs1_near, started)
        copies.append((i, reduce_far(i, total, rs1_far_src, rs1_far, rs1_fs, rs1_fr)))
    totals = [near_sum(i, rs1, rs1_near, started) for i in distant]
    pl.semaphore_wait(sem_c, 2)
    for i, total in zip(distant, totals):
        copies.append((i, reduce_far(i, total, rs1_far_src, rs1_far, rs1_fs, rs1_fr)))
    pending += [c for _, c in copies]

    local[first_fetch].wait()
    for k in range(second_fetch, third_fetch):
        local[k].wait()
    sums = far_sum(rs1, rs1_far, copies)

    rows = heads * seq
    query_sum, key_sum = sums[:rows, :head], sums[rows:, :head]
    value_sum, extra = sums[:rows, head:], sums[rows:, head:]
    which = lax.broadcasted_iota(jnp.int32, (rows, head), 0) // seq
    lane = lax.broadcasted_iota(jnp.int32, (rows, head), 1)
    beta_sum = jnp.sum(
        jnp.where(lane == t * heads + which, extra, 0.0), axis=1, keepdims=True
    )
    decay_sum = jnp.sum(
        jnp.where(lane == n_heads + t * heads + which, extra, 0.0), axis=1, keepdims=True
    )
    square_sum = lanes_of(extra, 2 * n_heads)
    first = lax.rsqrt(square_sum / width + epsilon)
    query_pre, key_pre, value_pre = first * query_sum, first * key_sum, first * value_sum
    query = query_pre * lax.rsqrt(jnp.sum(query_pre * query_pre, axis=1, keepdims=True) + epsilon)
    key = key_pre * lax.rsqrt(jnp.sum(key_pre * key_pre, axis=1, keepdims=True) + epsilon)
    beta = jax.nn.sigmoid(first * beta_sum)
    which1 = lax.broadcasted_iota(jnp.int32, (rows, 1), 0) // seq
    a_log = jnp.zeros((rows, 1), f32)
    dt_bias = jnp.zeros((rows, 1), f32)
    for h in range(heads):
        a_log = jnp.where(which1 == h, alog_ref[h], a_log)
        dt_bias = jnp.where(which1 == h, dt_ref[h], dt_bias)
    logit = first * decay_sum + dt_bias
    softplus = jnp.maximum(logit, 0.0) + jnp.log1p(jnp.exp(-jnp.abs(logit)))
    decay = jnp.exp(-jnp.exp(a_log) * softplus)
    query_t, key_t = query.T, key.T
    key_reads, query_reads = [], []
    for k in range(rows):
        matrix = state_v[k % seq, k // seq]
        key_reads.append(jnp.sum(matrix * key_t[:, k : k + 1], axis=0, keepdims=True))
        query_reads.append(jnp.sum(matrix * query_t[:, k : k + 1], axis=0, keepdims=True))
    key_read = jnp.concatenate(key_reads, axis=0)
    query_read = jnp.concatenate(query_reads, axis=0)
    fresh = beta * (value_pre - decay * key_read)
    meeting = jnp.sum(query * key, axis=1, keepdims=True)
    reading = decay * query_read + meeting * fresh
    normed = (
        reading
        * lax.rsqrt(jnp.mean(reading * reading, axis=1, keepdims=True) + epsilon)
        * hgain_ref[...]
    )

    def gather_far(buf, send, recv):
        copies = {}
        for i in ex.farthest_first:
            copy = ex.copy(
                buf.at[own], buf.at[2 * count + i], send.at[i], recv.at[i], ex.reach[i]
            )
            copy.start()
            copies[i] = copy
        return copies

    def gather_near(buf, copies, send, recv):
        started = []
        for i in ex.nearest_first:
            copies[i].wait_recv()
            for group, step in ex.near(i):
                k = group * count + i if group < 2 else 2 * count + i
                copy = ex.copy(
                    buf.at[2 * count + i],
                    buf.at[group * count + i],
                    send.at[k],
                    recv.at[k],
                    step,
                )
                copy.start()
                started.append(copy)
        return started

    ag2[own] = normed.astype(bf16).astype(f32)
    copies = gather_far(ag2, ag2_fs, ag2_fr)
    pending += list(copies.values())
    for k in range(rows):
        matrix = state_v[k % seq, k // seq]
        state_v[k % seq, k // seq] = (
            decay[k : k + 1] * matrix + key_t[:, k : k + 1] * fresh[k : k + 1]
        )
    store = pltpu.make_async_copy(state_v, state_out, loc.at[all_fetch])
    store.start()
    spread8 = placing(heads * seq, n_kv, seq, z)
    head_of_column = (
        lax.broadcasted_iota(jnp.int32, (block, n_kv * rows), 1) // seq
    ) % heads
    started = gather_near(ag2, copies, ag2_ns, ag2_nr)
    pending += started
    for copy in started:
        copy.wait_recv()
    everyone = ag2[...].reshape(n_kv * rows, head).astype(bf16)
    by_head = nt(wo_v[...], everyone)
    chosen = by_head[0:block]
    for h in range(1, heads):
        chosen = jnp.where(head_of_column == h, by_head[h * block : (h + 1) * block], chosen)
    att[t] = exact_nn(chosen, spread8).astype(bf16)
    copies = to_tp(lambda peer: att.at[t], att, att_s, att_r)
    pending += copies
    for k in range(third_fetch, all_fetch):
        local[k].wait()
    for copy in copies:
        copy.wait_recv()
    attended = att[0].astype(f32)
    for k in range(1, n_tp):
        attended += att[k].astype(f32)
    middle = (tok_t + attended).astype(bf16).astype(f32)
    mid[...] = middle.reshape(mid.shape)

    scaled_t = (middle * mixer_gain).astype(bf16)
    left = spread(scaled_t)
    rs3[...] = nn(left, wu_v[...]).astype(bf16).reshape(rs3.shape)
    started = reduce_near(rs3, rs3_near, rs3_ns, rs3_nr, ex.farthest_first)
    pending += list(started.values())
    square_part = jnp.sum(middle * middle, axis=0, keepdims=True)
    sq_src[...] = square_part
    sq_started = []
    for k, step in enumerate((1, -1, 2, -2)):
        copy = ex.copy(sq_src, sq_near.at[k], sq_ns.at[k], sq_nr.at[k], -step)
        copy.start()
        sq_started.append(copy)
    pending += sq_started
    copies = []
    for i in ex.farthest_first:
        total = near_sum(i, rs3, rs3_near, started)
        copies.append((i, reduce_far(i, total, rs3_far_src, rs3_far, rs3_fs, rs3_fr)))
    pending += [c for _, c in copies]
    for copy in sq_started:
        copy.wait_recv()
    base = square_part + sq_near[0] + sq_near[1]
    sq_far_src[0] = base + sq_near[2]
    sq_far_src[1] = base + sq_near[3]
    sq_far_src[2] = base
    sq_copies = []
    for i in ex.farthest_first:
        which_sum = 2 if i == count - 1 else (0 if i < half else 1)
        copy = ex.copy(
            sq_far_src.at[which_sum], sq_far.at[i], sq_fs.at[i], sq_fr.at[i], -ex.reach[i]
        )
        copy.start()
        sq_copies.append(copy)
    pending += sq_copies
    for copy in sq_copies:
        copy.wait_recv()
    square_two = square_part
    for i in range(count):
        square_two += sq_far[i]
    second_all = lax.rsqrt(square_two / width + epsilon)
    row_of = z * seq + lax.broadcasted_iota(
        jnp.int32, (parts * seq, second_all.shape[1]), 0
    ) % seq
    lane_of = lax.broadcasted_iota(jnp.int32, (parts * seq, second_all.shape[1]), 1)
    second = jnp.sum(jnp.where(lane_of == row_of, second_all, 0.0), axis=1, keepdims=True)
    up = far_sum(rs3, rs3_far, copies)
    hidden = jnp.square(jnp.maximum(second * up, 0.0)).astype(bf16)

    ag4[own] = hidden
    copies = gather_far(ag4, ag4_fs, ag4_fr)
    pending += list(copies.values())
    started = gather_near(ag4, copies, ag4_ns, ag4_nr)
    pending += started
    for copy in started:
        copy.wait_recv()
    everyone = ag4[...].reshape(n_kv * parts * seq, wide)
    by_part = nt(wdn_v[...], everyone)
    part_of_column = (
        lax.broadcasted_iota(jnp.int32, (block, n_kv * parts * seq), 1) // seq
    ) % parts
    chosen = by_part[0:block]
    for j in range(1, parts):
        chosen = jnp.where(part_of_column == j, by_part[j * block : (j + 1) * block], chosen)
    lowered_part = exact_nn(chosen, spread16).astype(bf16).astype(f32)
    low_src[...] = lowered_part.reshape(low_src.shape)
    copies = to_tp(lambda peer: low_src.at[peer], low, low_s, low_r)
    pending += copies
    low[t] = low_src[t]
    for copy in copies:
        copy.wait_recv()
    lowered = low[0]
    for k in range(1, n_tp):
        lowered += low[k]
    out_ref[...] = (mid[t] + lowered).astype(bf16)
    for copy in pending:
        copy.wait_send()
    store.wait()


def solution(mesh):
    n_kv, n_tp = mesh.shape["kv"], mesh.shape["tp"]

    def local(
        tokens,
        state,
        norm_gain,
        w_query,
        w_key,
        w_value,
        w_beta,
        w_decay,
        a_log,
        dt_bias,
        head_gain,
        w_out,
        mixer_gain,
        w_up,
        w_down,
    ):
        seq, heads, head = state.shape[:3]
        rows, mine = tokens.shape
        block = w_query.shape[0]
        parts = w_up.shape[1] * seq * n_kv // (rows * 2 * head)
        wide = w_up.shape[1] // parts
        count = n_kv // 4
        dims = (n_kv, n_tp, seq, heads, block * n_kv)
        vmem, hbm, smem = (
            pl.BlockSpec(memory_space=pltpu.VMEM),
            pl.BlockSpec(memory_space=pl.ANY),
            pl.BlockSpec(memory_space=pltpu.SMEM),
        )
        dma = pltpu.SemaphoreType.DMA
        blocks = (parts * seq, wide)
        near = (3 * count - 1,)
        n_local = 3 * heads + 2 + 1 + heads + 2 * parts + 1
        scratch = [
            pltpu.VMEM((n_tp, mine, rows), f32),
            pltpu.VMEM(state.shape, f32),
            pltpu.VMEM((2 * heads * block, 2 * head), bf16),
            pltpu.VMEM((2, w_beta.shape[1], head), bf16),
            pltpu.VMEM((heads * block, head), bf16),
            pltpu.VMEM((parts * block, wide), bf16),
            pltpu.VMEM((parts * block, wide), bf16),
            pltpu.VMEM((n_kv, *blocks), bf16),
            pltpu.VMEM((3 * count - 1, *blocks), bf16),
            pltpu.VMEM((count, *blocks), bf16),
            pltpu.VMEM((count, *blocks), bf16),
            pltpu.VMEM((n_kv, heads * seq, head), f32),
            pltpu.VMEM((n_tp, block, rows), bf16),
            pltpu.VMEM((n_tp, mine, rows), f32),
            pltpu.VMEM((n_kv, *blocks), bf16),
            pltpu.VMEM((3 * count - 1, *blocks), bf16),
            pltpu.VMEM((count, *blocks), bf16),
            pltpu.VMEM((count, *blocks), bf16),
            pltpu.VMEM((1, rows), f32),
            pltpu.VMEM((4, 1, rows), f32),
            pltpu.VMEM((3, 1, rows), f32),
            pltpu.VMEM((count, 1, rows), f32),
            pltpu.VMEM((n_kv, *blocks), bf16),
            pltpu.VMEM((n_tp, mine, rows), f32),
            pltpu.VMEM((n_tp, mine, rows), f32),
            dma((n_local,)),
            dma((n_tp - 1,)),
            dma((n_tp - 1,)),
            dma(near),
            dma(near),
            dma((count,)),
            dma((count,)),
            dma(near),
            dma(near),
            dma((count,)),
            dma((count,)),
            dma((n_tp - 1,)),
            dma((n_tp - 1,)),
            dma(near),
            dma(near),
            dma((count,)),
            dma((count,)),
            dma((4,)),
            dma((4,)),
            dma((count,)),
            dma((count,)),
            dma(near),
            dma(near),
            dma((count,)),
            dma((count,)),
            dma((n_tp - 1,)),
            dma((n_tp - 1,)),
            pltpu.SemaphoreType.REGULAR,
            pltpu.SemaphoreType.REGULAR,
            pltpu.SemaphoreType.REGULAR,
        ]
        mixed_t, new_state = pl.pallas_call(
            functools.partial(kernel, dims),
            out_shape=(
                jax.ShapeDtypeStruct((mine, rows), bf16),
                jax.ShapeDtypeStruct(state.shape, f32),
            ),
            in_specs=[
                vmem,
                hbm,
                vmem,
                hbm,
                hbm,
                hbm,
                hbm,
                hbm,
                smem,
                smem,
                vmem,
                hbm,
                vmem,
                hbm,
                hbm,
            ],
            out_specs=(vmem, hbm),
            scratch_shapes=scratch,
            compiler_params=pltpu.CompilerParams(collective_id=0, has_side_effects=True),
        )(
            tokens.T,
            state,
            norm_gain.astype(f32).reshape(1, block),
            w_query,
            w_key,
            w_value,
            w_beta.T,
            w_decay.T,
            a_log,
            dt_bias,
            head_gain.reshape(1, head),
            w_out.T,
            mixer_gain.astype(f32).reshape(1, block),
            w_up,
            w_down.T,
        )
        return mixed_t.T, new_state

    return jax.shard_map(
        local,
        mesh=mesh,
        in_specs=(
            P("grp", ("kv", "tp")),
            P(("grp", "kv"), "tp", None, None),
            P("kv"),
            P("kv", "tp"),
            P("kv", "tp"),
            P("kv", "tp"),
            P(),
            P(),
            P("tp"),
            P("tp"),
            P(),
            P("tp", "kv"),
            P("kv"),
            P("kv", "tp"),
            P("tp", "kv"),
        ),
        out_specs=(P("grp", ("kv", "tp")), P(("grp", "kv"), "tp", None, None)),
        check_vma=False,
    )
```

```python
import functools

import jax
import jax.numpy as jnp
from jax import lax
from jax.experimental import pallas as pl
from jax.experimental.pallas import tpu as pltpu
from jax.sharding import PartitionSpec as P

MESH = pl.DeviceIdType.MESH
epsilon = 1e-06
f32 = jnp.float32
bf16 = jnp.bfloat16


def nn(a, b):
    return jnp.dot(a, b, preferred_element_type=f32)


def nt(a, b):
    return lax.dot_general(a, b, (((1,), (1,)), ((), ())), preferred_element_type=f32)


def exact_nn(a, onehot):
    high = a.astype(bf16)
    low = (a - high.astype(f32)).astype(bf16)
    return nn(high, onehot) + nn(low, onehot)


def lanes_of(x, lane):
    at = lax.broadcasted_iota(jnp.int32, x.shape, 1)
    return jnp.sum(jnp.where(at == lane, x, 0.0), axis=1, keepdims=True)


def column_of(row):
    n = row.shape[1]
    eye = lax.broadcasted_iota(jnp.int32, (n, n), 0) == lax.broadcasted_iota(
        jnp.int32, (n, n), 1
    )
    return jnp.sum(jnp.where(eye, row, 0.0), axis=1, keepdims=True)


class Exchange:
    def __init__(self, n_kv, g, z, t):
        self.n_kv, self.g, self.z, self.t = n_kv, g, z, t
        self.half = (n_kv // 2 - 1) // 3
        up = [3 + 3 * i for i in range(self.half)]
        self.reach = up + [-u for u in up]
        self.count = 2 * self.half
        self.farthest_first = [
            k * self.half + i for i in reversed(range(self.half)) for k in (0, 1)
        ]
        self.nearest_first = list(reversed(self.farthest_first))
        self.own = self.middle(self.count)

    def middle(self, i):
        return self.count + 1 + i

    def near(self, i):
        n = self.count + 1
        above = [(i, i, 1)]
        if i == self.count - 1:
            return above
        j = i if i < self.count else i - 1
        return above + [(2 * n + j, n + j, -1)]

    def device(self, offset):
        return (self.g, lax.rem(self.z + offset + self.n_kv, self.n_kv), self.t)

    def copy(self, src, dst, send, recv, offset):
        return pltpu.make_async_remote_copy(
            src_ref=src,
            dst_ref=dst,
            send_sem=send,
            recv_sem=recv,
            device_id=self.device(offset),
            device_id_type=MESH,
        )


def placing(per_slot, n_kv, seq, z):
    half = (n_kv // 2 - 1) // 3
    n = 2 * half + 1
    shape = (n_kv * per_slot, n_kv * seq)
    m = lax.broadcasted_iota(jnp.int32, shape, 0)
    slot = m // per_slot
    group = (slot >= n).astype(jnp.int32) + (slot >= 2 * n).astype(jnp.int32)
    i = slot - n * group
    reach = jnp.where(i < half, 3 + 3 * i, 3 * half - 3 - 3 * i)
    reach = jnp.where((i == n - 1) | (slot == n_kv - 1), 0, reach)
    owner = (z - (reach + 1 - group) + n_kv) % n_kv
    row = owner * seq + m % seq
    return (row == lax.broadcasted_iota(jnp.int32, shape, 1)).astype(bf16)


def kernel(
    dims,
    tok_ref,
    state_hbm,
    gain_ref,
    wq_hbm,
    wk_hbm,
    wv_hbm,
    wb_hbm,
    wd_hbm,
    alog_ref,
    dt_ref,
    hgain_ref,
    wo_hbm,
    mgain_ref,
    wu_hbm,
    wdn_hbm,
    out_ref,
    state_out,
    tok_all,
    state_v,
    rhs1,
    wext,
    wo_v,
    wu_v,
    wdn_v,
    rs1,
    rs1_near,
    rs1_far_src,
    rs1_far,
    ag2,
    att,
    mid,
    rs3,
    rs3_near,
    rs3_far_src,
    rs3_far,
    sq_src,
    sq_near,
    sq_far_src,
    sq_far,
    ag4,
    low_src,
    low,
    loc,
    tok_s,
    tok_r,
    rs1_ns,
    rs1_nr,
    rs1_fs,
    rs1_fr,
    ag2_ns,
    ag2_nr,
    ag2_fs,
    ag2_fr,
    att_s,
    att_r,
    rs3_ns,
    rs3_nr,
    rs3_fs,
    rs3_fr,
    sq_ns,
    sq_nr,
    sq_fs,
    sq_fr,
    ag4_ns,
    ag4_nr,
    ag4_fs,
    ag4_fr,
    low_s,
    low_r,
    sem_a,
    sem_b,
    sem_c,
):
    n_kv, n_tp, seq, heads, width = dims
    g, z, t = lax.axis_index("grp"), lax.axis_index("kv"), lax.axis_index("tp")
    ex = Exchange(n_kv, g, z, t)
    count = ex.count
    block = tok_all.shape[0] * tok_all.shape[1]
    mine = tok_all.shape[1]
    head = hgain_ref.shape[1]
    own = ex.own

    def tp_peer(k):
        return (g, z, lax.rem(t + k, n_tp))

    barrier = pltpu.get_barrier_semaphore()
    for k in range(1, n_tp):
        pl.semaphore_signal(barrier, inc=1, device_id=tp_peer(k), device_id_type=MESH)
    for offset in (1, -1, 3, -3):
        pl.semaphore_signal(barrier, inc=1, device_id=ex.device(offset), device_id_type=MESH)

    local = []

    def fetch(src, dst):
        copy = pltpu.make_async_copy(src, dst, loc.at[len(local)])
        copy.start()
        local.append(copy)

    for i, w in enumerate((wq_hbm, wk_hbm)):
        for h in range(heads):
            at = (i * heads + h) * block
            fetch(w.at[:, h * head : (h + 1) * head], rhs1.at[at : at + block, 0:head])
    for h in range(heads):
        fetch(
            wv_hbm.at[:, h * head : (h + 1) * head],
            rhs1.at[h * block : (h + 1) * block, head : 2 * head],
        )
    lanes = wext.shape[2]
    at = pl.multiple_of((z * block // lanes) * lanes, lanes)
    fetch(wb_hbm.at[:, pl.ds(at, lanes)], wext.at[0])
    fetch(wd_hbm.at[:, pl.ds(at, lanes)], wext.at[1])
    first_fetch = len(local)
    fetch(state_hbm, state_v)
    second_fetch = len(local)
    for h in range(heads):
        fetch(wo_hbm.at[:, h * head : (h + 1) * head], wo_v.at[h * block : (h + 1) * block])
    third_fetch = len(local)
    parts = wu_v.shape[0] // block
    wide = wu_v.shape[1]
    for j in range(parts):
        fetch(wu_hbm.at[:, j * wide : (j + 1) * wide], wu_v.at[j * block : (j + 1) * block])
    for j in range(parts):
        fetch(wdn_hbm.at[:, j * wide : (j + 1) * wide], wdn_v.at[j * block : (j + 1) * block])
    all_fetch = len(local)

    tok_all[t] = tok_ref[...].astype(f32)
    rhs1[heads * block :, head:] = jnp.zeros((heads * block, head), bf16)
    spread16 = placing(parts * seq, n_kv, seq, z)
    part_of_row = (
        lax.broadcasted_iota(jnp.int32, (n_kv * parts * seq, parts * block), 0) // seq
    ) % parts
    part_mask = part_of_row == (
        lax.broadcasted_iota(jnp.int32, (n_kv * parts * seq, parts * block), 1) // block
    )
    gain = column_of(gain_ref[...])
    mixer_gain = column_of(mgain_ref[...])

    pl.semaphore_wait(barrier, n_tp - 1 + 4)
    for offset in (3, -3):
        pl.semaphore_signal(sem_a, inc=1, device_id=ex.device(offset), device_id_type=MESH)

    def to_tp(src_of, dst, send, recv):
        copies = []
        for k in range(1, n_tp):
            peer = lax.rem(t + k, n_tp)
            copy = pltpu.make_async_remote_copy(
                src_ref=src_of(peer),
                dst_ref=dst.at[t],
                send_sem=send.at[k - 1],
                recv_sem=recv.at[k - 1],
                device_id=(g, z, peer),
                device_id_type=MESH,
            )
            copy.start()
            copies.append(copy)
        return copies

    pending = []
    copies = to_tp(lambda peer: tok_all.at[t], tok_all, tok_s, tok_r)
    pending += copies
    for k in range(first_fetch):
        local[k].wait()
    odd = lax.rem(z, lanes // block) if lanes // block > 1 else 0
    pieces = []
    for i in range(2):
        piece = wext[i][:, 0:block]
        for k in range(1, lanes // block):
            piece = jnp.where(odd == k, wext[i][:, k * block : (k + 1) * block], piece)
        pieces.append(piece)
    n_heads = pieces[0].shape[0]
    wext_t = jnp.concatenate(
        pieces + [jnp.zeros((head - 2 * n_heads, block), bf16)], axis=0
    )
    at_row = lax.broadcasted_iota(jnp.int32, (head, block), 0)
    square_t = (at_row == 2 * n_heads).astype(bf16)
    ext_t = jnp.concatenate([wext_t, square_t], axis=1)

    pl.semaphore_wait(sem_a, 2)
    for offset in (6, -6):
        pl.semaphore_signal(sem_b, inc=1, device_id=ex.device(offset), device_id_type=MESH)
    for copy in copies:
        copy.wait_recv()

    def spread(x_t):
        stacked = jnp.concatenate([x_t] * parts, axis=0)
        rows = nt(spread16, stacked)
        return jnp.where(part_mask, rows, 0.0).astype(bf16)

    tok_t = tok_all[...].reshape(block, tok_all.shape[2])
    scaled_t = (tok_t * gain).astype(bf16)
    left = spread(scaled_t)
    both = jnp.concatenate([scaled_t, (tok_t * tok_t).astype(bf16)], axis=0)
    left2 = nt(spread16, both)
    left2 = jnp.where(part_of_row[:, 0 : 2 * block] >= heads, left2, 0.0).astype(bf16)
    product = nn(left, rhs1[...])
    extra = nt(left2, ext_t)
    product = jnp.concatenate([product[:, :head], product[:, head:] + extra], axis=1)
    rs1[...] = product.astype(bf16).reshape(rs1.shape)

    def reduce_near(buf, near_buf, send, recv):
        started = {}
        for i in ex.farthest_first + [count]:
            for slot, k, step in ex.near(i):
                copy = ex.copy(buf.at[slot], near_buf.at[k], send.at[k], recv.at[k], -step)
                copy.start()
                started[k] = copy
        return started

    def near_sum(i, buf, near_buf, started):
        total = buf[ex.middle(i)].astype(f32)
        for _, k, _ in ex.near(i):
            started[k].wait_recv()
            total += near_buf[k].astype(f32)
        return total

    def reduce_far(i, total, far_src, far_buf, send, recv):
        far_src[i] = total.astype(far_src.dtype)
        copy = ex.copy(far_src.at[i], far_buf.at[i], send.at[i], recv.at[i], -ex.reach[i])
        copy.start()
        return copy

    def far_sum(total, far_buf, copies):
        for i, copy in reversed(copies):
            copy.wait_recv()
            total += far_buf[i].astype(f32)
        return total

    started = reduce_near(rs1, rs1_near, rs1_ns, rs1_nr)
    pending += list(started.values())
    pl.semaphore_wait(sem_b, 2)
    for offset in (3, -3):
        pl.semaphore_signal(sem_c, inc=1, device_id=ex.device(offset), device_id_type=MESH)
    copies = []
    last = [i for i in ex.farthest_first if abs(ex.reach[i]) > 12]
    for i in ex.farthest_first:
        if i not in last:
            total = near_sum(i, rs1, rs1_near, started)
            copies.append((i, reduce_far(i, total, rs1_far_src, rs1_far, rs1_fs, rs1_fr)))
    totals = [near_sum(i, rs1, rs1_near, started) for i in last]
    pl.semaphore_wait(sem_c, 2)
    for i, total in zip(last, totals):
        copies.insert(0, (i, reduce_far(i, total, rs1_far_src, rs1_far, rs1_fs, rs1_fr)))
    home = near_sum(count, rs1, rs1_near, started)
    pending += [c for _, c in copies]

    local[first_fetch].wait()
    for k in range(second_fetch, third_fetch):
        local[k].wait()
    sums = far_sum(home, rs1_far, copies)

    rows = heads * seq
    query_sum, key_sum = sums[:rows, :head], sums[rows:, :head]
    value_sum, extra = sums[:rows, head:], sums[rows:, head:]
    which = lax.broadcasted_iota(jnp.int32, (rows, head), 0) // seq
    lane = lax.broadcasted_iota(jnp.int32, (rows, head), 1)
    beta_sum = jnp.sum(
        jnp.where(lane == t * heads + which, extra, 0.0), axis=1, keepdims=True
    )
    decay_sum = jnp.sum(
        jnp.where(lane == n_heads + t * heads + which, extra, 0.0), axis=1, keepdims=True
    )
    square_sum = lanes_of(extra, 2 * n_heads)
    first = lax.rsqrt(square_sum / width + epsilon)
    query_pre, key_pre, value_pre = first * query_sum, first * key_sum, first * value_sum
    query = query_pre * lax.rsqrt(jnp.sum(query_pre * query_pre, axis=1, keepdims=True) + epsilon)
    key = key_pre * lax.rsqrt(jnp.sum(key_pre * key_pre, axis=1, keepdims=True) + epsilon)
    beta = jax.nn.sigmoid(first * beta_sum)
    which1 = lax.broadcasted_iota(jnp.int32, (rows, 1), 0) // seq
    a_log = jnp.zeros((rows, 1), f32)
    dt_bias = jnp.zeros((rows, 1), f32)
    for h in range(heads):
        a_log = jnp.where(which1 == h, alog_ref[h], a_log)
        dt_bias = jnp.where(which1 == h, dt_ref[h], dt_bias)
    logit = first * decay_sum + dt_bias
    softplus = jnp.maximum(logit, 0.0) + jnp.log1p(jnp.exp(-jnp.abs(logit)))
    decay = jnp.exp(-jnp.exp(a_log) * softplus)
    query_t, key_t = query.T, key.T
    key_reads, query_reads = [], []
    for k in range(rows):
        matrix = state_v[k % seq, k // seq]
        key_reads.append(jnp.sum(matrix * key_t[:, k : k + 1], axis=0, keepdims=True))
        query_reads.append(jnp.sum(matrix * query_t[:, k : k + 1], axis=0, keepdims=True))
    key_read = jnp.concatenate(key_reads, axis=0)
    query_read = jnp.concatenate(query_reads, axis=0)
    fresh = beta * (value_pre - decay * key_read)
    meeting = jnp.sum(query * key, axis=1, keepdims=True)
    reading = decay * query_read + meeting * fresh
    normed = (
        reading
        * lax.rsqrt(jnp.mean(reading * reading, axis=1, keepdims=True) + epsilon)
        * hgain_ref[...]
    )

    def gather_far(buf, far_send, far_recv, send, recv):
        copies = {}
        for i in ex.farthest_first:
            copy = ex.copy(
                buf.at[own],
                buf.at[ex.middle(i)],
                far_send.at[i],
                far_recv.at[i],
                ex.reach[i],
            )
            copy.start()
            copies[i] = copy
        return copies, pass_on(count, buf, send, recv)

    def pass_on(i, buf, send, recv):
        started = []
        for slot, k, step in ex.near(i):
            copy = ex.copy(buf.at[ex.middle(i)], buf.at[slot], send.at[k], recv.at[k], step)
            copy.start()
            started.append(copy)
        return started

    def gather_near(buf, copies, send, recv):
        started = []
        for i in ex.nearest_first:
            copies[i].wait_recv()
            started += pass_on(i, buf, send, recv)
        return started

    ag2[own] = normed.astype(bf16)
    copies, started = gather_far(ag2, ag2_fs, ag2_fr, ag2_ns, ag2_nr)
    pending += list(copies.values())
    for k in range(rows):
        matrix = state_v[k % seq, k // seq]
        state_v[k % seq, k // seq] = (
            decay[k : k + 1] * matrix + key_t[:, k : k + 1] * fresh[k : k + 1]
        )
    store = pltpu.make_async_copy(state_v, state_out, loc.at[all_fetch])
    store.start()
    spread8 = placing(heads * seq, n_kv, seq, z)
    head_of_column = (
        lax.broadcasted_iota(jnp.int32, (block, n_kv * rows), 1) // seq
    ) % heads
    started += gather_near(ag2, copies, ag2_ns, ag2_nr)
    pending += started
    for copy in started:
        copy.wait_recv()
    everyone = ag2[...].astype(f32).reshape(n_kv * rows, head).astype(bf16)
    by_head = nt(wo_v[...], everyone)
    chosen = by_head[0:block]
    for h in range(1, heads):
        chosen = jnp.where(head_of_column == h, by_head[h * block : (h + 1) * block], chosen)
    att[t] = exact_nn(chosen, spread8).astype(bf16)
    copies = to_tp(lambda peer: att.at[t], att, att_s, att_r)
    pending += copies
    for k in range(third_fetch, all_fetch):
        local[k].wait()
    for copy in copies:
        copy.wait_recv()
    attended = att[0].astype(f32)
    for k in range(1, n_tp):
        attended += att[k].astype(f32)
    middle = (tok_t + attended).astype(bf16).astype(f32)
    mid[...] = middle.reshape(mid.shape)

    scaled_t = (middle * mixer_gain).astype(bf16)
    left = spread(scaled_t)
    rs3[...] = nn(left, wu_v[...]).astype(bf16).reshape(rs3.shape)
    started = reduce_near(rs3, rs3_near, rs3_ns, rs3_nr)
    pending += list(started.values())
    square_part = jnp.sum(middle * middle, axis=0, keepdims=True)
    sq_src[...] = square_part
    sq_started = []
    for k, step in enumerate((1, -1)):
        copy = ex.copy(sq_src, sq_near.at[k], sq_ns.at[k], sq_nr.at[k], -step)
        copy.start()
        sq_started.append(copy)
    pending += sq_started
    copies = []
    for i in ex.farthest_first:
        total = near_sum(i, rs3, rs3_near, started)
        copies.append((i, reduce_far(i, total, rs3_far_src, rs3_far, rs3_fs, rs3_fr)))
    pending += [c for _, c in copies]
    for copy in sq_started:
        copy.wait_recv()
    above = square_part + sq_near[0]
    square_two = above + sq_near[1]
    sq_far_src[0] = square_two
    sq_far_src[1] = above
    sq_copies = []
    for i in ex.farthest_first:
        copy = ex.copy(
            sq_far_src.at[int(i == count - 1)],
            sq_far.at[i],
            sq_fs.at[i],
            sq_fr.at[i],
            -ex.reach[i],
        )
        copy.start()
        sq_copies.append(copy)
    pending += sq_copies
    home = near_sum(count, rs3, rs3_near, started)
    for copy in sq_copies:
        copy.wait_recv()
    for i in range(count):
        square_two += sq_far[i]
    second_all = lax.rsqrt(square_two / width + epsilon)
    row_of = z * seq + lax.broadcasted_iota(
        jnp.int32, (parts * seq, second_all.shape[1]), 0
    ) % seq
    lane_of = lax.broadcasted_iota(jnp.int32, (parts * seq, second_all.shape[1]), 1)
    second = jnp.sum(jnp.where(lane_of == row_of, second_all, 0.0), axis=1, keepdims=True)
    up = far_sum(home, rs3_far, copies)
    hidden = jnp.square(jnp.maximum(second * up, 0.0)).astype(bf16)

    ag4[own] = hidden
    copies, started = gather_far(ag4, ag4_fs, ag4_fr, ag4_ns, ag4_nr)
    pending += list(copies.values())
    started += gather_near(ag4, copies, ag4_ns, ag4_nr)
    pending += started
    for copy in started:
        copy.wait_recv()
    everyone = ag4[...].reshape(n_kv * parts * seq, wide)
    by_part = nt(wdn_v[...], everyone)
    part_of_column = (
        lax.broadcasted_iota(jnp.int32, (block, n_kv * parts * seq), 1) // seq
    ) % parts
    chosen = by_part[0:block]
    for j in range(1, parts):
        chosen = jnp.where(part_of_column == j, by_part[j * block : (j + 1) * block], chosen)
    lowered_part = exact_nn(chosen, spread16).astype(bf16).astype(f32)
    low_src[...] = lowered_part.reshape(low_src.shape)
    copies = to_tp(lambda peer: low_src.at[peer], low, low_s, low_r)
    pending += copies
    low[t] = low_src[t]
    for copy in copies:
        copy.wait_recv()
    lowered = low[0]
    for k in range(1, n_tp):
        lowered += low[k]
    out_ref[...] = (mid[t] + lowered).astype(bf16)
    for copy in pending:
        copy.wait_send()
    store.wait()


def solution(mesh):
    n_kv, n_tp = mesh.shape["kv"], mesh.shape["tp"]

    def local(
        tokens,
        state,
        norm_gain,
        w_query,
        w_key,
        w_value,
        w_beta,
        w_decay,
        a_log,
        dt_bias,
        head_gain,
        w_out,
        mixer_gain,
        w_up,
        w_down,
    ):
        seq, heads, head = state.shape[:3]
        rows, mine = tokens.shape
        block = w_query.shape[0]
        parts = w_up.shape[1] // (2 * head)
        wide = w_up.shape[1] // parts
        count = 2 * ((n_kv // 2 - 1) // 3)
        dims = (n_kv, n_tp, seq, heads, block * n_kv)
        vmem, hbm, smem = (
            pl.BlockSpec(memory_space=pltpu.VMEM),
            pl.BlockSpec(memory_space=pl.ANY),
            pl.BlockSpec(memory_space=pltpu.SMEM),
        )
        dma = pltpu.SemaphoreType.DMA
        blocks = (parts * seq, wide)
        near = (n_kv - count - 1,)
        n_local = 3 * heads + 2 + 1 + heads + 2 * parts + 1
        scratch = [
            pltpu.VMEM((n_tp, mine, rows), f32),
            pltpu.VMEM(state.shape, f32),
            pltpu.VMEM((2 * heads * block, 2 * head), bf16),
            pltpu.VMEM((2, w_beta.shape[1], head), bf16),
            pltpu.VMEM((heads * block, head), bf16),
            pltpu.VMEM((parts * block, wide), bf16),
            pltpu.VMEM((parts * block, wide), bf16),
            pltpu.VMEM((n_kv, *blocks), bf16),
            pltpu.VMEM((*near, *blocks), bf16),
            pltpu.VMEM((count, *blocks), bf16),
            pltpu.VMEM((count, *blocks), bf16),
            pltpu.VMEM((n_kv, heads * seq, head), bf16),
            pltpu.VMEM((n_tp, block, rows), bf16),
            pltpu.VMEM((n_tp, mine, rows), f32),
            pltpu.VMEM((n_kv, *blocks), bf16),
            pltpu.VMEM((*near, *blocks), bf16),
            pltpu.VMEM((count, *blocks), bf16),
            pltpu.VMEM((count, *blocks), bf16),
            pltpu.VMEM((1, rows), f32),
            pltpu.VMEM((2, 1, rows), f32),
            pltpu.VMEM((2, 1, rows), f32),
            pltpu.VMEM((count, 1, rows), f32),
            pltpu.VMEM((n_kv, *blocks), bf16),
            pltpu.VMEM((n_tp, mine, rows), f32),
            pltpu.VMEM((n_tp, mine, rows), f32),
            dma((n_local,)),
            dma((n_tp - 1,)),
            dma((n_tp - 1,)),
            dma(near),
            dma(near),
            dma((count,)),
            dma((count,)),
            dma(near),
            dma(near),
            dma((count,)),
            dma((count,)),
            dma((n_tp - 1,)),
            dma((n_tp - 1,)),
            dma(near),
            dma(near),
            dma((count,)),
            dma((count,)),
            dma((2,)),
            dma((2,)),
            dma((count,)),
            dma((count,)),
            dma(near),
            dma(near),
            dma((count,)),
            dma((count,)),
            dma((n_tp - 1,)),
            dma((n_tp - 1,)),
            pltpu.SemaphoreType.REGULAR,
            pltpu.SemaphoreType.REGULAR,
            pltpu.SemaphoreType.REGULAR,
        ]
        mixed_t, new_state = pl.pallas_call(
            functools.partial(kernel, dims),
            out_shape=(
                jax.ShapeDtypeStruct((mine, rows), bf16),
                jax.ShapeDtypeStruct(state.shape, f32),
            ),
            in_specs=[
                vmem,
                hbm,
                vmem,
                hbm,
                hbm,
                hbm,
                hbm,
                hbm,
                smem,
                smem,
                vmem,
                hbm,
                vmem,
                hbm,
                hbm,
            ],
            out_specs=(vmem, hbm),
            scratch_shapes=scratch,
            compiler_params=pltpu.CompilerParams(collective_id=0, has_side_effects=True),
        )(
            tokens.T,
            state,
            norm_gain.astype(f32).reshape(1, block),
            w_query,
            w_key,
            w_value,
            w_beta.T,
            w_decay.T,
            a_log,
            dt_bias,
            head_gain.reshape(1, head),
            w_out.T,
            mixer_gain.astype(f32).reshape(1, block),
            w_up,
            w_down.T,
        )
        return mixed_t.T, new_state

    return jax.shard_map(
        local,
        mesh=mesh,
        in_specs=(
            P("grp", ("kv", "tp")),
            P(("grp", "kv"), "tp", None, None),
            P("kv"),
            P("kv", "tp"),
            P("kv", "tp"),
            P("kv", "tp"),
            P(),
            P(),
            P("tp"),
            P("tp"),
            P(),
            P("tp", "kv"),
            P("kv"),
            P("kv", "tp"),
            P("tp", "kv"),
        ),
        out_specs=(P("grp", ("kv", "tp")), P(("grp", "kv"), "tp", None, None)),
        check_vma=False,
    )
```

```python
import functools

import jax
import jax.numpy as jnp
from jax import lax
from jax.experimental import pallas as pl
from jax.experimental.pallas import tpu as pltpu
from jax.sharding import PartitionSpec as P

MESH = pl.DeviceIdType.MESH
epsilon = 1e-06
f32 = jnp.float32
bf16 = jnp.bfloat16


def nn(a, b):
    return jnp.dot(a, b, preferred_element_type=f32)


def nt(a, b):
    return lax.dot_general(a, b, (((1,), (1,)), ((), ())), preferred_element_type=f32)


def exact_nn(a, onehot):
    high = a.astype(bf16)
    low = (a - high.astype(f32)).astype(bf16)
    return nn(high, onehot) + nn(low, onehot)


def lanes_of(x, lane):
    at = lax.broadcasted_iota(jnp.int32, x.shape, 1)
    return jnp.sum(jnp.where(at == lane, x, 0.0), axis=1, keepdims=True)


def column_of(row):
    n = row.shape[1]
    eye = lax.broadcasted_iota(jnp.int32, (n, n), 0) == lax.broadcasted_iota(
        jnp.int32, (n, n), 1
    )
    return jnp.sum(jnp.where(eye, row, 0.0), axis=1, keepdims=True)


UP_WINDOW = (-1, 0, 1, 2)
DOWN_WINDOW = (-2, -1, 0, 1)


class Exchange:
    def __init__(self, n_kv, g, z, t):
        self.n_kv, self.g, self.z, self.t = n_kv, g, z, t
        self.half = n_kv // 8
        up = [2 + 4 * i for i in range(self.half)]
        self.reach = up + [-u for u in up]
        self.count = 2 * self.half
        self.steps = [(0, 1), (1, -1)]
        self.farthest_first = [
            k * self.half + i for i in reversed(range(self.half)) for k in (0, 1)
        ]
        self.nearest_first = list(reversed(self.farthest_first))

    def device(self, offset):
        return (self.g, lax.rem(self.z + offset + self.n_kv, self.n_kv), self.t)

    def near(self, i):
        last = () if i == self.count - 1 else ((3, 2 if i < self.half else -2),)
        return self.steps + list(last)

    def copy(self, src, dst, send, recv, offset):
        return pltpu.make_async_remote_copy(
            src_ref=src,
            dst_ref=dst,
            send_sem=send,
            recv_sem=recv,
            device_id=self.device(offset),
            device_id_type=MESH,
        )


def placing(per_slot, n_kv, seq, z):
    count = n_kv // 4
    half = count // 2
    shape = (n_kv * per_slot, n_kv * seq)
    m = lax.broadcasted_iota(jnp.int32, shape, 0)
    slot = m // per_slot
    i = slot % count
    group = slot // count
    reach = jnp.where(i < half, 2 + 4 * i, 4 * half - 2 - 4 * i)
    side = jnp.where(i < half, 2, -2)
    step = jnp.where(group == 0, 1, jnp.where(group == 1, -1, jnp.where(group == 2, 0, side)))
    offset = jnp.where(slot == n_kv - 1, 0, reach + step)
    owner = (z - offset + n_kv) % n_kv
    row = owner * seq + m % seq
    return (row == lax.broadcasted_iota(jnp.int32, shape, 1)).astype(bf16)


def kernel(
    dims,
    tok_ref,
    state_hbm,
    gain_ref,
    wq_hbm,
    wk_hbm,
    wv_hbm,
    wb_hbm,
    wd_hbm,
    alog_ref,
    dt_ref,
    hgain_ref,
    wo_hbm,
    mgain_ref,
    wu_hbm,
    wdn_hbm,
    out_ref,
    state_out,
    tok_all,
    tok_near,
    state_v,
    rhs1,
    wext,
    wo_v,
    wu_v,
    wdn_v,
    rs1,
    rs1_near,
    rs1_far_src,
    rs1_far,
    ag2_src,
    ag2,
    diag,
    att,
    mid_src,
    mid,
    rs3,
    rs3_far,
    sq_src,
    sq_far,
    ag4_src,
    ag4,
    fin_src,
    fin,
    loc,
    tok_s,
    tok_r,
    rs1_ns,
    rs1_nr,
    rs1_fs,
    rs1_fr,
    win_s,
    win_r,
    ag2_s,
    ag2_r,
    att_s,
    att_r,
    rs3_s,
    rs3_r,
    sq_s,
    sq_r,
    mid_s,
    mid_r,
    ag4_s,
    ag4_r,
    fin_s,
    fin_r,
    sem_a,
    sem_b,
    sem_c,
):
    n_kv, n_tp, seq, heads, width = dims
    g, z, t = lax.axis_index("grp"), lax.axis_index("kv"), lax.axis_index("tp")
    ex = Exchange(n_kv, g, z, t)
    count, half = ex.count, ex.half
    mine = tok_ref.shape[0]
    block = n_tp * mine
    all_rows = tok_ref.shape[1]
    head = hgain_ref.shape[1]
    own = n_kv - 1

    def tp_peer(k):
        return (g, z, lax.rem(t + k, n_tp))

    barrier = pltpu.get_barrier_semaphore()
    for k in range(1, n_tp):
        pl.semaphore_signal(barrier, inc=1, device_id=tp_peer(k), device_id_type=MESH)
    for offset in (1, -1, 2, -2):
        pl.semaphore_signal(barrier, inc=1, device_id=ex.device(offset), device_id_type=MESH)

    local = []

    def fetch(src, dst):
        copy = pltpu.make_async_copy(src, dst, loc.at[len(local)])
        copy.start()
        local.append(copy)

    for i, w in enumerate((wq_hbm, wk_hbm)):
        for h in range(heads):
            at = (i * heads + h) * block
            fetch(w.at[:, h * head : (h + 1) * head], rhs1.at[at : at + block, 0:head])
    for h in range(heads):
        fetch(
            wv_hbm.at[:, h * head : (h + 1) * head],
            rhs1.at[h * block : (h + 1) * block, head : 2 * head],
        )
    lanes = wext.shape[2]
    at = pl.multiple_of((z * block // lanes) * lanes, lanes)
    fetch(wb_hbm.at[:, pl.ds(at, lanes)], wext.at[0])
    fetch(wd_hbm.at[:, pl.ds(at, lanes)], wext.at[1])
    first_fetch = len(local)
    fetch(state_hbm, state_v)
    second_fetch = len(local)
    parts = wu_v.shape[1] // (2 * head)
    wide = 2 * head
    kinds = heads * seq
    n_win = len(UP_WINDOW)
    out_wide = heads * head
    here_up, here_down = UP_WINDOW.index(0), DOWN_WINDOW.index(0)
    fetch(wo_hbm, wo_v.at[:, here_up * out_wide : (here_up + 1) * out_wide])
    fetch(wu_hbm, wu_v.at[here_up * block : (here_up + 1) * block])
    fetch(wdn_hbm, wdn_v.at[here_down * block : (here_down + 1) * block])
    all_fetch = len(local)

    tok_all[t] = tok_ref[...].astype(f32)
    gain_row = mgain_ref[...].astype(f32).reshape(1, block)
    gain_row = jnp.concatenate([gain_row, jnp.zeros((1, all_rows - block), f32)], axis=1)
    tok_all[n_tp] = jnp.broadcast_to(gain_row, (mine, all_rows))
    rhs1[heads * block :, head:] = jnp.zeros((heads * block, head), bf16)
    diag[...] = jnp.zeros(diag.shape, bf16)
    spread16 = placing(parts * seq, n_kv, seq, z)
    part_of_row = (
        lax.broadcasted_iota(jnp.int32, (n_kv * parts * seq, parts * block), 0) // seq
    ) % parts
    part_mask = part_of_row == (
        lax.broadcasted_iota(jnp.int32, (n_kv * parts * seq, parts * block), 1) // block
    )
    gain = column_of(gain_ref[...].astype(f32).reshape(1, block))

    pl.semaphore_wait(barrier, n_tp - 1 + 4)
    for offset in (2, -2):
        pl.semaphore_signal(sem_a, inc=1, device_id=ex.device(offset), device_id_type=MESH)

    def to_tp(src_of, dst, send, recv):
        copies = []
        for k in range(1, n_tp):
            peer = lax.rem(t + k, n_tp)
            copy = pltpu.make_async_remote_copy(
                src_ref=src_of(peer),
                dst_ref=dst.at[t],
                send_sem=send.at[k - 1],
                recv_sem=recv.at[k - 1],
                device_id=(g, z, peer),
                device_id_type=MESH,
            )
            copy.start()
            copies.append(copy)
        return copies

    pending = []
    copies = to_tp(lambda peer: tok_all.at[t], tok_all, tok_s, tok_r)
    pending += copies
    for k in range(first_fetch):
        local[k].wait()
    odd = lax.rem(z, lanes // block) if lanes // block > 1 else 0
    pieces = []
    for i in range(2):
        piece = wext[i][:, 0:block]
        for k in range(1, lanes // block):
            piece = jnp.where(odd == k, wext[i][:, k * block : (k + 1) * block], piece)
        pieces.append(piece)
    n_heads = pieces[0].shape[0]
    wext_t = jnp.concatenate(
        pieces + [jnp.zeros((head - 2 * n_heads, block), bf16)], axis=0
    )
    at_row = lax.broadcasted_iota(jnp.int32, (head, block), 0)
    square_t = (at_row == 2 * n_heads).astype(bf16)
    ext_t = jnp.concatenate([wext_t, square_t], axis=1)

    pl.semaphore_wait(sem_a, 2)
    for offset in (4, -4):
        pl.semaphore_signal(sem_b, inc=1, device_id=ex.device(offset), device_id_type=MESH)
    for copy in copies:
        copy.wait_recv()

    def spread(x_t):
        stacked = jnp.concatenate([x_t] * parts, axis=0)
        rows = nt(spread16, stacked)
        return jnp.where(part_mask, rows, 0.0).astype(bf16)

    tok_t = tok_all[0:n_tp].reshape(block, all_rows)
    scaled_t = (tok_t * gain).astype(bf16)
    left = spread(scaled_t)
    both = jnp.concatenate([scaled_t, (tok_t * tok_t).astype(bf16)], axis=0)
    left2 = nt(spread16, both)
    left2 = jnp.where(part_of_row[:, 0 : 2 * block] >= heads, left2, 0.0).astype(bf16)
    product = nn(left, rhs1[...])
    extra = nt(left2, ext_t)
    product = jnp.concatenate([product[:, :head], product[:, head:] + extra], axis=1)
    rs1[...] = product.astype(bf16).reshape(rs1.shape)

    def reduce_near(buf, near_buf, send, recv, order):
        started = {}
        for i in order:
            for group, step in ex.near(i):
                k = group * count + i if group < 2 else 2 * count + i
                copy = ex.copy(
                    buf.at[group * count + i],
                    near_buf.at[k],
                    send.at[k],
                    recv.at[k],
                    -step,
                )
                copy.start()
                started[k] = copy
        return started

    def near_sum(i, buf, near_buf, started):
        total = buf[2 * count + i].astype(f32)
        for group, step in ex.near(i):
            k = group * count + i if group < 2 else 2 * count + i
            started[k].wait_recv()
            total += near_buf[k].astype(f32)
        return total

    def reduce_far(i, total, far_src, far_buf, send, recv):
        far_src[i] = total.astype(far_src.dtype)
        copy = ex.copy(far_src.at[i], far_buf.at[i], send.at[i], recv.at[i], -ex.reach[i])
        copy.start()
        return copy

    def far_sum(buf, far_buf, copies):
        total = buf[own].astype(f32)
        for i, copy in copies:
            copy.wait_recv()
            total += far_buf[i].astype(f32)
        return total

    close = [i for i in ex.nearest_first if abs(ex.reach[i]) <= 8]
    distant = [i for i in ex.farthest_first if abs(ex.reach[i]) > 8]
    started = reduce_near(rs1, rs1_near, rs1_ns, rs1_nr, distant + close)
    pending += list(started.values())
    pl.semaphore_wait(sem_b, 2)
    for offset in (8, -8):
        pl.semaphore_signal(sem_c, inc=1, device_id=ex.device(offset), device_id_type=MESH)
    copies = []
    for i in close:
        total = near_sum(i, rs1, rs1_near, started)
        copies.append((i, reduce_far(i, total, rs1_far_src, rs1_far, rs1_fs, rs1_fr)))
    totals = [near_sum(i, rs1, rs1_near, started) for i in distant]
    pl.semaphore_wait(sem_c, 2)
    for i, total in zip(distant, totals):
        copies.append((i, reduce_far(i, total, rs1_far_src, rs1_far, rs1_fs, rs1_fr)))
    pending += [c for _, c in copies]

    window = []

    def to_window(src, dst_of, offsets):
        begun = []
        for w, offset in enumerate(offsets):
            if offset:
                k = len(window)
                copy = ex.copy(src, dst_of(w), win_s.at[k], win_r.at[k], -offset)
                copy.start()
                window.append(copy)
                begun.append(copy)
        return begun

    tok_window = to_window(tok_all, lambda w: tok_near.at[w], UP_WINDOW)
    wo_window = to_window(
        wo_hbm, lambda w: wo_v.at[:, w * out_wide : (w + 1) * out_wide], UP_WINDOW
    )
    wu_window = to_window(wu_hbm, lambda w: wu_v.at[w * block : (w + 1) * block], UP_WINDOW)
    wdn_window = to_window(
        wdn_hbm, lambda w: wdn_v.at[w * block : (w + 1) * block], DOWN_WINDOW
    )
    pending += window

    local[first_fetch].wait()
    sums = far_sum(rs1, rs1_far, copies)

    rows = heads * seq
    query_sum, key_sum = sums[:rows, :head], sums[rows:, :head]
    value_sum, extra = sums[:rows, head:], sums[rows:, head:]
    which = lax.broadcasted_iota(jnp.int32, (rows, head), 0) // seq
    lane = lax.broadcasted_iota(jnp.int32, (rows, head), 1)
    beta_sum = jnp.sum(
        jnp.where(lane == t * heads + which, extra, 0.0), axis=1, keepdims=True
    )
    decay_sum = jnp.sum(
        jnp.where(lane == n_heads + t * heads + which, extra, 0.0), axis=1, keepdims=True
    )
    square_sum = lanes_of(extra, 2 * n_heads)
    first = lax.rsqrt(square_sum / width + epsilon)
    query_pre, key_pre, value_pre = first * query_sum, first * key_sum, first * value_sum
    query = query_pre * lax.rsqrt(jnp.sum(query_pre * query_pre, axis=1, keepdims=True) + epsilon)
    key = key_pre * lax.rsqrt(jnp.sum(key_pre * key_pre, axis=1, keepdims=True) + epsilon)
    beta = jax.nn.sigmoid(first * beta_sum)
    which1 = lax.broadcasted_iota(jnp.int32, (rows, 1), 0) // seq
    a_log = jnp.zeros((rows, 1), f32)
    dt_bias = jnp.zeros((rows, 1), f32)
    for h in range(heads):
        a_log = jnp.where(which1 == h, alog_ref[h], a_log)
        dt_bias = jnp.where(which1 == h, dt_ref[h], dt_bias)
    logit = first * decay_sum + dt_bias
    softplus = jnp.maximum(logit, 0.0) + jnp.log1p(jnp.exp(-jnp.abs(logit)))
    decay = jnp.exp(-jnp.exp(a_log) * softplus)
    query_t, key_t = query.T, key.T
    key_reads, query_reads = [], []
    for k in range(rows):
        matrix = state_v[k % seq, k // seq]
        key_reads.append(jnp.sum(matrix * key_t[:, k : k + 1], axis=0, keepdims=True))
        query_reads.append(jnp.sum(matrix * query_t[:, k : k + 1], axis=0, keepdims=True))
    key_read = jnp.concatenate(key_reads, axis=0)
    query_read = jnp.concatenate(query_reads, axis=0)
    fresh = beta * (value_pre - decay * key_read)
    meeting = jnp.sum(query * key, axis=1, keepdims=True)
    reading = decay * query_read + meeting * fresh
    normed = (
        reading
        * lax.rsqrt(jnp.mean(reading * reading, axis=1, keepdims=True) + epsilon)
        * hgain_ref[...]
    )

    def to_far(src_of, dst, send, recv, sign):
        copies = []
        for i in ex.farthest_first:
            copy = ex.copy(src_of(i), dst.at[i], send.at[i], recv.at[i], sign * ex.reach[i])
            copy.start()
            copies.append(copy)
        return copies

    ag2_src[...] = normed.astype(bf16)
    ag2_copies = to_far(lambda i: ag2_src, ag2, ag2_s, ag2_r, 1)
    pending += ag2_copies
    for k in range(rows):
        matrix = state_v[k % seq, k // seq]
        state_v[k % seq, k // seq] = (
            decay[k : k + 1] * matrix + key_t[:, k : k + 1] * fresh[k : k + 1]
        )
    store = pltpu.make_async_copy(state_v, state_out, loc.at[all_fetch])
    store.start()

    def iota(shape, dim):
        return lax.broadcasted_iota(jnp.int32, shape, dim)

    def owner_row(slot, r):
        half = ex.half
        reach = jnp.where(slot < half, 2 + 4 * slot, 4 * half - 2 - 4 * slot)
        return (z - reach + n_kv) % n_kv * seq + r

    per_w = count * seq
    shape = (n_win * all_rows, all_rows)
    lane = iota(shape, 1)
    lane_owner = owner_row(lane % per_w // seq, lane % seq)
    window_pick = (
        (lane // per_w == iota(shape, 0) // all_rows) & (lane_owner == iota(shape, 0) % all_rows)
    ).astype(bf16)
    shape = (per_w, all_rows)
    place_rows = (owner_row(iota(shape, 0) // seq, iota(shape, 0) % seq) == iota(shape, 1)).astype(
        bf16
    )
    head_picks = []
    shape = (per_w, count * kinds)
    for h in range(heads):
        r0, c1 = iota(shape, 0), iota(shape, 1)
        head_picks.append(
            (
                (c1 // kinds == r0 // seq) & (c1 % seq == r0 % seq) & (c1 // seq % heads == h)
            ).astype(bf16)
        )
    shape = (count * parts * seq, all_rows)
    r0, c1 = iota(shape, 0), iota(shape, 1)
    spread_rows = (
        (r0 // (parts * seq) == c1 % per_w // seq) & (r0 % seq == c1 % seq)
    ).astype(bf16)
    shape = (per_w, count * parts * seq)
    r0, c1 = iota(shape, 0), iota(shape, 1)
    part_picks = [
        (
            (c1 // (parts * seq) == r0 // seq) & (c1 % seq == r0 % seq) & (c1 // seq % parts == j)
        ).astype(bf16)
        for j in range(parts)
    ]
    for copy in tok_window:
        copy.wait_recv()
    token_parts = []
    mixer_gain = jnp.zeros((block, all_rows), f32)
    lane = iota((block, all_rows), 1)
    for w, offset in enumerate(UP_WINDOW):
        source = tok_near.at[w] if offset else tok_all
        token_parts.append(source[0:n_tp].reshape(block, all_rows).astype(bf16))
        column = column_of(source[n_tp][0:1, 0:block])
        mixer_gain = jnp.where(lane // per_w == w, column, mixer_gain)
    token_w = nn(jnp.concatenate(token_parts, axis=1), window_pick)
    for k in range(second_fetch, all_fetch):
        local[k].wait()
    for copy in ag2_copies:
        copy.wait_recv()
    for copy in wo_window:
        copy.wait_recv()
    everyone = ag2[...].astype(f32).reshape(count * kinds, head).astype(bf16)
    for h in range(heads):
        picked = nn(head_picks[h], everyone).astype(bf16)
        for w in range(n_win):
            at = w * out_wide + h * head
            diag[w * per_w : (w + 1) * per_w, at : at + head] = picked
    att[t] = nt(wo_v[...], diag[...]).astype(bf16)
    copies = to_tp(lambda peer: att.at[t], att, att_s, att_r)
    pending += copies
    for copy in copies:
        copy.wait_recv()
    for copy in wu_window:
        copy.wait_recv()

    attended = att[0].astype(f32)
    for k in range(1, n_tp):
        attended += att[k].astype(f32)
    middle_b = (token_w + attended).astype(bf16)
    middle = middle_b.astype(f32)
    scaled = jnp.concatenate([middle * mixer_gain] * n_win, axis=0)
    shape = scaled.shape
    scaled = jnp.where(iota(shape, 1) // per_w == iota(shape, 0) // block, scaled, 0.0)
    left = nt(spread_rows, scaled.astype(bf16))
    part = iota(left.shape, 0) // seq % parts
    product = jnp.zeros((left.shape[0], wide), f32)
    for j in range(parts):
        product += nn(
            jnp.where(part == j, left, 0.0).astype(bf16), wu_v[:, j * wide : (j + 1) * wide]
        )
    rs3[...] = product.astype(bf16).reshape(rs3.shape)
    sq_src[...] = jnp.sum(middle * middle, axis=0, keepdims=True)
    rs3_copies = to_far(lambda i: rs3.at[i], rs3_far, rs3_s, rs3_r, -1)
    sq_copies = to_far(lambda i: sq_src, sq_far, sq_s, sq_r, -1)
    pending += rs3_copies + sq_copies
    mid_copies = []
    for w, offset in enumerate(UP_WINDOW):
        placed = nt(middle_b, window_pick[w * all_rows : (w + 1) * all_rows]).astype(bf16)
        mid_src[w] = placed.reshape(n_tp, mine, all_rows)
        if offset:
            copy = ex.copy(mid_src.at[w, t], mid.at[w], mid_s.at[w], mid_r.at[w], offset)
            copy.start()
            mid_copies.append(copy)
        else:
            mid[w] = mid_src[w, t]
    pending += mid_copies
    for copy in sq_copies:
        copy.wait_recv()
    lane = iota((1, all_rows), 1)
    squares = jnp.zeros((1, all_rows), f32)
    for i in range(count):
        squares += jnp.where(lane % per_w // seq == i, sq_far[i], 0.0)
    shape = (parts * seq, all_rows)
    squares = jnp.sum(
        jnp.where(iota(shape, 1) % seq == iota(shape, 0) % seq, squares, 0.0),
        axis=1,
        keepdims=True,
    )
    second = lax.rsqrt(squares / width + epsilon)
    up = jnp.zeros((parts * seq, wide), f32)
    for copy in reversed(rs3_copies):
        copy.wait_recv()
    for i in range(count):
        up += rs3_far[i].astype(f32)
    ag4_src[...] = jnp.square(jnp.maximum(second * up, 0.0)).astype(bf16)

    ag4_copies = to_far(lambda i: ag4_src, ag4, ag4_s, ag4_r, 1)
    pending += ag4_copies
    for copy in wdn_window:
        copy.wait_recv()
    for copy in mid_copies:
        copy.wait_recv()
    middle = mid[0].astype(f32)
    for w in range(1, n_win):
        middle += mid[w].astype(f32)
    for copy in ag4_copies:
        copy.wait_recv()
    everyone = ag4[...].reshape(count * parts * seq, wide)
    picked = jnp.concatenate(
        [nn(part_picks[j], everyone).astype(bf16) for j in range(parts)], axis=1
    )
    lowered_part = nt(wdn_v[...], picked).astype(bf16)
    fin_src[...] = nn(lowered_part, place_rows).astype(bf16).reshape(fin_src.shape)
    copies = []
    for w, offset in enumerate(DOWN_WINDOW):
        row = lax.rem(z + offset + n_kv, n_kv)
        for k in range(n_tp):
            if offset == 0 and k == 0:
                fin[w, t] = fin_src[w, t]
                continue
            peer = lax.rem(t + k, n_tp)
            copy = pltpu.make_async_remote_copy(
                src_ref=fin_src.at[w, peer],
                dst_ref=fin.at[w, t],
                send_sem=fin_s.at[w * n_tp + k],
                recv_sem=fin_r.at[w * n_tp + k],
                device_id=(g, row, peer),
                device_id_type=MESH,
            )
            copy.start()
            copies.append(copy)
    pending += copies
    for copy in copies:
        copy.wait_recv()
    lowered = jnp.zeros((mine, all_rows), f32)
    for w in range(n_win):
        for k in range(n_tp):
            lowered += fin[w, k].astype(f32)
    out_ref[...] = (middle + lowered).astype(bf16)
    for copy in pending:
        copy.wait_send()
    store.wait()


def solution(mesh):
    n_kv, n_tp = mesh.shape["kv"], mesh.shape["tp"]

    def local(
        tokens,
        state,
        norm_gain,
        w_query,
        w_key,
        w_value,
        w_beta,
        w_decay,
        a_log,
        dt_bias,
        head_gain,
        w_out,
        mixer_gain,
        w_up,
        w_down,
    ):
        seq, heads, head = state.shape[:3]
        rows, mine = tokens.shape
        block = w_query.shape[0]
        parts = w_up.shape[1] // (2 * head)
        wide = w_up.shape[1] // parts
        count = n_kv // 4
        dims = (n_kv, n_tp, seq, heads, block * n_kv)
        vmem, hbm, smem = (
            pl.BlockSpec(memory_space=pltpu.VMEM),
            pl.BlockSpec(memory_space=pl.ANY),
            pl.BlockSpec(memory_space=pltpu.SMEM),
        )
        dma = pltpu.SemaphoreType.DMA
        blocks = (parts * seq, wide)
        near = (3 * count - 1,)
        far = (count,)
        n_local = 3 * heads + 2 + 1 + 3 + 1
        n_win = len(UP_WINDOW)
        scratch = [
            pltpu.VMEM((n_tp + 1, mine, rows), f32),
            pltpu.VMEM((n_win, n_tp + 1, mine, rows), f32),
            pltpu.VMEM(state.shape, f32),
            pltpu.VMEM((2 * heads * block, 2 * head), bf16),
            pltpu.VMEM((2, w_beta.shape[1], head), bf16),
            pltpu.VMEM((block, n_win * heads * head), bf16),
            pltpu.VMEM((n_win * block, w_up.shape[1]), bf16),
            pltpu.VMEM((n_win * block, w_down.shape[0]), bf16),
            pltpu.VMEM((n_kv, *blocks), bf16),
            pltpu.VMEM((*near, *blocks), bf16),
            pltpu.VMEM((count, *blocks), bf16),
            pltpu.VMEM((count, *blocks), bf16),
            pltpu.VMEM((heads * seq, head), bf16),
            pltpu.VMEM((count, heads * seq, head), bf16),
            pltpu.VMEM((rows, n_win * heads * head), bf16),
            pltpu.VMEM((n_tp, block, rows), bf16),
            pltpu.VMEM((n_win, n_tp, mine, rows), bf16),
            pltpu.VMEM((n_win, mine, rows), bf16),
            pltpu.VMEM((count, *blocks), bf16),
            pltpu.VMEM((count, *blocks), bf16),
            pltpu.VMEM((1, rows), f32),
            pltpu.VMEM((count, 1, rows), f32),
            pltpu.VMEM(blocks, bf16),
            pltpu.VMEM((count, *blocks), bf16),
            pltpu.VMEM((n_win, n_tp, mine, rows), bf16),
            pltpu.VMEM((n_win, n_tp, mine, rows), bf16),
            dma((n_local,)),
            dma((n_tp - 1,)),
            dma((n_tp - 1,)),
            dma(near),
            dma(near),
            dma(far),
            dma(far),
            dma((4 * (n_win - 1),)),
            dma((4 * (n_win - 1),)),
            dma(far),
            dma(far),
            dma((n_tp - 1,)),
            dma((n_tp - 1,)),
            dma(far),
            dma(far),
            dma(far),
            dma(far),
            dma((n_win,)),
            dma((n_win,)),
            dma(far),
            dma(far),
            dma((n_win * n_tp,)),
            dma((n_win * n_tp,)),
            pltpu.SemaphoreType.REGULAR,
            pltpu.SemaphoreType.REGULAR,
            pltpu.SemaphoreType.REGULAR,
        ]
        mixed_t, new_state = pl.pallas_call(
            functools.partial(kernel, dims),
            out_shape=(
                jax.ShapeDtypeStruct((mine, rows), bf16),
                jax.ShapeDtypeStruct(state.shape, f32),
            ),
            in_specs=[
                vmem,
                hbm,
                vmem,
                hbm,
                hbm,
                hbm,
                hbm,
                hbm,
                smem,
                smem,
                vmem,
                hbm,
                vmem,
                hbm,
                hbm,
            ],
            out_specs=(vmem, hbm),
            scratch_shapes=scratch,
            compiler_params=pltpu.CompilerParams(collective_id=0, has_side_effects=True),
        )(
            tokens.T,
            state,
            norm_gain,
            w_query,
            w_key,
            w_value,
            w_beta.T,
            w_decay.T,
            a_log,
            dt_bias,
            head_gain.reshape(1, head),
            w_out.T,
            mixer_gain,
            w_up,
            w_down.T,
        )
        return mixed_t.T, new_state

    return jax.shard_map(
        local,
        mesh=mesh,
        in_specs=(
            P("grp", ("kv", "tp")),
            P(("grp", "kv"), "tp", None, None),
            P("kv"),
            P("kv", "tp"),
            P("kv", "tp"),
            P("kv", "tp"),
            P(),
            P(),
            P("tp"),
            P("tp"),
            P(),
            P("tp", "kv"),
            P("kv"),
            P("kv", "tp"),
            P("tp", "kv"),
        ),
        out_specs=(P("grp", ("kv", "tp")), P(("grp", "kv"), "tp", None, None)),
        check_vma=False,
    )
```

```python
import functools

import jax
import jax.numpy as jnp
from jax import lax
from jax.experimental import pallas as pl
from jax.experimental.pallas import tpu as pltpu
from jax.sharding import PartitionSpec as P

MESH = pl.DeviceIdType.MESH
epsilon = 1e-06
f32 = jnp.float32
bf16 = jnp.bfloat16


def nn(a, b):
    return jnp.dot(a, b, preferred_element_type=f32)


def nt(a, b):
    return lax.dot_general(a, b, (((1,), (1,)), ((), ())), preferred_element_type=f32)


def exact_nn(a, onehot):
    high = a.astype(bf16)
    low = (a - high.astype(f32)).astype(bf16)
    return nn(high, onehot) + nn(low, onehot)


def lanes_of(x, lane):
    at = lax.broadcasted_iota(jnp.int32, x.shape, 1)
    return jnp.sum(jnp.where(at == lane, x, 0.0), axis=1, keepdims=True)


def column_of(row):
    n = row.shape[1]
    eye = lax.broadcasted_iota(jnp.int32, (n, n), 0) == lax.broadcasted_iota(
        jnp.int32, (n, n), 1
    )
    return jnp.sum(jnp.where(eye, row, 0.0), axis=1, keepdims=True)


UP_WINDOW = (-1, 0, 1, 2)
DOWN_WINDOW = (-2, -1, 0, 1)


class Exchange:
    def __init__(self, n_kv, g, z, t):
        self.n_kv, self.g, self.z, self.t = n_kv, g, z, t
        self.half = n_kv // 8
        up = [2 + 4 * i for i in range(self.half)]
        self.reach = up + [-u for u in up]
        self.count = 2 * self.half
        self.steps = [(0, 1), (1, -1)]
        self.farthest_first = [
            k * self.half + i for i in reversed(range(self.half)) for k in (0, 1)
        ]
        self.nearest_first = list(reversed(self.farthest_first))

    def device(self, offset):
        return (self.g, lax.rem(self.z + offset + self.n_kv, self.n_kv), self.t)

    def near(self, i):
        last = () if i == self.count - 1 else ((3, 2 if i < self.half else -2),)
        return self.steps + list(last)

    def copy(self, src, dst, send, recv, offset):
        return pltpu.make_async_remote_copy(
            src_ref=src,
            dst_ref=dst,
            send_sem=send,
            recv_sem=recv,
            device_id=self.device(offset),
            device_id_type=MESH,
        )


def placing(per_slot, n_kv, seq, z):
    count = n_kv // 4
    half = count // 2
    shape = (n_kv * per_slot, n_kv * seq)
    m = lax.broadcasted_iota(jnp.int32, shape, 0)
    slot = m // per_slot
    i = slot % count
    group = slot // count
    reach = jnp.where(i < half, 2 + 4 * i, 4 * half - 2 - 4 * i)
    side = jnp.where(i < half, 2, -2)
    step = jnp.where(group == 0, 1, jnp.where(group == 1, -1, jnp.where(group == 2, 0, side)))
    offset = jnp.where(slot == n_kv - 1, 0, reach + step)
    owner = (z - offset + n_kv) % n_kv
    row = owner * seq + m % seq
    return (row == lax.broadcasted_iota(jnp.int32, shape, 1)).astype(bf16)


def kernel(
    dims,
    tok_ref,
    state_hbm,
    gain_ref,
    wq_hbm,
    wk_hbm,
    wv_hbm,
    wb_hbm,
    wd_hbm,
    alog_ref,
    dt_ref,
    hgain_ref,
    wo_hbm,
    mgain_ref,
    wu_hbm,
    wdn_hbm,
    out_ref,
    state_out,
    tok_all,
    tok_near,
    state_v,
    rhs1,
    wext,
    wo_v,
    wu_v,
    wdn_v,
    rs1,
    rs1_near,
    rs1_far_src,
    rs1_far,
    ag2_src,
    ag2,
    diag,
    att,
    mid_src,
    mid,
    rs3,
    rs3_far,
    sq_src,
    sq_far,
    ag4_src,
    ag4,
    fin_src,
    fin,
    loc,
    tok_s,
    tok_r,
    rs1_ns,
    rs1_nr,
    rs1_fs,
    rs1_fr,
    win_s,
    win_r,
    ag2_s,
    ag2_r,
    att_s,
    att_r,
    rs3_s,
    rs3_r,
    sq_s,
    sq_r,
    mid_s,
    mid_r,
    ag4_s,
    ag4_r,
    fin_s,
    fin_r,
    sem_a,
    sem_b,
    sem_c,
):
    n_kv, n_tp, seq, heads, width = dims
    g, z, t = lax.axis_index("grp"), lax.axis_index("kv"), lax.axis_index("tp")
    ex = Exchange(n_kv, g, z, t)
    count, half = ex.count, ex.half
    mine = tok_ref.shape[0]
    block = n_tp * mine
    all_rows = tok_ref.shape[1]
    head = hgain_ref.shape[1]
    own = n_kv - 1

    def tp_peer(k):
        return (g, z, lax.rem(t + k, n_tp))

    barrier = pltpu.get_barrier_semaphore()
    for k in range(1, n_tp):
        pl.semaphore_signal(barrier, inc=1, device_id=tp_peer(k), device_id_type=MESH)
    for offset in (1, -1, 2, -2):
        pl.semaphore_signal(barrier, inc=1, device_id=ex.device(offset), device_id_type=MESH)

    local = []

    def fetch(src, dst):
        copy = pltpu.make_async_copy(src, dst, loc.at[len(local)])
        copy.start()
        local.append(copy)

    for i, w in enumerate((wq_hbm, wk_hbm)):
        for h in range(heads):
            at = (i * heads + h) * block
            fetch(w.at[:, h * head : (h + 1) * head], rhs1.at[at : at + block, 0:head])
    for h in range(heads):
        fetch(
            wv_hbm.at[:, h * head : (h + 1) * head],
            rhs1.at[h * block : (h + 1) * block, head : 2 * head],
        )
    lanes = wext.shape[2]
    at = pl.multiple_of((z * block // lanes) * lanes, lanes)
    fetch(wb_hbm.at[:, pl.ds(at, lanes)], wext.at[0])
    fetch(wd_hbm.at[:, pl.ds(at, lanes)], wext.at[1])
    first_fetch = len(local)
    fetch(state_hbm, state_v)
    second_fetch = len(local)
    parts = wu_v.shape[1] // (2 * head)
    wide = 2 * head
    kinds = heads * seq
    n_win = len(UP_WINDOW)
    out_wide = heads * head
    here_up, here_down = UP_WINDOW.index(0), DOWN_WINDOW.index(0)
    fetch(wo_hbm, wo_v.at[:, here_up * out_wide : (here_up + 1) * out_wide])
    fetch(wu_hbm, wu_v.at[here_up * block : (here_up + 1) * block])
    fetch(wdn_hbm, wdn_v.at[here_down * block : (here_down + 1) * block])
    all_fetch = len(local)

    tok_all[t] = tok_ref[...]
    gain_row = mgain_ref[...].astype(f32).reshape(1, block)
    gain_row = jnp.concatenate([gain_row, jnp.zeros((1, all_rows - block), f32)], axis=1)
    tok_all[n_tp] = jnp.broadcast_to(gain_row, (mine, all_rows)).astype(bf16)
    rhs1[heads * block :, head:] = jnp.zeros((heads * block, head), bf16)
    diag[...] = jnp.zeros(diag.shape, bf16)
    spread16 = placing(parts * seq, n_kv, seq, z)
    part_of_row = (
        lax.broadcasted_iota(jnp.int32, (n_kv * parts * seq, parts * block), 0) // seq
    ) % parts
    part_mask = part_of_row == (
        lax.broadcasted_iota(jnp.int32, (n_kv * parts * seq, parts * block), 1) // block
    )
    gain = column_of(gain_ref[...].astype(f32).reshape(1, block))

    pl.semaphore_wait(barrier, n_tp - 1 + 4)
    for offset in (2, -2):
        pl.semaphore_signal(sem_a, inc=1, device_id=ex.device(offset), device_id_type=MESH)

    def to_tp(src_of, dst, send, recv):
        copies = []
        for k in range(1, n_tp):
            peer = lax.rem(t + k, n_tp)
            copy = pltpu.make_async_remote_copy(
                src_ref=src_of(peer),
                dst_ref=dst.at[t],
                send_sem=send.at[k - 1],
                recv_sem=recv.at[k - 1],
                device_id=(g, z, peer),
                device_id_type=MESH,
            )
            copy.start()
            copies.append(copy)
        return copies

    pending = []
    copies = to_tp(lambda peer: tok_all.at[t], tok_all, tok_s, tok_r)
    pending += copies
    for k in range(first_fetch):
        local[k].wait()
    odd = lax.rem(z, lanes // block) if lanes // block > 1 else 0
    pieces = []
    for i in range(2):
        piece = wext[i][:, 0:block]
        for k in range(1, lanes // block):
            piece = jnp.where(odd == k, wext[i][:, k * block : (k + 1) * block], piece)
        pieces.append(piece)
    n_heads = pieces[0].shape[0]
    wext_t = jnp.concatenate(
        pieces + [jnp.zeros((head - 2 * n_heads, block), bf16)], axis=0
    )
    at_row = lax.broadcasted_iota(jnp.int32, (head, block), 0)
    square_t = (at_row == 2 * n_heads).astype(bf16)
    ext_t = jnp.concatenate([wext_t, square_t], axis=1)

    pl.semaphore_wait(sem_a, 2)
    for offset in (4, -4):
        pl.semaphore_signal(sem_b, inc=1, device_id=ex.device(offset), device_id_type=MESH)
    for copy in copies:
        copy.wait_recv()

    def spread(x_t):
        stacked = jnp.concatenate([x_t] * parts, axis=0)
        rows = nt(spread16, stacked)
        return jnp.where(part_mask, rows, 0.0).astype(bf16)

    tok_t = tok_all[0:n_tp].astype(f32).reshape(block, all_rows)
    scaled_t = (tok_t * gain).astype(bf16)
    left = spread(scaled_t)
    both = jnp.concatenate([scaled_t, (tok_t * tok_t).astype(bf16)], axis=0)
    left2 = nt(spread16, both)
    left2 = jnp.where(part_of_row[:, 0 : 2 * block] >= heads, left2, 0.0).astype(bf16)
    product = nn(left, rhs1[...])
    extra = nt(left2, ext_t)
    product = jnp.concatenate([product[:, :head], product[:, head:] + extra], axis=1)
    rs1[...] = product.astype(bf16).reshape(rs1.shape)

    def reduce_near(buf, near_buf, send, recv, order):
        started = {}
        for i in order:
            for group, step in ex.near(i):
                k = group * count + i if group < 2 else 2 * count + i
                copy = ex.copy(
                    buf.at[group * count + i],
                    near_buf.at[k],
                    send.at[k],
                    recv.at[k],
                    -step,
                )
                copy.start()
                started[k] = copy
        return started

    def near_sum(i, buf, near_buf, started):
        total = buf[2 * count + i].astype(f32)
        for group, step in ex.near(i):
            k = group * count + i if group < 2 else 2 * count + i
            started[k].wait_recv()
            total += near_buf[k].astype(f32)
        return total

    def reduce_far(i, total, far_src, far_buf, send, recv):
        far_src[i] = total.astype(far_src.dtype)
        copy = ex.copy(far_src.at[i], far_buf.at[i], send.at[i], recv.at[i], -ex.reach[i])
        copy.start()
        return copy

    def far_sum(buf, far_buf, copies):
        total = buf[own].astype(f32)
        for i, copy in copies:
            copy.wait_recv()
            total += far_buf[i].astype(f32)
        return total

    close = [i for i in ex.nearest_first if abs(ex.reach[i]) <= 8]
    distant = [i for i in ex.farthest_first if abs(ex.reach[i]) > 8]
    started = reduce_near(rs1, rs1_near, rs1_ns, rs1_nr, distant + close)
    pending += list(started.values())
    pl.semaphore_wait(sem_b, 2)
    for offset in (8, -8):
        pl.semaphore_signal(sem_c, inc=1, device_id=ex.device(offset), device_id_type=MESH)
    copies = []
    for i in close:
        total = near_sum(i, rs1, rs1_near, started)
        copies.append((i, reduce_far(i, total, rs1_far_src, rs1_far, rs1_fs, rs1_fr)))
    totals = [near_sum(i, rs1, rs1_near, started) for i in distant]
    pl.semaphore_wait(sem_c, 2)
    for i, total in zip(distant, totals):
        copies.append((i, reduce_far(i, total, rs1_far_src, rs1_far, rs1_fs, rs1_fr)))
    pending += [c for _, c in copies]

    window = []

    def to_window(src, dst_of, offsets):
        begun = []
        for w, offset in enumerate(offsets):
            if offset:
                k = len(window)
                copy = ex.copy(src, dst_of(w), win_s.at[k], win_r.at[k], -offset)
                copy.start()
                window.append(copy)
                begun.append(copy)
        return begun

    tok_window = to_window(tok_all, lambda w: tok_near.at[w], UP_WINDOW)
    wo_window = to_window(
        wo_hbm, lambda w: wo_v.at[:, w * out_wide : (w + 1) * out_wide], UP_WINDOW
    )

    local[first_fetch].wait()
    sums = far_sum(rs1, rs1_far, copies)

    rows = heads * seq
    query_sum, key_sum = sums[:rows, :head], sums[rows:, :head]
    value_sum, extra = sums[:rows, head:], sums[rows:, head:]
    which = lax.broadcasted_iota(jnp.int32, (rows, head), 0) // seq
    lane = lax.broadcasted_iota(jnp.int32, (rows, head), 1)
    beta_sum = jnp.sum(
        jnp.where(lane == t * heads + which, extra, 0.0), axis=1, keepdims=True
    )
    decay_sum = jnp.sum(
        jnp.where(lane == n_heads + t * heads + which, extra, 0.0), axis=1, keepdims=True
    )
    square_sum = lanes_of(extra, 2 * n_heads)
    first = lax.rsqrt(square_sum / width + epsilon)
    query_pre, key_pre, value_pre = first * query_sum, first * key_sum, first * value_sum
    query = query_pre * lax.rsqrt(jnp.sum(query_pre * query_pre, axis=1, keepdims=True) + epsilon)
    key = key_pre * lax.rsqrt(jnp.sum(key_pre * key_pre, axis=1, keepdims=True) + epsilon)
    beta = jax.nn.sigmoid(first * beta_sum)
    which1 = lax.broadcasted_iota(jnp.int32, (rows, 1), 0) // seq
    a_log = jnp.zeros((rows, 1), f32)
    dt_bias = jnp.zeros((rows, 1), f32)
    for h in range(heads):
        a_log = jnp.where(which1 == h, alog_ref[h], a_log)
        dt_bias = jnp.where(which1 == h, dt_ref[h], dt_bias)
    logit = first * decay_sum + dt_bias
    softplus = jnp.maximum(logit, 0.0) + jnp.log1p(jnp.exp(-jnp.abs(logit)))
    decay = jnp.exp(-jnp.exp(a_log) * softplus)
    query_t, key_t = query.T, key.T
    key_reads, query_reads = [], []
    for k in range(rows):
        matrix = state_v[k % seq, k // seq]
        key_reads.append(jnp.sum(matrix * key_t[:, k : k + 1], axis=0, keepdims=True))
        query_reads.append(jnp.sum(matrix * query_t[:, k : k + 1], axis=0, keepdims=True))
    key_read = jnp.concatenate(key_reads, axis=0)
    query_read = jnp.concatenate(query_reads, axis=0)
    fresh = beta * (value_pre - decay * key_read)
    meeting = jnp.sum(query * key, axis=1, keepdims=True)
    reading = decay * query_read + meeting * fresh
    normed = (
        reading
        * lax.rsqrt(jnp.mean(reading * reading, axis=1, keepdims=True) + epsilon)
        * hgain_ref[...]
    )

    def to_far(src_of, dst, send, recv, sign):
        copies = []
        for i in ex.farthest_first:
            copy = ex.copy(src_of(i), dst.at[i], send.at[i], recv.at[i], sign * ex.reach[i])
            copy.start()
            copies.append(copy)
        return copies

    ag2_src[...] = normed.astype(bf16)
    ag2_copies = to_far(lambda i: ag2_src, ag2, ag2_s, ag2_r, 1)
    pending += ag2_copies
    wu_window = to_window(wu_hbm, lambda w: wu_v.at[w * block : (w + 1) * block], UP_WINDOW)
    wdn_window = to_window(
        wdn_hbm, lambda w: wdn_v.at[w * block : (w + 1) * block], DOWN_WINDOW
    )
    pending += window
    for k in range(rows):
        matrix = state_v[k % seq, k // seq]
        state_out[k % seq, k // seq] = (
            decay[k : k + 1] * matrix + key_t[:, k : k + 1] * fresh[k : k + 1]
        )

    def iota(shape, dim):
        return lax.broadcasted_iota(jnp.int32, shape, dim)

    def owner_row(slot, r):
        half = ex.half
        reach = jnp.where(slot < half, 2 + 4 * slot, 4 * half - 2 - 4 * slot)
        return (z - reach + n_kv) % n_kv * seq + r

    per_w = count * seq
    shape = (n_win * all_rows, all_rows)
    lane = iota(shape, 1)
    lane_owner = owner_row(lane % per_w // seq, lane % seq)
    window_pick = (
        (lane // per_w == iota(shape, 0) // all_rows) & (lane_owner == iota(shape, 0) % all_rows)
    ).astype(bf16)
    shape = (per_w, all_rows)
    place_rows = (owner_row(iota(shape, 0) // seq, iota(shape, 0) % seq) == iota(shape, 1)).astype(
        bf16
    )
    head_picks = []
    shape = (per_w, count * kinds)
    for h in range(heads):
        r0, c1 = iota(shape, 0), iota(shape, 1)
        head_picks.append(
            (
                (c1 // kinds == r0 // seq) & (c1 % seq == r0 % seq) & (c1 // seq % heads == h)
            ).astype(bf16)
        )
    shape = (count * parts * seq, all_rows)
    r0, c1 = iota(shape, 0), iota(shape, 1)
    spread_rows = (
        (r0 // (parts * seq) == c1 % per_w // seq) & (r0 % seq == c1 % seq)
    ).astype(bf16)
    shape = (per_w, count * parts * seq)
    r0, c1 = iota(shape, 0), iota(shape, 1)
    part_picks = [
        (
            (c1 // (parts * seq) == r0 // seq) & (c1 % seq == r0 % seq) & (c1 // seq % parts == j)
        ).astype(bf16)
        for j in range(parts)
    ]
    for copy in tok_window:
        copy.wait_recv()
    token_parts = []
    mixer_gain = jnp.zeros((block, all_rows), f32)
    lane = iota((block, all_rows), 1)
    for w, offset in enumerate(UP_WINDOW):
        source = tok_near.at[w] if offset else tok_all
        token_parts.append(source[0:n_tp].astype(f32).reshape(block, all_rows).astype(bf16))
        column = column_of(source[n_tp].astype(f32)[0:1, 0:block])
        mixer_gain = jnp.where(lane // per_w == w, column, mixer_gain)
    token_w = nn(jnp.concatenate(token_parts, axis=1), window_pick)
    for k in range(second_fetch, all_fetch):
        local[k].wait()
    for copy in ag2_copies:
        copy.wait_recv()
    for copy in wo_window:
        copy.wait_recv()
    everyone = ag2[...].astype(f32).reshape(count * kinds, head).astype(bf16)
    for h in range(heads):
        picked = nn(head_picks[h], everyone).astype(bf16)
        for w in range(n_win):
            at = w * out_wide + h * head
            diag[w * per_w : (w + 1) * per_w, at : at + head] = picked
    att[t] = nt(wo_v[...], diag[...]).astype(bf16)
    copies = to_tp(lambda peer: att.at[t], att, att_s, att_r)
    pending += copies
    for copy in copies:
        copy.wait_recv()
    for copy in wu_window:
        copy.wait_recv()

    attended = att[0].astype(f32)
    for k in range(1, n_tp):
        attended += att[k].astype(f32)
    middle_b = (token_w + attended).astype(bf16)
    middle = middle_b.astype(f32)
    scaled = jnp.concatenate([middle * mixer_gain] * n_win, axis=0)
    shape = scaled.shape
    scaled = jnp.where(iota(shape, 1) // per_w == iota(shape, 0) // block, scaled, 0.0)
    left = nt(spread_rows, scaled.astype(bf16))
    part = iota(left.shape, 0) // seq % parts
    product = jnp.zeros((left.shape[0], wide), f32)
    for j in range(parts):
        product += nn(
            jnp.where(part == j, left, 0.0).astype(bf16), wu_v[:, j * wide : (j + 1) * wide]
        )
    rs3[...] = product.astype(bf16).reshape(rs3.shape)
    sq_src[...] = jnp.sum(middle * middle, axis=0, keepdims=True)
    rs3_copies = to_far(lambda i: rs3.at[i], rs3_far, rs3_s, rs3_r, -1)
    sq_copies = to_far(lambda i: sq_src, sq_far, sq_s, sq_r, -1)
    pending += rs3_copies + sq_copies
    mid_copies = []
    for w, offset in enumerate(UP_WINDOW):
        placed = nt(middle_b, window_pick[w * all_rows : (w + 1) * all_rows]).astype(bf16)
        mid_src[w] = placed.reshape(n_tp, mine, all_rows)
        if offset:
            copy = ex.copy(mid_src.at[w, t], mid.at[w], mid_s.at[w], mid_r.at[w], offset)
            copy.start()
            mid_copies.append(copy)
        else:
            mid[w] = mid_src[w, t]
    pending += mid_copies
    for copy in sq_copies:
        copy.wait_recv()
    lane = iota((1, all_rows), 1)
    squares = jnp.zeros((1, all_rows), f32)
    for i in range(count):
        squares += jnp.where(lane % per_w // seq == i, sq_far[i], 0.0)
    shape = (parts * seq, all_rows)
    squares = jnp.sum(
        jnp.where(iota(shape, 1) % seq == iota(shape, 0) % seq, squares, 0.0),
        axis=1,
        keepdims=True,
    )
    second = lax.rsqrt(squares / width + epsilon)
    up = jnp.zeros((parts * seq, wide), f32)
    for copy in reversed(rs3_copies):
        copy.wait_recv()
    for i in range(count):
        up += rs3_far[i].astype(f32)
    ag4_src[...] = jnp.square(jnp.maximum(second * up, 0.0)).astype(bf16)

    ag4_copies = to_far(lambda i: ag4_src, ag4, ag4_s, ag4_r, 1)
    pending += ag4_copies
    for copy in wdn_window:
        copy.wait_recv()
    for copy in mid_copies:
        copy.wait_recv()
    middle = mid[0].astype(f32)
    for w in range(1, n_win):
        middle += mid[w].astype(f32)
    for copy in ag4_copies:
        copy.wait_recv()
    everyone = ag4[...].reshape(count * parts * seq, wide)
    picked = jnp.concatenate(
        [nn(part_picks[j], everyone).astype(bf16) for j in range(parts)], axis=1
    )
    lowered_part = nt(wdn_v[...], picked).astype(bf16)
    fin_src[...] = nn(lowered_part, place_rows).astype(bf16).reshape(fin_src.shape)
    copies = []
    for w, offset in enumerate(DOWN_WINDOW):
        row = lax.rem(z + offset + n_kv, n_kv)
        for k in range(n_tp):
            if offset == 0 and k == 0:
                fin[w, t] = fin_src[w, t]
                continue
            peer = lax.rem(t + k, n_tp)
            copy = pltpu.make_async_remote_copy(
                src_ref=fin_src.at[w, peer],
                dst_ref=fin.at[w, t],
                send_sem=fin_s.at[w * n_tp + k],
                recv_sem=fin_r.at[w * n_tp + k],
                device_id=(g, row, peer),
                device_id_type=MESH,
            )
            copy.start()
            copies.append(copy)
    pending += copies
    for copy in copies:
        copy.wait_recv()
    lowered = jnp.zeros((mine, all_rows), f32)
    for w in range(n_win):
        for k in range(n_tp):
            lowered += fin[w, k].astype(f32)
    out_ref[...] = (middle + lowered).astype(bf16)
    for copy in pending:
        copy.wait_send()


def solution(mesh):
    n_kv, n_tp = mesh.shape["kv"], mesh.shape["tp"]

    def local(
        tokens,
        state,
        norm_gain,
        w_query,
        w_key,
        w_value,
        w_beta,
        w_decay,
        a_log,
        dt_bias,
        head_gain,
        w_out,
        mixer_gain,
        w_up,
        w_down,
    ):
        seq, heads, head = state.shape[:3]
        rows, mine = tokens.shape
        block = w_query.shape[0]
        parts = w_up.shape[1] // (2 * head)
        wide = w_up.shape[1] // parts
        count = n_kv // 4
        dims = (n_kv, n_tp, seq, heads, block * n_kv)
        vmem, hbm, smem = (
            pl.BlockSpec(memory_space=pltpu.VMEM),
            pl.BlockSpec(memory_space=pltpu.HBM),
            pl.BlockSpec(memory_space=pltpu.SMEM),
        )
        dma = pltpu.SemaphoreType.DMA
        blocks = (parts * seq, wide)
        near = (3 * count - 1,)
        far = (count,)
        n_local = 3 * heads + 2 + 1 + 3 + 1
        n_win = len(UP_WINDOW)
        scratch = [
            pltpu.VMEM((n_tp + 1, mine, rows), bf16),
            pltpu.VMEM((n_win, n_tp + 1, mine, rows), bf16),
            pltpu.VMEM(state.shape, f32),
            pltpu.VMEM((2 * heads * block, 2 * head), bf16),
            pltpu.VMEM((2, w_beta.shape[1], head), bf16),
            pltpu.VMEM((block, n_win * heads * head), bf16),
            pltpu.VMEM((n_win * block, w_up.shape[1]), bf16),
            pltpu.VMEM((n_win * block, w_down.shape[0]), bf16),
            pltpu.VMEM((n_kv, *blocks), bf16),
            pltpu.VMEM((*near, *blocks), bf16),
            pltpu.VMEM((count, *blocks), bf16),
            pltpu.VMEM((count, *blocks), bf16),
            pltpu.VMEM((heads * seq, head), bf16),
            pltpu.VMEM((count, heads * seq, head), bf16),
            pltpu.VMEM((rows, n_win * heads * head), bf16),
            pltpu.VMEM((n_tp, block, rows), bf16),
            pltpu.VMEM((n_win, n_tp, mine, rows), bf16),
            pltpu.VMEM((n_win, mine, rows), bf16),
            pltpu.VMEM((count, *blocks), bf16),
            pltpu.VMEM((count, *blocks), bf16),
            pltpu.VMEM((1, rows), f32),
            pltpu.VMEM((count, 1, rows), f32),
            pltpu.VMEM(blocks, bf16),
            pltpu.VMEM((count, *blocks), bf16),
            pltpu.VMEM((n_win, n_tp, mine, rows), bf16),
            pltpu.VMEM((n_win, n_tp, mine, rows), bf16),
            dma((n_local,)),
            dma((n_tp - 1,)),
            dma((n_tp - 1,)),
            dma(near),
            dma(near),
            dma(far),
            dma(far),
            dma((4 * (n_win - 1),)),
            dma((4 * (n_win - 1),)),
            dma(far),
            dma(far),
            dma((n_tp - 1,)),
            dma((n_tp - 1,)),
            dma(far),
            dma(far),
            dma(far),
            dma(far),
            dma((n_win,)),
            dma((n_win,)),
            dma(far),
            dma(far),
            dma((n_win * n_tp,)),
            dma((n_win * n_tp,)),
            pltpu.SemaphoreType.REGULAR,
            pltpu.SemaphoreType.REGULAR,
            pltpu.SemaphoreType.REGULAR,
        ]
        mixed_t, new_state = pl.pallas_call(
            functools.partial(kernel, dims),
            out_shape=(
                jax.ShapeDtypeStruct((mine, rows), bf16),
                jax.ShapeDtypeStruct(state.shape, f32),
            ),
            in_specs=[
                vmem,
                hbm,
                vmem,
                hbm,
                hbm,
                hbm,
                hbm,
                hbm,
                smem,
                smem,
                vmem,
                hbm,
                vmem,
                hbm,
                hbm,
            ],
            out_specs=(vmem, vmem),
            scratch_shapes=scratch,
            compiler_params=pltpu.CompilerParams(collective_id=0, has_side_effects=True, vmem_limit_bytes=32 * 2**20),
        )(
            tokens.T,
            pltpu.with_memory_space_constraint(state, pltpu.HBM),
            norm_gain,
            pltpu.with_memory_space_constraint(w_query, pltpu.HBM),
            pltpu.with_memory_space_constraint(w_key, pltpu.HBM),
            pltpu.with_memory_space_constraint(w_value, pltpu.HBM),
            pltpu.with_memory_space_constraint(w_beta.T, pltpu.HBM),
            pltpu.with_memory_space_constraint(w_decay.T, pltpu.HBM),
            a_log,
            dt_bias,
            head_gain.reshape(1, head),
            pltpu.with_memory_space_constraint(w_out.T, pltpu.HBM),
            mixer_gain,
            pltpu.with_memory_space_constraint(w_up, pltpu.HBM),
            pltpu.with_memory_space_constraint(w_down.T, pltpu.HBM),
        )
        return mixed_t.T, new_state

    return jax.shard_map(
        local,
        mesh=mesh,
        in_specs=(
            P("grp", ("kv", "tp")),
            P(("grp", "kv"), "tp", None, None),
            P("kv"),
            P("kv", "tp"),
            P("kv", "tp"),
            P("kv", "tp"),
            P(),
            P(),
            P("tp"),
            P("tp"),
            P(),
            P("tp", "kv"),
            P("kv"),
            P("kv", "tp"),
            P("tp", "kv"),
        ),
        out_specs=(P("grp", ("kv", "tp")), P(("grp", "kv"), "tp", None, None)),
        check_vma=False,
    )
```

```python
import functools

import jax
import jax.numpy as jnp
from jax import lax
from jax.experimental import pallas as pl
from jax.experimental.pallas import tpu as pltpu
from jax.sharding import PartitionSpec as P

MESH = pl.DeviceIdType.MESH
epsilon = 1e-06
f32 = jnp.float32
bf16 = jnp.bfloat16


def nn(a, b):
    return jnp.dot(a, b, preferred_element_type=f32)


def nt(a, b):
    return lax.dot_general(a, b, (((1,), (1,)), ((), ())), preferred_element_type=f32)


def exact_nn(a, onehot):
    high = a.astype(bf16)
    low = (a - high.astype(f32)).astype(bf16)
    return nn(high, onehot) + nn(low, onehot)


def lanes_of(x, lane):
    at = lax.broadcasted_iota(jnp.int32, x.shape, 1)
    return jnp.sum(jnp.where(at == lane, x, 0.0), axis=1, keepdims=True)


def column_of(row):
    n = row.shape[1]
    eye = lax.broadcasted_iota(jnp.int32, (n, n), 0) == lax.broadcasted_iota(
        jnp.int32, (n, n), 1
    )
    return jnp.sum(jnp.where(eye, row, 0.0), axis=1, keepdims=True)


UP_WINDOW = (-1, 0, 1, 2)
DOWN_WINDOW = (-2, -1, 0, 1)


class Exchange:
    def __init__(self, n_kv, g, z, t):
        self.n_kv, self.g, self.z, self.t = n_kv, g, z, t
        self.half = n_kv // 8
        up = [2 + 4 * i for i in range(self.half)]
        self.reach = up + [-u for u in up]
        self.count = 2 * self.half
        self.steps = [(0, 1), (1, -1)]
        self.farthest_first = [
            k * self.half + i for i in reversed(range(self.half)) for k in (0, 1)
        ]
        self.nearest_first = list(reversed(self.farthest_first))

    def device(self, offset):
        return (self.g, lax.rem(self.z + offset + self.n_kv, self.n_kv), self.t)

    def near(self, i):
        last = () if i == self.count - 1 else ((3, 2 if i < self.half else -2),)
        return self.steps + list(last)

    def copy(self, src, dst, send, recv, offset):
        return pltpu.make_async_remote_copy(
            src_ref=src,
            dst_ref=dst,
            send_sem=send,
            recv_sem=recv,
            device_id=self.device(offset),
            device_id_type=MESH,
        )


def placing(per_slot, n_kv, seq, z):
    count = n_kv // 4
    half = count // 2
    shape = (n_kv * per_slot, n_kv * seq)
    m = lax.broadcasted_iota(jnp.int32, shape, 0)
    slot = m // per_slot
    i = slot % count
    group = slot // count
    reach = jnp.where(i < half, 2 + 4 * i, 4 * half - 2 - 4 * i)
    side = jnp.where(i < half, 2, -2)
    step = jnp.where(group == 0, 1, jnp.where(group == 1, -1, jnp.where(group == 2, 0, side)))
    offset = jnp.where(slot == n_kv - 1, 0, reach + step)
    owner = (z - offset + n_kv) % n_kv
    row = owner * seq + m % seq
    return (row == lax.broadcasted_iota(jnp.int32, shape, 1)).astype(bf16)


def kernel(
    dims,
    tok_ref,
    state_hbm,
    gain_ref,
    wq_hbm,
    wk_hbm,
    wv_hbm,
    wb_hbm,
    wd_hbm,
    alog_ref,
    dt_ref,
    hgain_ref,
    wo_hbm,
    mgain_ref,
    wu_hbm,
    wdn_hbm,
    out_ref,
    state_out,
    tok_all,
    tok_near,
    state_v,
    rhs1,
    wext,
    wo_v,
    wu_v,
    wdn_v,
    rs1,
    rs1_near,
    rs1_far_src,
    rs1_far,
    ag2_src,
    ag2,
    diag,
    att,
    mid_src,
    mid,
    rs3,
    rs3_far,
    sq_src,
    sq_far,
    ag4_src,
    ag4,
    fin_src,
    fin,
    gain_v,
    mgain_v,
    hgain_v,
    alog_v,
    dt_v,
    loc,
    tok_s,
    tok_r,
    rs1_ns,
    rs1_nr,
    rs1_fs,
    rs1_fr,
    win_s,
    win_r,
    ag2_s,
    ag2_r,
    att_s,
    att_r,
    rs3_s,
    rs3_r,
    sq_s,
    sq_r,
    mid_s,
    mid_r,
    ag4_s,
    ag4_r,
    fin_s,
    fin_r,
    sem_a,
    sem_b,
    sem_c,
):
    n_kv, n_tp, seq, heads, width = dims
    g, z, t = lax.axis_index("grp"), lax.axis_index("kv"), lax.axis_index("tp")
    ex = Exchange(n_kv, g, z, t)
    count, half = ex.count, ex.half
    mine = tok_ref.shape[0]
    block = n_tp * mine
    all_rows = tok_ref.shape[1]
    head = hgain_v.shape[1]
    own = n_kv - 1

    def tp_peer(k):
        return (g, z, lax.rem(t + k, n_tp))

    barrier = pltpu.get_barrier_semaphore()
    for k in range(1, n_tp):
        pl.semaphore_signal(barrier, inc=1, device_id=tp_peer(k), device_id_type=MESH)
    for offset in (1, -1, 2, -2):
        pl.semaphore_signal(barrier, inc=1, device_id=ex.device(offset), device_id_type=MESH)

    def waiter(ref, send, recv):
        return pltpu.make_async_remote_copy(
            src_ref=ref,
            dst_ref=ref,
            send_sem=send,
            recv_sem=recv,
            device_id=tp_peer(1),
            device_id_type=MESH,
        )

    def fetch(src, dst, k):
        copy = pltpu.make_async_copy(src, dst, loc.at[k])
        copy.start()
        return copy

    got_tok = fetch(tok_ref, tok_all.at[t], 0)
    got_mgain = fetch(mgain_ref, mgain_v, 1)
    got_gain = fetch(gain_ref, gain_v, 2)
    lanes = wext.shape[2]
    at = pl.multiple_of((z * block // lanes) * lanes, lanes)
    got_ext = [
        fetch(wb_hbm.at[:, pl.ds(at, lanes)], wext.at[0], 3),
        fetch(wd_hbm.at[:, pl.ds(at, lanes)], wext.at[1], 4),
    ]
    for i, w in enumerate((wq_hbm, wk_hbm)):
        for h in range(heads):
            at = (i * heads + h) * block
            fetch(w.at[:, h * head : (h + 1) * head], rhs1.at[at : at + block, 0:head], 5)
    for h in range(heads):
        fetch(
            wv_hbm.at[:, h * head : (h + 1) * head],
            rhs1.at[h * block : (h + 1) * block, head : 2 * head],
            5,
        )
    whole = rhs1.at[0 : 3 * heads * block // 2]
    got_rhs1 = pltpu.make_async_copy(whole, whole, loc.at[5])
    got_small = [
        fetch(hgain_ref, hgain_v, 6),
        fetch(alog_ref, alog_v, 7),
        fetch(dt_ref, dt_v, 8),
    ]
    got_state = fetch(state_hbm, state_v, 9)
    parts = wu_v.shape[1] // (2 * head)
    wide = 2 * head
    kinds = heads * seq
    n_win = len(UP_WINDOW)
    out_wide = heads * head
    here_up, here_down = UP_WINDOW.index(0), DOWN_WINDOW.index(0)
    got_weights = [
        fetch(wo_hbm, wo_v.at[:, here_up * out_wide : (here_up + 1) * out_wide], 10),
        fetch(wu_hbm, wu_v.at[here_up * block : (here_up + 1) * block], 11),
        fetch(wdn_hbm, wdn_v.at[here_down * block : (here_down + 1) * block], 12),
    ]

    rhs1[heads * block :, head:] = jnp.zeros((heads * block, head), bf16)
    diag[...] = jnp.zeros(diag.shape, bf16)
    spread16 = placing(parts * seq, n_kv, seq, z)
    part_of_row = (
        lax.broadcasted_iota(jnp.int32, (n_kv * parts * seq, parts * block), 0) // seq
    ) % parts
    part_mask = part_of_row == (
        lax.broadcasted_iota(jnp.int32, (n_kv * parts * seq, parts * block), 1) // block
    )
    got_mgain.wait()
    gain_row = mgain_v[...].astype(f32).reshape(1, block)
    gain_row = jnp.concatenate([gain_row, jnp.zeros((1, all_rows - block), f32)], axis=1)
    tok_all[n_tp] = jnp.broadcast_to(gain_row, (mine, all_rows)).astype(bf16)
    got_gain.wait()
    gain = column_of(gain_v[...].astype(f32).reshape(1, block))
    got_tok.wait()

    pl.semaphore_wait(barrier, n_tp - 1 + 4)
    for offset in (2, -2):
        pl.semaphore_signal(sem_a, inc=1, device_id=ex.device(offset), device_id_type=MESH)

    def to_tp(dst, send, recv):
        for k in range(1, n_tp):
            peer = lax.rem(t + k, n_tp)
            pltpu.make_async_remote_copy(
                src_ref=dst.at[t],
                dst_ref=dst.at[t],
                send_sem=send,
                recv_sem=recv,
                device_id=(g, z, peer),
                device_id_type=MESH,
            ).start()
        return waiter(dst.at[0 : n_tp - 1], send, recv)

    pending = []
    tok_sent = to_tp(tok_all, tok_s, tok_r)
    pending.append(tok_sent)
    got_rhs1.wait()
    for copy in got_ext:
        copy.wait()
    odd = lax.rem(z, lanes // block) if lanes // block > 1 else 0
    pieces = []
    for i in range(2):
        piece = wext[i][:, 0:block]
        for k in range(1, lanes // block):
            piece = jnp.where(odd == k, wext[i][:, k * block : (k + 1) * block], piece)
        pieces.append(piece)
    n_heads = pieces[0].shape[0]
    wext_t = jnp.concatenate(
        pieces + [jnp.zeros((head - 2 * n_heads, block), bf16)], axis=0
    )
    at_row = lax.broadcasted_iota(jnp.int32, (head, block), 0)
    square_t = (at_row == 2 * n_heads).astype(bf16)
    ext_t = jnp.concatenate([wext_t, square_t], axis=1)

    pl.semaphore_wait(sem_a, 2)
    for offset in (4, -4):
        pl.semaphore_signal(sem_b, inc=1, device_id=ex.device(offset), device_id_type=MESH)
    tok_sent.wait_recv()

    def spread(x_t):
        stacked = jnp.concatenate([x_t] * parts, axis=0)
        rows = nt(spread16, stacked)
        return jnp.where(part_mask, rows, 0.0).astype(bf16)

    tok_t = tok_all[0:n_tp].astype(f32).reshape(block, all_rows)
    scaled_t = (tok_t * gain).astype(bf16)
    left = spread(scaled_t)
    both = jnp.concatenate([scaled_t, (tok_t * tok_t).astype(bf16)], axis=0)
    left2 = nt(spread16, both)
    left2 = jnp.where(part_of_row[:, 0 : 2 * block] >= heads, left2, 0.0).astype(bf16)
    product = nn(left, rhs1[...])
    extra = nt(left2, ext_t)
    product = jnp.concatenate([product[:, :head], product[:, head:] + extra], axis=1)
    rs1[...] = product.astype(bf16).reshape(rs1.shape)

    for i in ex.farthest_first:
        for group, step in ex.near(i):
            k = group * count + i if group < 2 else 2 * count + i
            ex.copy(
                rs1.at[group * count + i], rs1_near.at[k], rs1_ns, rs1_nr, -step
            ).start()
    near_sent = waiter(rs1.at[0 : 3 * count - 1], rs1_ns, rs1_nr)
    pending.append(near_sent)
    pl.semaphore_wait(sem_b, 2)
    for offset in (8, -8):
        pl.semaphore_signal(sem_c, inc=1, device_id=ex.device(offset), device_id_type=MESH)
    near_sent.wait_recv()
    for i in range(count):
        total = rs1[2 * count + i].astype(f32)
        for group, step in ex.near(i):
            k = group * count + i if group < 2 else 2 * count + i
            total += rs1_near[k].astype(f32)
        rs1_far_src[i] = total.astype(bf16)
    pl.semaphore_wait(sem_c, 2)

    def to_far(src_of, dst, send, recv, sign):
        for i in ex.farthest_first:
            ex.copy(src_of(i), dst.at[i], send, recv, sign * ex.reach[i]).start()
        sent = waiter(dst, send, recv)
        pending.append(sent)
        return sent

    far_sent = to_far(lambda i: rs1_far_src.at[i], rs1_far, rs1_fs, rs1_fr, -1)

    def to_window(src, dst_of, whole, k, offsets):
        for w, offset in enumerate(offsets):
            if offset:
                ex.copy(src, dst_of(w), win_s.at[k], win_r.at[k], -offset).start()
        sent = waiter(whole, win_s.at[k], win_r.at[k])
        pending.append(sent)
        return sent

    tok_window = to_window(
        tok_all, lambda w: tok_near.at[w], tok_near.at[0 : n_win - 1], 0, UP_WINDOW
    )
    wo_window = to_window(
        wo_hbm,
        lambda w: wo_v.at[:, w * out_wide : (w + 1) * out_wide],
        wo_v.at[:, 0 : (n_win - 1) * out_wide],
        1,
        UP_WINDOW,
    )

    got_state.wait()
    for copy in got_small:
        copy.wait()
    far_sent.wait_recv()
    sums = rs1[own].astype(f32)
    for i in range(count):
        sums += rs1_far[i].astype(f32)

    rows = heads * seq
    query_sum, key_sum = sums[:rows, :head], sums[rows:, :head]
    value_sum, extra = sums[:rows, head:], sums[rows:, head:]
    which = lax.broadcasted_iota(jnp.int32, (rows, head), 0) // seq
    lane = lax.broadcasted_iota(jnp.int32, (rows, head), 1)
    beta_sum = jnp.sum(
        jnp.where(lane == t * heads + which, extra, 0.0), axis=1, keepdims=True
    )
    decay_sum = jnp.sum(
        jnp.where(lane == n_heads + t * heads + which, extra, 0.0), axis=1, keepdims=True
    )
    square_sum = lanes_of(extra, 2 * n_heads)
    first = lax.rsqrt(square_sum / width + epsilon)
    query_pre, key_pre, value_pre = first * query_sum, first * key_sum, first * value_sum
    query = query_pre * lax.rsqrt(jnp.sum(query_pre * query_pre, axis=1, keepdims=True) + epsilon)
    key = key_pre * lax.rsqrt(jnp.sum(key_pre * key_pre, axis=1, keepdims=True) + epsilon)
    beta = jax.nn.sigmoid(first * beta_sum)
    which1 = lax.broadcasted_iota(jnp.int32, (rows, 1), 0) // seq
    a_logs, dt_biases = alog_v[...].reshape(1, heads), dt_v[...].reshape(1, heads)
    a_log = jnp.zeros((rows, 1), f32)
    dt_bias = jnp.zeros((rows, 1), f32)
    for h in range(heads):
        a_log = jnp.where(which1 == h, a_logs[:, h : h + 1], a_log)
        dt_bias = jnp.where(which1 == h, dt_biases[:, h : h + 1], dt_bias)
    logit = first * decay_sum + dt_bias
    softplus = jnp.maximum(logit, 0.0) + jnp.log1p(jnp.exp(-jnp.abs(logit)))
    decay = jnp.exp(-jnp.exp(a_log) * softplus)
    query_t, key_t = query.T, key.T
    key_reads, query_reads = [], []
    for k in range(rows):
        matrix = state_v[k % seq, k // seq]
        key_reads.append(jnp.sum(matrix * key_t[:, k : k + 1], axis=0, keepdims=True))
        query_reads.append(jnp.sum(matrix * query_t[:, k : k + 1], axis=0, keepdims=True))
    key_read = jnp.concatenate(key_reads, axis=0)
    query_read = jnp.concatenate(query_reads, axis=0)
    fresh = beta * (value_pre - decay * key_read)
    meeting = jnp.sum(query * key, axis=1, keepdims=True)
    reading = decay * query_read + meeting * fresh
    normed = (
        reading
        * lax.rsqrt(jnp.mean(reading * reading, axis=1, keepdims=True) + epsilon)
        * hgain_v[...]
    )

    ag2_src[...] = normed.astype(bf16)
    ag2_sent = to_far(lambda i: ag2_src, ag2, ag2_s, ag2_r, 1)
    wu_window = to_window(
        wu_hbm,
        lambda w: wu_v.at[w * block : (w + 1) * block],
        wu_v.at[0 : (n_win - 1) * block],
        2,
        UP_WINDOW,
    )
    wdn_window = to_window(
        wdn_hbm,
        lambda w: wdn_v.at[w * block : (w + 1) * block],
        wdn_v.at[0 : (n_win - 1) * block],
        3,
        DOWN_WINDOW,
    )
    for k in range(rows):
        matrix = state_v[k % seq, k // seq]
        state_out[k % seq, k // seq] = (
            decay[k : k + 1] * matrix + key_t[:, k : k + 1] * fresh[k : k + 1]
        )

    def iota(shape, dim):
        return lax.broadcasted_iota(jnp.int32, shape, dim)

    def owner_row(slot, r):
        half = ex.half
        reach = jnp.where(slot < half, 2 + 4 * slot, 4 * half - 2 - 4 * slot)
        return (z - reach + n_kv) % n_kv * seq + r

    per_w = count * seq
    shape = (n_win * all_rows, all_rows)
    lane = iota(shape, 1)
    lane_owner = owner_row(lane % per_w // seq, lane % seq)
    window_pick = (
        (lane // per_w == iota(shape, 0) // all_rows) & (lane_owner == iota(shape, 0) % all_rows)
    ).astype(bf16)
    shape = (per_w, all_rows)
    place_rows = (owner_row(iota(shape, 0) // seq, iota(shape, 0) % seq) == iota(shape, 1)).astype(
        bf16
    )
    head_picks = []
    shape = (per_w, count * kinds)
    for h in range(heads):
        r0, c1 = iota(shape, 0), iota(shape, 1)
        head_picks.append(
            (
                (c1 // kinds == r0 // seq) & (c1 % seq == r0 % seq) & (c1 // seq % heads == h)
            ).astype(bf16)
        )
    shape = (count * parts * seq, all_rows)
    r0, c1 = iota(shape, 0), iota(shape, 1)
    spread_rows = (
        (r0 // (parts * seq) == c1 % per_w // seq) & (r0 % seq == c1 % seq)
    ).astype(bf16)
    shape = (per_w, count * parts * seq)
    r0, c1 = iota(shape, 0), iota(shape, 1)
    part_picks = [
        (
            (c1 // (parts * seq) == r0 // seq) & (c1 % seq == r0 % seq) & (c1 // seq % parts == j)
        ).astype(bf16)
        for j in range(parts)
    ]
    tok_window.wait_recv()
    token_parts = []
    mixer_gain = jnp.zeros((block, all_rows), f32)
    lane = iota((block, all_rows), 1)
    for w, offset in enumerate(UP_WINDOW):
        source = tok_near.at[w] if offset else tok_all
        token_parts.append(source[0:n_tp].astype(f32).reshape(block, all_rows).astype(bf16))
        column = column_of(source[n_tp].astype(f32)[0:1, 0:block])
        mixer_gain = jnp.where(lane // per_w == w, column, mixer_gain)
    token_w = nn(jnp.concatenate(token_parts, axis=1), window_pick)
    for copy in got_weights:
        copy.wait()
    ag2_sent.wait_recv()
    wo_window.wait_recv()
    everyone = ag2[...].astype(f32).reshape(count * kinds, head).astype(bf16)
    for h in range(heads):
        picked = nn(head_picks[h], everyone).astype(bf16)
        for w in range(n_win):
            at = w * out_wide + h * head
            diag[w * per_w : (w + 1) * per_w, at : at + head] = picked
    att[t] = nt(wo_v[...], diag[...]).astype(bf16)
    att_sent = to_tp(att, att_s, att_r)
    pending.append(att_sent)
    att_sent.wait_recv()
    wu_window.wait_recv()

    attended = att[0].astype(f32)
    for k in range(1, n_tp):
        attended += att[k].astype(f32)
    middle_b = (token_w + attended).astype(bf16)
    middle = middle_b.astype(f32)
    scaled = jnp.concatenate([middle * mixer_gain] * n_win, axis=0)
    shape = scaled.shape
    scaled = jnp.where(iota(shape, 1) // per_w == iota(shape, 0) // block, scaled, 0.0)
    left = nt(spread_rows, scaled.astype(bf16))
    part = iota(left.shape, 0) // seq % parts
    product = jnp.zeros((left.shape[0], wide), f32)
    for j in range(parts):
        product += nn(
            jnp.where(part == j, left, 0.0).astype(bf16), wu_v[:, j * wide : (j + 1) * wide]
        )
    rs3[...] = product.astype(bf16).reshape(rs3.shape)
    sq_src[...] = jnp.sum(middle * middle, axis=0, keepdims=True)
    rs3_sent = to_far(lambda i: rs3.at[i], rs3_far, rs3_s, rs3_r, -1)
    sq_sent = to_far(lambda i: sq_src, sq_far, sq_s, sq_r, -1)
    for w, offset in enumerate(UP_WINDOW):
        placed = nt(middle_b, window_pick[w * all_rows : (w + 1) * all_rows]).astype(bf16)
        mid_src[w] = placed.reshape(n_tp, mine, all_rows)
        if offset:
            ex.copy(mid_src.at[w, t], mid.at[w], mid_s, mid_r, offset).start()
        else:
            mid[w] = mid_src[w, t]
    mid_sent = waiter(mid.at[0 : n_win - 1], mid_s, mid_r)
    pending.append(mid_sent)
    sq_sent.wait_recv()
    lane = iota((1, all_rows), 1)
    squares = jnp.zeros((1, all_rows), f32)
    for i in range(count):
        squares += jnp.where(lane % per_w // seq == i, sq_far[i], 0.0)
    shape = (parts * seq, all_rows)
    squares = jnp.sum(
        jnp.where(iota(shape, 1) % seq == iota(shape, 0) % seq, squares, 0.0),
        axis=1,
        keepdims=True,
    )
    second = lax.rsqrt(squares / width + epsilon)
    up = jnp.zeros((parts * seq, wide), f32)
    rs3_sent.wait_recv()
    for i in range(count):
        up += rs3_far[i].astype(f32)
    ag4_src[...] = jnp.square(jnp.maximum(second * up, 0.0)).astype(bf16)

    ag4_sent = to_far(lambda i: ag4_src, ag4, ag4_s, ag4_r, 1)
    wdn_window.wait_recv()
    mid_sent.wait_recv()
    middle = mid[0].astype(f32)
    for w in range(1, n_win):
        middle += mid[w].astype(f32)
    ag4_sent.wait_recv()
    everyone = ag4[...].reshape(count * parts * seq, wide)
    picked = jnp.concatenate(
        [nn(part_picks[j], everyone).astype(bf16) for j in range(parts)], axis=1
    )
    lowered_part = nt(wdn_v[...], picked).astype(bf16)
    fin_src[...] = nn(lowered_part, place_rows).astype(bf16).reshape(fin_src.shape)
    for w, offset in enumerate(DOWN_WINDOW):
        row = lax.rem(z + offset + n_kv, n_kv)
        for k in range(n_tp):
            if offset == 0 and k == 0:
                fin[w * n_tp + t] = fin_src[w * n_tp + t]
                continue
            peer = lax.rem(t + k, n_tp)
            pltpu.make_async_remote_copy(
                src_ref=fin_src.at[w * n_tp + peer],
                dst_ref=fin.at[w * n_tp + t],
                send_sem=fin_s,
                recv_sem=fin_r,
                device_id=(g, row, peer),
                device_id_type=MESH,
            ).start()
    fin_sent = waiter(fin.at[0 : n_win * n_tp - 1], fin_s, fin_r)
    pending.append(fin_sent)
    fin_sent.wait_recv()
    lowered = jnp.sum(fin[...].astype(f32), axis=0)
    out_ref[...] = (middle + lowered).astype(bf16)
    for copy in pending:
        copy.wait_send()


def solution(mesh):
    n_kv, n_tp = mesh.shape["kv"], mesh.shape["tp"]

    def local(
        tokens,
        state,
        norm_gain,
        w_query,
        w_key,
        w_value,
        w_beta,
        w_decay,
        a_log,
        dt_bias,
        head_gain,
        w_out,
        mixer_gain,
        w_up,
        w_down,
    ):
        seq, heads, head = state.shape[:3]
        rows, mine = tokens.shape
        block = w_query.shape[0]
        parts = w_up.shape[1] // (2 * head)
        wide = w_up.shape[1] // parts
        count = n_kv // 4
        dims = (n_kv, n_tp, seq, heads, block * n_kv)
        vmem, hbm = (
            pl.BlockSpec(memory_space=pltpu.VMEM),
            pl.BlockSpec(memory_space=pltpu.HBM),
        )
        dma = pltpu.SemaphoreType.DMA
        blocks = (parts * seq, wide)
        near = (3 * count - 1,)
        n_win = len(UP_WINDOW)
        scratch = [
            pltpu.VMEM((n_tp + 1, mine, rows), bf16),
            pltpu.VMEM((n_win, n_tp + 1, mine, rows), bf16),
            pltpu.VMEM(state.shape, f32),
            pltpu.VMEM((2 * heads * block, 2 * head), bf16),
            pltpu.VMEM((2, w_beta.shape[1], head), bf16),
            pltpu.VMEM((block, n_win * heads * head), bf16),
            pltpu.VMEM((n_win * block, w_up.shape[1]), bf16),
            pltpu.VMEM((n_win * block, w_down.shape[0]), bf16),
            pltpu.VMEM((n_kv, *blocks), bf16),
            pltpu.VMEM((*near, *blocks), bf16),
            pltpu.VMEM((count, *blocks), bf16),
            pltpu.VMEM((count, *blocks), bf16),
            pltpu.VMEM((heads * seq, head), bf16),
            pltpu.VMEM((count, heads * seq, head), bf16),
            pltpu.VMEM((rows, n_win * heads * head), bf16),
            pltpu.VMEM((n_tp, block, rows), bf16),
            pltpu.VMEM((n_win, n_tp, mine, rows), bf16),
            pltpu.VMEM((n_win, mine, rows), bf16),
            pltpu.VMEM((count, *blocks), bf16),
            pltpu.VMEM((count, *blocks), bf16),
            pltpu.VMEM((1, rows), f32),
            pltpu.VMEM((count, 1, rows), f32),
            pltpu.VMEM(blocks, bf16),
            pltpu.VMEM((count, *blocks), bf16),
            pltpu.VMEM((n_win * n_tp, mine, rows), bf16),
            pltpu.VMEM((n_win * n_tp, mine, rows), bf16),
            pltpu.VMEM(norm_gain.shape, bf16),
            pltpu.VMEM(mixer_gain.shape, bf16),
            pltpu.VMEM((1, head), f32),
            pltpu.VMEM(a_log.shape, f32),
            pltpu.VMEM(dt_bias.shape, f32),
            dma((13,)),
            *[dma] * 6,
            dma((4,)),
            dma((4,)),
            *[dma] * 14,
            pltpu.SemaphoreType.REGULAR,
            pltpu.SemaphoreType.REGULAR,
            pltpu.SemaphoreType.REGULAR,
        ]
        mixed_t, new_state = pl.pallas_call(
            functools.partial(kernel, dims),
            out_shape=(
                jax.ShapeDtypeStruct((mine, rows), bf16),
                jax.ShapeDtypeStruct(state.shape, f32),
            ),
            in_specs=[hbm] * 15,
            out_specs=(vmem, vmem),
            scratch_shapes=scratch,
            compiler_params=pltpu.CompilerParams(collective_id=0, has_side_effects=True, vmem_limit_bytes=32 * 2**20),
        )(
            *[
                pltpu.with_memory_space_constraint(x, pltpu.HBM)
                for x in (
                    tokens.T,
                    state,
                    norm_gain,
                    w_query,
                    w_key,
                    w_value,
                    w_beta.T,
                    w_decay.T,
                    a_log,
                    dt_bias,
                    head_gain.reshape(1, head),
                    w_out.T,
                    mixer_gain,
                    w_up,
                    w_down.T,
                )
            ]
        )
        return mixed_t.T, new_state

    return jax.shard_map(
        local,
        mesh=mesh,
        in_specs=(
            P("grp", ("kv", "tp")),
            P(("grp", "kv"), "tp", None, None),
            P("kv"),
            P("kv", "tp"),
            P("kv", "tp"),
            P("kv", "tp"),
            P(),
            P(),
            P("tp"),
            P("tp"),
            P(),
            P("tp", "kv"),
            P("kv"),
            P("kv", "tp"),
            P("tp", "kv"),
        ),
        out_specs=(P("grp", ("kv", "tp")), P(("grp", "kv"), "tp", None, None)),
        check_vma=False,
    )
```

```python
import functools

import jax
import jax.numpy as jnp
from jax import lax
from jax.experimental import pallas as pl
from jax.experimental.pallas import tpu as pltpu
from jax.sharding import PartitionSpec as P

MESH = pl.DeviceIdType.MESH
epsilon = 1e-06
f32 = jnp.float32
bf16 = jnp.bfloat16


def nn(a, b):
    return jnp.dot(a, b, preferred_element_type=f32)


def nt(a, b):
    return lax.dot_general(a, b, (((1,), (1,)), ((), ())), preferred_element_type=f32)


def exact_nn(a, onehot):
    high = a.astype(bf16)
    low = (a - high.astype(f32)).astype(bf16)
    return nn(high, onehot) + nn(low, onehot)


def lanes_of(x, lane):
    at = lax.broadcasted_iota(jnp.int32, x.shape, 1)
    return jnp.sum(jnp.where(at == lane, x, 0.0), axis=1, keepdims=True)


def column_of(row):
    n = row.shape[1]
    eye = lax.broadcasted_iota(jnp.int32, (n, n), 0) == lax.broadcasted_iota(
        jnp.int32, (n, n), 1
    )
    return jnp.sum(jnp.where(eye, row, 0.0), axis=1, keepdims=True)


UP_WINDOW = (-1, 0, 1, 2)
DOWN_WINDOW = (-2, -1, 0, 1)


class Exchange:
    def __init__(self, n_kv, g, z, t):
        self.n_kv, self.g, self.z, self.t = n_kv, g, z, t
        self.half = n_kv // 8
        up = [2 + 4 * i for i in range(self.half)]
        self.reach = up + [-u for u in up]
        self.count = 2 * self.half
        self.steps = [(0, 1), (1, -1)]
        self.farthest_first = [
            k * self.half + i for i in reversed(range(self.half)) for k in (0, 1)
        ]
        self.nearest_first = list(reversed(self.farthest_first))

    def device(self, offset):
        return (self.g, lax.rem(self.z + offset + self.n_kv, self.n_kv), self.t)

    def near(self, i):
        last = () if i == self.count - 1 else ((3, 2 if i < self.half else -2),)
        return self.steps + list(last)

    def copy(self, src, dst, send, recv, offset):
        return pltpu.make_async_remote_copy(
            src_ref=src,
            dst_ref=dst,
            send_sem=send,
            recv_sem=recv,
            device_id=self.device(offset),
            device_id_type=MESH,
        )


def placing(per_slot, n_kv, seq, z):
    count = n_kv // 4
    half = count // 2
    shape = (n_kv * per_slot, n_kv * seq)
    m = lax.broadcasted_iota(jnp.int32, shape, 0)
    slot = m // per_slot
    i = slot % count
    group = slot // count
    reach = jnp.where(i < half, 2 + 4 * i, 4 * half - 2 - 4 * i)
    side = jnp.where(i < half, 2, -2)
    step = jnp.where(group == 0, 1, jnp.where(group == 1, -1, jnp.where(group == 2, 0, side)))
    offset = jnp.where(slot == n_kv - 1, 0, reach + step)
    owner = (z - offset + n_kv) % n_kv
    row = owner * seq + m % seq
    return (row == lax.broadcasted_iota(jnp.int32, shape, 1)).astype(bf16)


def kernel(
    dims,
    tok_ref,
    state_hbm,
    gain_ref,
    wq_hbm,
    wk_hbm,
    wv_hbm,
    wb_hbm,
    wd_hbm,
    alog_ref,
    dt_ref,
    hgain_ref,
    wo_hbm,
    mgain_ref,
    wu_hbm,
    wdn_hbm,
    out_ref,
    state_out,
    tok_all,
    tok_near,
    state_v,
    rhs1,
    wext,
    wo_v,
    wu_v,
    wdn_v,
    rs1,
    rs1_near,
    rs1_far_src,
    rs1_far,
    ag2_src,
    ag2,
    diag,
    att,
    mid_src,
    mid,
    rs3,
    rs3_far,
    sq_src,
    sq_far,
    ag4_src,
    ag4,
    fin_src,
    fin,
    gain_v,
    mgain_v,
    hgain_v,
    alog_v,
    dt_v,
    loc,
    tok_s,
    tok_r,
    rs1_ns,
    rs1_nr,
    rs1_fs,
    rs1_fr,
    win_s,
    win_r,
    ag2_s,
    ag2_r,
    att_s,
    att_r,
    rs3_s,
    rs3_r,
    sq_s,
    sq_r,
    mid_s,
    mid_r,
    ag4_s,
    ag4_r,
    fin_s,
    fin_r,
    sem_a,
    sem_b,
):
    n_kv, n_tp, seq, heads, width = dims
    g, z, t = lax.axis_index("grp"), lax.axis_index("kv"), lax.axis_index("tp")
    ex = Exchange(n_kv, g, z, t)
    count, half = ex.count, ex.half
    mine = tok_ref.shape[0]
    block = n_tp * mine
    all_rows = tok_ref.shape[1]
    head = hgain_v.shape[1]
    own = n_kv - 1

    def tp_peer(k):
        return (g, z, lax.rem(t + k, n_tp))

    barrier = pltpu.get_barrier_semaphore()
    for k in range(1, n_tp):
        pl.semaphore_signal(barrier, inc=1, device_id=tp_peer(k), device_id_type=MESH)
    for offset in (1, -1, 2, -2, 4, -4):
        pl.semaphore_signal(barrier, inc=1, device_id=ex.device(offset), device_id_type=MESH)

    def waiter(ref, send, recv):
        return pltpu.make_async_remote_copy(
            src_ref=ref,
            dst_ref=ref,
            send_sem=send,
            recv_sem=recv,
            device_id=tp_peer(1),
            device_id_type=MESH,
        )

    def fetch(src, dst, k):
        copy = pltpu.make_async_copy(src, dst, loc.at[k])
        copy.start()
        return copy

    got_tok = fetch(tok_ref, tok_all.at[t], 0)
    got_mgain = fetch(mgain_ref, mgain_v, 1)
    got_gain = fetch(gain_ref, gain_v, 2)
    lanes = wext.shape[2]
    at = pl.multiple_of((z * block // lanes) * lanes, lanes)
    got_ext = [
        fetch(wb_hbm.at[:, pl.ds(at, lanes)], wext.at[0], 3),
        fetch(wd_hbm.at[:, pl.ds(at, lanes)], wext.at[1], 4),
    ]
    for i, w in enumerate((wq_hbm, wk_hbm)):
        for h in range(heads):
            at = (i * heads + h) * block
            fetch(w.at[:, h * head : (h + 1) * head], rhs1.at[at : at + block, 0:head], 5)
    for h in range(heads):
        fetch(
            wv_hbm.at[:, h * head : (h + 1) * head],
            rhs1.at[h * block : (h + 1) * block, head : 2 * head],
            5,
        )
    whole = rhs1.at[0 : 3 * heads * block // 2]
    got_rhs1 = pltpu.make_async_copy(whole, whole, loc.at[5])
    got_small = [
        fetch(hgain_ref, hgain_v, 6),
        fetch(alog_ref, alog_v, 7),
        fetch(dt_ref, dt_v, 8),
    ]
    got_state = fetch(state_hbm, state_v, 9)
    parts = wu_v.shape[1] // (2 * head)
    wide = 2 * head
    kinds = heads * seq
    n_win = len(UP_WINDOW)
    out_wide = heads * head
    here_up, here_down = UP_WINDOW.index(0), DOWN_WINDOW.index(0)
    got_weights = [
        fetch(wo_hbm, wo_v.at[:, here_up * out_wide : (here_up + 1) * out_wide], 10),
        fetch(wu_hbm, wu_v.at[here_up * block : (here_up + 1) * block], 11),
        fetch(wdn_hbm, wdn_v.at[here_down * block : (here_down + 1) * block], 12),
    ]

    rhs1[heads * block :, head:] = jnp.zeros((heads * block, head), bf16)
    diag[...] = jnp.zeros(diag.shape, bf16)
    spread16 = placing(parts * seq, n_kv, seq, z)
    part_of_row = (
        lax.broadcasted_iota(jnp.int32, (n_kv * parts * seq, parts * block), 0) // seq
    ) % parts
    part_mask = part_of_row == (
        lax.broadcasted_iota(jnp.int32, (n_kv * parts * seq, parts * block), 1) // block
    )
    got_mgain.wait()
    gain_row = mgain_v[...].astype(f32).reshape(1, block)
    gain_row = jnp.concatenate([gain_row, jnp.zeros((1, all_rows - block), f32)], axis=1)
    tok_all[n_tp] = jnp.broadcast_to(gain_row, (mine, all_rows)).astype(bf16)
    got_gain.wait()
    gain = column_of(gain_v[...].astype(f32).reshape(1, block))
    got_tok.wait()

    pl.semaphore_wait(barrier, n_tp - 1 + 6)
    for offset in (4, -4):
        pl.semaphore_signal(sem_a, inc=1, device_id=ex.device(offset), device_id_type=MESH)

    def to_tp(dst, send, recv):
        for k in range(1, n_tp):
            peer = lax.rem(t + k, n_tp)
            pltpu.make_async_remote_copy(
                src_ref=dst.at[t],
                dst_ref=dst.at[t],
                send_sem=send,
                recv_sem=recv,
                device_id=(g, z, peer),
                device_id_type=MESH,
            ).start()
        return waiter(dst.at[0 : n_tp - 1], send, recv)

    pending = []
    tok_sent = to_tp(tok_all, tok_s, tok_r)
    pending.append(tok_sent)
    got_rhs1.wait()
    for copy in got_ext:
        copy.wait()
    odd = lax.rem(z, lanes // block) if lanes // block > 1 else 0
    pieces = []
    for i in range(2):
        piece = wext[i][:, 0:block]
        for k in range(1, lanes // block):
            piece = jnp.where(odd == k, wext[i][:, k * block : (k + 1) * block], piece)
        pieces.append(piece)
    n_heads = pieces[0].shape[0]
    wext_t = jnp.concatenate(
        pieces + [jnp.zeros((head - 2 * n_heads, block), bf16)], axis=0
    )
    at_row = lax.broadcasted_iota(jnp.int32, (head, block), 0)
    square_t = (at_row == 2 * n_heads).astype(bf16)
    ext_t = jnp.concatenate([wext_t, square_t], axis=1)

    tok_sent.wait_recv()
    pl.semaphore_wait(sem_a, 2)
    for offset in (8, -8):
        pl.semaphore_signal(sem_b, inc=1, device_id=ex.device(offset), device_id_type=MESH)

    def spread(x_t):
        stacked = jnp.concatenate([x_t] * parts, axis=0)
        rows = nt(spread16, stacked)
        return jnp.where(part_mask, rows, 0.0).astype(bf16)

    tok_t = tok_all[0:n_tp].astype(f32).reshape(block, all_rows)
    scaled_t = (tok_t * gain).astype(bf16)
    left = spread(scaled_t)
    both = jnp.concatenate([scaled_t, (tok_t * tok_t).astype(bf16)], axis=0)
    left2 = nt(spread16, both)
    left2 = jnp.where(part_of_row[:, 0 : 2 * block] >= heads, left2, 0.0).astype(bf16)
    product = nn(left, rhs1[...])
    extra = nt(left2, ext_t)
    product = jnp.concatenate([product[:, :head], product[:, head:] + extra], axis=1)
    rs1[...] = product.astype(bf16).reshape(rs1.shape)

    for i in ex.farthest_first:
        for group, step in ex.near(i):
            k = group * count + i if group < 2 else 2 * count + i
            ex.copy(
                rs1.at[group * count + i], rs1_near.at[k], rs1_ns, rs1_nr, -step
            ).start()
    near_sent = waiter(rs1.at[0 : 3 * count - 1], rs1_ns, rs1_nr)
    pending.append(near_sent)
    near_sent.wait_recv()
    for i in range(count):
        total = rs1[2 * count + i].astype(f32)
        for group, step in ex.near(i):
            k = group * count + i if group < 2 else 2 * count + i
            total += rs1_near[k].astype(f32)
        rs1_far_src[i] = total.astype(bf16)
    pl.semaphore_wait(sem_b, 2)

    def to_far(src_of, dst, send, recv, sign):
        for i in ex.farthest_first:
            ex.copy(src_of(i), dst.at[i], send, recv, sign * ex.reach[i]).start()
        sent = waiter(dst, send, recv)
        pending.append(sent)
        return sent

    far_sent = to_far(lambda i: rs1_far_src.at[i], rs1_far, rs1_fs, rs1_fr, -1)

    def to_window(src, dst_of, whole, k, offsets):
        for w, offset in enumerate(offsets):
            if offset:
                ex.copy(src, dst_of(w), win_s.at[k], win_r.at[k], -offset).start()
        sent = waiter(whole, win_s.at[k], win_r.at[k])
        pending.append(sent)
        return sent

    tok_window = to_window(
        tok_all, lambda w: tok_near.at[w], tok_near.at[0 : n_win - 1], 0, UP_WINDOW
    )
    wo_window = to_window(
        wo_hbm,
        lambda w: wo_v.at[:, w * out_wide : (w + 1) * out_wide],
        wo_v.at[:, 0 : (n_win - 1) * out_wide],
        1,
        UP_WINDOW,
    )

    got_state.wait()
    for copy in got_small:
        copy.wait()
    far_sent.wait_recv()
    sums = rs1[own].astype(f32)
    for i in range(count):
        sums += rs1_far[i].astype(f32)

    rows = heads * seq
    query_sum, key_sum = sums[:rows, :head], sums[rows:, :head]
    value_sum, extra = sums[:rows, head:], sums[rows:, head:]
    which = lax.broadcasted_iota(jnp.int32, (rows, head), 0) // seq
    lane = lax.broadcasted_iota(jnp.int32, (rows, head), 1)
    beta_sum = jnp.sum(
        jnp.where(lane == t * heads + which, extra, 0.0), axis=1, keepdims=True
    )
    decay_sum = jnp.sum(
        jnp.where(lane == n_heads + t * heads + which, extra, 0.0), axis=1, keepdims=True
    )
    square_sum = lanes_of(extra, 2 * n_heads)
    first = lax.rsqrt(square_sum / width + epsilon)
    query_pre, key_pre, value_pre = first * query_sum, first * key_sum, first * value_sum
    query = query_pre * lax.rsqrt(jnp.sum(query_pre * query_pre, axis=1, keepdims=True) + epsilon)
    key = key_pre * lax.rsqrt(jnp.sum(key_pre * key_pre, axis=1, keepdims=True) + epsilon)
    beta = jax.nn.sigmoid(first * beta_sum)
    which1 = lax.broadcasted_iota(jnp.int32, (rows, 1), 0) // seq
    a_logs, dt_biases = alog_v[...].reshape(1, heads), dt_v[...].reshape(1, heads)
    a_log = jnp.zeros((rows, 1), f32)
    dt_bias = jnp.zeros((rows, 1), f32)
    for h in range(heads):
        a_log = jnp.where(which1 == h, a_logs[:, h : h + 1], a_log)
        dt_bias = jnp.where(which1 == h, dt_biases[:, h : h + 1], dt_bias)
    logit = first * decay_sum + dt_bias
    softplus = jnp.maximum(logit, 0.0) + jnp.log1p(jnp.exp(-jnp.abs(logit)))
    decay = jnp.exp(-jnp.exp(a_log) * softplus)
    query_t, key_t = query.T, key.T
    key_reads, query_reads = [], []
    for k in range(rows):
        matrix = state_v[k % seq, k // seq]
        key_reads.append(jnp.sum(matrix * key_t[:, k : k + 1], axis=0, keepdims=True))
        query_reads.append(jnp.sum(matrix * query_t[:, k : k + 1], axis=0, keepdims=True))
    key_read = jnp.concatenate(key_reads, axis=0)
    query_read = jnp.concatenate(query_reads, axis=0)
    fresh = beta * (value_pre - decay * key_read)
    meeting = jnp.sum(query * key, axis=1, keepdims=True)
    reading = decay * query_read + meeting * fresh
    normed = (
        reading
        * lax.rsqrt(jnp.mean(reading * reading, axis=1, keepdims=True) + epsilon)
        * hgain_v[...]
    )

    ag2_src[...] = normed.astype(bf16)
    ag2_sent = to_far(lambda i: ag2_src, ag2, ag2_s, ag2_r, 1)
    wu_window = to_window(
        wu_hbm,
        lambda w: wu_v.at[w * block : (w + 1) * block],
        wu_v.at[0 : (n_win - 1) * block],
        2,
        UP_WINDOW,
    )
    wdn_window = to_window(
        wdn_hbm,
        lambda w: wdn_v.at[w * block : (w + 1) * block],
        wdn_v.at[0 : (n_win - 1) * block],
        3,
        DOWN_WINDOW,
    )
    for k in range(rows):
        matrix = state_v[k % seq, k // seq]
        state_out[k % seq, k // seq] = (
            decay[k : k + 1] * matrix + key_t[:, k : k + 1] * fresh[k : k + 1]
        )

    def iota(shape, dim):
        return lax.broadcasted_iota(jnp.int32, shape, dim)

    def owner_row(slot, r):
        half = ex.half
        reach = jnp.where(slot < half, 2 + 4 * slot, 4 * half - 2 - 4 * slot)
        return (z - reach + n_kv) % n_kv * seq + r

    per_w = count * seq
    shape = (n_win * all_rows, all_rows)
    lane = iota(shape, 1)
    lane_owner = owner_row(lane % per_w // seq, lane % seq)
    window_pick = (
        (lane // per_w == iota(shape, 0) // all_rows) & (lane_owner == iota(shape, 0) % all_rows)
    ).astype(bf16)
    shape = (per_w, all_rows)
    place_rows = (owner_row(iota(shape, 0) // seq, iota(shape, 0) % seq) == iota(shape, 1)).astype(
        bf16
    )
    head_picks = []
    shape = (per_w, count * kinds)
    for h in range(heads):
        r0, c1 = iota(shape, 0), iota(shape, 1)
        head_picks.append(
            (
                (c1 // kinds == r0 // seq) & (c1 % seq == r0 % seq) & (c1 // seq % heads == h)
            ).astype(bf16)
        )
    shape = (count * parts * seq, all_rows)
    r0, c1 = iota(shape, 0), iota(shape, 1)
    spread_rows = (
        (r0 // (parts * seq) == c1 % per_w // seq) & (r0 % seq == c1 % seq)
    ).astype(bf16)
    shape = (per_w, count * parts * seq)
    r0, c1 = iota(shape, 0), iota(shape, 1)
    part_picks = [
        (
            (c1 // (parts * seq) == r0 // seq) & (c1 % seq == r0 % seq) & (c1 // seq % parts == j)
        ).astype(bf16)
        for j in range(parts)
    ]
    tok_window.wait_recv()
    token_parts = []
    mixer_gain = jnp.zeros((block, all_rows), f32)
    lane = iota((block, all_rows), 1)
    for w, offset in enumerate(UP_WINDOW):
        source = tok_near.at[w] if offset else tok_all
        token_parts.append(source[0:n_tp].astype(f32).reshape(block, all_rows).astype(bf16))
        column = column_of(source[n_tp].astype(f32)[0:1, 0:block])
        mixer_gain = jnp.where(lane // per_w == w, column, mixer_gain)
    token_w = nn(jnp.concatenate(token_parts, axis=1), window_pick)
    for copy in got_weights:
        copy.wait()
    ag2_sent.wait_recv()
    wo_window.wait_recv()
    everyone = ag2[...].astype(f32).reshape(count * kinds, head).astype(bf16)
    for h in range(heads):
        picked = nn(head_picks[h], everyone).astype(bf16)
        for w in range(n_win):
            at = w * out_wide + h * head
            diag[w * per_w : (w + 1) * per_w, at : at + head] = picked
    att[t] = nt(wo_v[...], diag[...]).astype(bf16)
    att_sent = to_tp(att, att_s, att_r)
    pending.append(att_sent)
    att_sent.wait_recv()
    wu_window.wait_recv()

    attended = att[0].astype(f32)
    for k in range(1, n_tp):
        attended += att[k].astype(f32)
    middle_b = (token_w + attended).astype(bf16)
    middle = middle_b.astype(f32)
    scaled = jnp.concatenate([middle * mixer_gain] * n_win, axis=0)
    shape = scaled.shape
    scaled = jnp.where(iota(shape, 1) // per_w == iota(shape, 0) // block, scaled, 0.0)
    left = nt(spread_rows, scaled.astype(bf16))
    part = iota(left.shape, 0) // seq % parts
    product = jnp.zeros((left.shape[0], wide), f32)
    for j in range(parts):
        product += nn(
            jnp.where(part == j, left, 0.0).astype(bf16), wu_v[:, j * wide : (j + 1) * wide]
        )
    rs3[...] = product.astype(bf16).reshape(rs3.shape)
    sq_src[...] = jnp.sum(middle * middle, axis=0, keepdims=True)
    rs3_sent = to_far(lambda i: rs3.at[i], rs3_far, rs3_s, rs3_r, -1)
    sq_sent = to_far(lambda i: sq_src, sq_far, sq_s, sq_r, -1)
    for w, offset in enumerate(UP_WINDOW):
        placed = nt(middle_b, window_pick[w * all_rows : (w + 1) * all_rows]).astype(bf16)
        mid_src[w] = placed.reshape(n_tp, mine, all_rows)
        if offset:
            ex.copy(mid_src.at[w, t], mid.at[w], mid_s, mid_r, offset).start()
        else:
            mid[w] = mid_src[w, t]
    mid_sent = waiter(mid.at[0 : n_win - 1], mid_s, mid_r)
    pending.append(mid_sent)
    sq_sent.wait_recv()
    lane = iota((1, all_rows), 1)
    squares = jnp.zeros((1, all_rows), f32)
    for i in range(count):
        squares += jnp.where(lane % per_w // seq == i, sq_far[i], 0.0)
    shape = (parts * seq, all_rows)
    squares = jnp.sum(
        jnp.where(iota(shape, 1) % seq == iota(shape, 0) % seq, squares, 0.0),
        axis=1,
        keepdims=True,
    )
    second = lax.rsqrt(squares / width + epsilon)
    up = jnp.zeros((parts * seq, wide), f32)
    rs3_sent.wait_recv()
    for i in range(count):
        up += rs3_far[i].astype(f32)
    ag4_src[...] = jnp.square(jnp.maximum(second * up, 0.0)).astype(bf16)

    ag4_sent = to_far(lambda i: ag4_src, ag4, ag4_s, ag4_r, 1)
    wdn_window.wait_recv()
    mid_sent.wait_recv()
    middle = mid[0].astype(f32)
    for w in range(1, n_win):
        middle += mid[w].astype(f32)
    ag4_sent.wait_recv()
    everyone = ag4[...].reshape(count * parts * seq, wide)
    picked = jnp.concatenate(
        [nn(part_picks[j], everyone).astype(bf16) for j in range(parts)], axis=1
    )
    lowered_part = nt(wdn_v[...], picked).astype(bf16)
    fin_src[...] = nn(lowered_part, place_rows).astype(bf16).reshape(fin_src.shape)
    for w, offset in enumerate(DOWN_WINDOW):
        row = lax.rem(z + offset + n_kv, n_kv)
        for k in range(n_tp):
            if offset == 0 and k == 0:
                fin[w * n_tp + t] = fin_src[w * n_tp + t]
                continue
            peer = lax.rem(t + k, n_tp)
            pltpu.make_async_remote_copy(
                src_ref=fin_src.at[w * n_tp + peer],
                dst_ref=fin.at[w * n_tp + t],
                send_sem=fin_s,
                recv_sem=fin_r,
                device_id=(g, row, peer),
                device_id_type=MESH,
            ).start()
    fin_sent = waiter(fin.at[0 : n_win * n_tp - 1], fin_s, fin_r)
    pending.append(fin_sent)
    fin_sent.wait_recv()
    lowered = jnp.sum(fin[...].astype(f32), axis=0)
    out_ref[...] = (middle + lowered).astype(bf16)
    for copy in pending:
        copy.wait_send()


def solution(mesh):
    n_kv, n_tp = mesh.shape["kv"], mesh.shape["tp"]

    def local(
        tokens,
        state,
        norm_gain,
        w_query,
        w_key,
        w_value,
        w_beta,
        w_decay,
        a_log,
        dt_bias,
        head_gain,
        w_out,
        mixer_gain,
        w_up,
        w_down,
    ):
        seq, heads, head = state.shape[:3]
        rows, mine = tokens.shape
        block = w_query.shape[0]
        parts = w_up.shape[1] // (2 * head)
        wide = w_up.shape[1] // parts
        count = n_kv // 4
        dims = (n_kv, n_tp, seq, heads, block * n_kv)
        vmem, hbm = (
            pl.BlockSpec(memory_space=pltpu.VMEM),
            pl.BlockSpec(memory_space=pltpu.HBM),
        )
        dma = pltpu.SemaphoreType.DMA
        blocks = (parts * seq, wide)
        near = (3 * count - 1,)
        n_win = len(UP_WINDOW)
        scratch = [
            pltpu.VMEM((n_tp + 1, mine, rows), bf16),
            pltpu.VMEM((n_win, n_tp + 1, mine, rows), bf16),
            pltpu.VMEM(state.shape, f32),
            pltpu.VMEM((2 * heads * block, 2 * head), bf16),
            pltpu.VMEM((2, w_beta.shape[1], head), bf16),
            pltpu.VMEM((block, n_win * heads * head), bf16),
            pltpu.VMEM((n_win * block, w_up.shape[1]), bf16),
            pltpu.VMEM((n_win * block, w_down.shape[0]), bf16),
            pltpu.VMEM((n_kv, *blocks), bf16),
            pltpu.VMEM((*near, *blocks), bf16),
            pltpu.VMEM((count, *blocks), bf16),
            pltpu.VMEM((count, *blocks), bf16),
            pltpu.VMEM((heads * seq, head), bf16),
            pltpu.VMEM((count, heads * seq, head), bf16),
            pltpu.VMEM((rows, n_win * heads * head), bf16),
            pltpu.VMEM((n_tp, block, rows), bf16),
            pltpu.VMEM((n_win, n_tp, mine, rows), bf16),
            pltpu.VMEM((n_win, mine, rows), bf16),
            pltpu.VMEM((count, *blocks), bf16),
            pltpu.VMEM((count, *blocks), bf16),
            pltpu.VMEM((1, rows), f32),
            pltpu.VMEM((count, 1, rows), f32),
            pltpu.VMEM(blocks, bf16),
            pltpu.VMEM((count, *blocks), bf16),
            pltpu.VMEM((n_win * n_tp, mine, rows), bf16),
            pltpu.VMEM((n_win * n_tp, mine, rows), bf16),
            pltpu.VMEM(norm_gain.shape, bf16),
            pltpu.VMEM(mixer_gain.shape, bf16),
            pltpu.VMEM((1, head), f32),
            pltpu.VMEM(a_log.shape, f32),
            pltpu.VMEM(dt_bias.shape, f32),
            dma((13,)),
            *[dma] * 6,
            dma((4,)),
            dma((4,)),
            *[dma] * 14,
            pltpu.SemaphoreType.REGULAR,
            pltpu.SemaphoreType.REGULAR,
        ]
        mixed_t, new_state = pl.pallas_call(
            functools.partial(kernel, dims),
            out_shape=(
                jax.ShapeDtypeStruct((mine, rows), bf16),
                jax.ShapeDtypeStruct(state.shape, f32),
            ),
            in_specs=[hbm] * 15,
            out_specs=(vmem, vmem),
            scratch_shapes=scratch,
            compiler_params=pltpu.CompilerParams(collective_id=0, has_side_effects=True, vmem_limit_bytes=32 * 2**20),
        )(
            *[
                pltpu.with_memory_space_constraint(x, pltpu.HBM)
                for x in (
                    tokens.T,
                    state,
                    norm_gain,
                    w_query,
                    w_key,
                    w_value,
                    w_beta.T,
                    w_decay.T,
                    a_log,
                    dt_bias,
                    head_gain.reshape(1, head),
                    w_out.T,
                    mixer_gain,
                    w_up,
                    w_down.T,
                )
            ]
        )
        return mixed_t.T, new_state

    return jax.shard_map(
        local,
        mesh=mesh,
        in_specs=(
            P("grp", ("kv", "tp")),
            P(("grp", "kv"), "tp", None, None),
            P("kv"),
            P("kv", "tp"),
            P("kv", "tp"),
            P("kv", "tp"),
            P(),
            P(),
            P("tp"),
            P("tp"),
            P(),
            P("tp", "kv"),
            P("kv"),
            P("kv", "tp"),
            P("tp", "kv"),
        ),
        out_specs=(P("grp", ("kv", "tp")), P(("grp", "kv"), "tp", None, None)),
        check_vma=False,
    )
```

```python
import functools

import jax
import jax.numpy as jnp
from jax import lax
from jax.experimental import pallas as pl
from jax.experimental.pallas import tpu as pltpu
from jax.sharding import PartitionSpec as P

MESH = pl.DeviceIdType.MESH
epsilon = 1e-06
f32 = jnp.float32
bf16 = jnp.bfloat16


def nn(a, b):
    return jnp.dot(a, b, preferred_element_type=f32)


def nt(a, b):
    return lax.dot_general(a, b, (((1,), (1,)), ((), ())), preferred_element_type=f32)


def exact_nn(a, onehot):
    high = a.astype(bf16)
    low = (a - high.astype(f32)).astype(bf16)
    return nn(high, onehot) + nn(low, onehot)


def lanes_of(x, lane):
    at = lax.broadcasted_iota(jnp.int32, x.shape, 1)
    return jnp.sum(jnp.where(at == lane, x, 0.0), axis=1, keepdims=True)


def column_of(row):
    n = row.shape[1]
    eye = lax.broadcasted_iota(jnp.int32, (n, n), 0) == lax.broadcasted_iota(
        jnp.int32, (n, n), 1
    )
    return jnp.sum(jnp.where(eye, row, 0.0), axis=1, keepdims=True)


UP_WINDOW = (-1, 0, 1, 2)
DOWN_WINDOW = (-2, -1, 0, 1)


class Exchange:
    def __init__(self, n_kv, g, z, t):
        self.n_kv, self.g, self.z, self.t = n_kv, g, z, t
        self.half = n_kv // 8
        up = [2 + 4 * i for i in range(self.half)]
        self.reach = up + [-u for u in up]
        self.count = 2 * self.half
        self.steps = [(0, 1), (1, -1)]
        self.farthest_first = [
            k * self.half + i for i in reversed(range(self.half)) for k in (0, 1)
        ]
        self.nearest_first = list(reversed(self.farthest_first))

    def device(self, offset):
        return (self.g, lax.rem(self.z + offset + self.n_kv, self.n_kv), self.t)

    def near(self, i):
        last = () if i == self.count - 1 else ((3, 2 if i < self.half else -2),)
        return self.steps + list(last)

    def copy(self, src, dst, send, recv, offset):
        return pltpu.make_async_remote_copy(
            src_ref=src,
            dst_ref=dst,
            send_sem=send,
            recv_sem=recv,
            device_id=self.device(offset),
            device_id_type=MESH,
        )


def placing(per_slot, n_kv, seq, z):
    count = n_kv // 4
    half = count // 2
    shape = (n_kv * per_slot, n_kv * seq)
    m = lax.broadcasted_iota(jnp.int32, shape, 0)
    slot = m // per_slot
    i = slot % count
    group = slot // count
    reach = jnp.where(i < half, 2 + 4 * i, 4 * half - 2 - 4 * i)
    side = jnp.where(i < half, 2, -2)
    step = jnp.where(group == 0, 1, jnp.where(group == 1, -1, jnp.where(group == 2, 0, side)))
    offset = jnp.where(slot == n_kv - 1, 0, reach + step)
    owner = (z - offset + n_kv) % n_kv
    row = owner * seq + m % seq
    return (row == lax.broadcasted_iota(jnp.int32, shape, 1)).astype(bf16)


def kernel(
    dims,
    tok_ref,
    state_hbm,
    gain_ref,
    wq_hbm,
    wk_hbm,
    wv_hbm,
    wb_hbm,
    wd_hbm,
    alog_ref,
    dt_ref,
    hgain_ref,
    wo_hbm,
    mgain_ref,
    wu_hbm,
    wdn_hbm,
    out_ref,
    state_out,
    tok_all,
    tok_near,
    state_v,
    rhs1,
    wext,
    wo_v,
    wu_v,
    wdn_v,
    rs1,
    rs1_near,
    rs1_far_src,
    rs1_far,
    ag2_src,
    ag2,
    diag,
    att,
    mid_src,
    mid,
    rs3,
    rs3_far,
    sq_src,
    sq_far,
    ag4_src,
    ag4,
    fin_src,
    fin,
    gain_v,
    mgain_v,
    hgain_v,
    alog_v,
    dt_v,
    loc,
    tok_s,
    tok_r,
    rs1_ns,
    rs1_nr,
    rs1_fs,
    rs1_fr,
    win_s,
    win_r,
    ag2_s,
    ag2_r,
    att_s,
    att_r,
    rs3_s,
    rs3_r,
    sq_s,
    sq_r,
    mid_s,
    mid_r,
    ag4_s,
    ag4_r,
    fin_s,
    fin_r,
    sem_a,
    sem_b,
):
    n_kv, n_tp, seq, heads, width = dims
    g, z, t = lax.axis_index("grp"), lax.axis_index("kv"), lax.axis_index("tp")
    ex = Exchange(n_kv, g, z, t)
    count, half = ex.count, ex.half
    mine = tok_ref.shape[0]
    block = n_tp * mine
    all_rows = tok_ref.shape[1]
    head = hgain_v.shape[1]
    own = n_kv - 1

    def tp_peer(k):
        return (g, z, lax.rem(t + k, n_tp))

    barrier = pltpu.get_barrier_semaphore()
    for k in range(1, n_tp):
        pl.semaphore_signal(barrier, inc=1, device_id=tp_peer(k), device_id_type=MESH)
    for offset in (1, -1, 2, -2, 4, -4):
        pl.semaphore_signal(barrier, inc=1, device_id=ex.device(offset), device_id_type=MESH)

    def waiter(ref, send, recv):
        return pltpu.make_async_remote_copy(
            src_ref=ref,
            dst_ref=ref,
            send_sem=send,
            recv_sem=recv,
            device_id=tp_peer(1),
            device_id_type=MESH,
        )

    def fetch(src, dst, k):
        copy = pltpu.make_async_copy(src, dst, loc.at[k])
        copy.start()
        return copy

    got_tok = fetch(tok_ref, tok_all.at[t], 0)
    got_mgain = fetch(mgain_ref, mgain_v, 1)
    got_gain = fetch(gain_ref, gain_v, 2)
    lanes = wext.shape[2]
    at = pl.multiple_of((z * block // lanes) * lanes, lanes)
    got_ext = [
        fetch(wb_hbm.at[:, pl.ds(at, lanes)], wext.at[0], 3),
        fetch(wd_hbm.at[:, pl.ds(at, lanes)], wext.at[1], 4),
    ]
    for i, w in enumerate((wq_hbm, wk_hbm)):
        for h in range(heads):
            at = (i * heads + h) * block
            fetch(w.at[:, h * head : (h + 1) * head], rhs1.at[at : at + block, 0:head], 5)
    for h in range(heads):
        fetch(
            wv_hbm.at[:, h * head : (h + 1) * head],
            rhs1.at[h * block : (h + 1) * block, head : 2 * head],
            5,
        )
    whole = rhs1.at[0 : 3 * heads * block // 2]
    got_rhs1 = pltpu.make_async_copy(whole, whole, loc.at[5])
    got_small = [
        fetch(hgain_ref, hgain_v, 6),
        fetch(alog_ref, alog_v, 7),
        fetch(dt_ref, dt_v, 8),
    ]
    got_state = fetch(state_hbm, state_v, 9)
    parts = wu_v.shape[1] // (2 * head)
    wide = 2 * head
    kinds = heads * seq
    n_win = len(UP_WINDOW)
    out_wide = heads * head
    here_up, here_down = UP_WINDOW.index(0), DOWN_WINDOW.index(0)
    got_weights = [
        fetch(wo_hbm, wo_v.at[:, here_up * out_wide : (here_up + 1) * out_wide], 10),
        fetch(wu_hbm, wu_v.at[here_up * block : (here_up + 1) * block], 11),
        fetch(wdn_hbm, wdn_v.at[here_down * block : (here_down + 1) * block], 12),
    ]

    rhs1[heads * block :, head:] = jnp.zeros((heads * block, head), bf16)
    diag[...] = jnp.zeros(diag.shape, bf16)
    spread16 = placing(parts * seq, n_kv, seq, z)
    part_of_row = (
        lax.broadcasted_iota(jnp.int32, (n_kv * parts * seq, parts * block), 0) // seq
    ) % parts
    part_mask = part_of_row == (
        lax.broadcasted_iota(jnp.int32, (n_kv * parts * seq, parts * block), 1) // block
    )
    got_mgain.wait()
    gain_row = mgain_v[...].astype(f32).reshape(1, block)
    gain_row = jnp.concatenate([gain_row, jnp.zeros((1, all_rows - block), f32)], axis=1)
    tok_all[n_tp] = jnp.broadcast_to(gain_row, (mine, all_rows)).astype(bf16)
    got_gain.wait()
    gain = column_of(gain_v[...].astype(f32).reshape(1, block))
    got_tok.wait()

    pl.semaphore_wait(barrier, n_tp - 1 + 6)
    for offset in (4, -4):
        pl.semaphore_signal(sem_a, inc=1, device_id=ex.device(offset), device_id_type=MESH)

    def to_tp(dst, send, recv):
        for k in sorted(range(1, n_tp), key=lambda k: -min(k, n_tp - k)):
            peer = lax.rem(t + k, n_tp)
            pltpu.make_async_remote_copy(
                src_ref=dst.at[t],
                dst_ref=dst.at[t],
                send_sem=send,
                recv_sem=recv,
                device_id=(g, z, peer),
                device_id_type=MESH,
            ).start()
        return waiter(dst.at[0 : n_tp - 1], send, recv)

    pending = []
    tok_sent = to_tp(tok_all, tok_s, tok_r)
    pending.append(tok_sent)
    got_rhs1.wait()
    for copy in got_ext:
        copy.wait()
    odd = lax.rem(z, lanes // block) if lanes // block > 1 else 0
    pieces = []
    for i in range(2):
        piece = wext[i][:, 0:block]
        for k in range(1, lanes // block):
            piece = jnp.where(odd == k, wext[i][:, k * block : (k + 1) * block], piece)
        pieces.append(piece)
    n_heads = pieces[0].shape[0]
    wext_t = jnp.concatenate(
        pieces + [jnp.zeros((head - 2 * n_heads, block), bf16)], axis=0
    )
    at_row = lax.broadcasted_iota(jnp.int32, (head, block), 0)
    square_t = (at_row == 2 * n_heads).astype(bf16)
    ext_t = jnp.concatenate([wext_t, square_t], axis=1)

    tok_sent.wait_recv()
    pl.semaphore_wait(sem_a, 2)
    for offset in (8, -8):
        pl.semaphore_signal(sem_b, inc=1, device_id=ex.device(offset), device_id_type=MESH)

    def spread(x_t):
        stacked = jnp.concatenate([x_t] * parts, axis=0)
        rows = nt(spread16, stacked)
        return jnp.where(part_mask, rows, 0.0).astype(bf16)

    tok_t = tok_all[0:n_tp].astype(f32).reshape(block, all_rows)
    scaled_t = (tok_t * gain).astype(bf16)
    left = spread(scaled_t)
    both = jnp.concatenate([scaled_t, (tok_t * tok_t).astype(bf16)], axis=0)
    left2 = nt(spread16, both)
    left2 = jnp.where(part_of_row[:, 0 : 2 * block] >= heads, left2, 0.0).astype(bf16)
    product = nn(left, rhs1[...])
    extra = nt(left2, ext_t)
    product = jnp.concatenate([product[:, :head], product[:, head:] + extra], axis=1)
    rs1[...] = product.astype(bf16).reshape(rs1.shape)

    def to_far(chosen, src_of, dst, send, recv, sign):
        for i in chosen:
            ex.copy(src_of(i), dst.at[i], send, recv, sign * ex.reach[i]).start()

    def far_waiter(dst, send, recv):
        sent = waiter(dst, send, recv)
        pending.append(sent)
        return sent

    distant, close = ex.farthest_first[:count // 2], ex.farthest_first[count // 2 :]

    near_sent = []
    for part, chosen in enumerate((distant, close)):
        started = 0
        for i in chosen:
            for group, step in ex.near(i):
                k = group * count + i if group < 2 else 2 * count + i
                ex.copy(
                    rs1.at[group * count + i],
                    rs1_near.at[k],
                    rs1_ns.at[part],
                    rs1_nr.at[part],
                    -step,
                ).start()
                started += 1
        near_sent.append(waiter(rs1.at[0:started], rs1_ns.at[part], rs1_nr.at[part]))
    pending += near_sent

    def near_sums(chosen):
        for i in chosen:
            total = rs1[2 * count + i].astype(f32)
            for group, step in ex.near(i):
                k = group * count + i if group < 2 else 2 * count + i
                total += rs1_near[k].astype(f32)
            rs1_far_src[i] = total.astype(bf16)

    near_sent[0].wait_recv()
    near_sums(distant)
    pl.semaphore_wait(sem_b, 2)
    to_far(distant, lambda i: rs1_far_src.at[i], rs1_far, rs1_fs, rs1_fr, -1)
    near_sent[1].wait_recv()
    near_sums(close)
    to_far(close, lambda i: rs1_far_src.at[i], rs1_far, rs1_fs, rs1_fr, -1)
    far_sent = far_waiter(rs1_far, rs1_fs, rs1_fr)

    def to_window(src, dst_of, whole, k, offsets):
        for w, offset in enumerate(offsets):
            if offset:
                ex.copy(src, dst_of(w), win_s.at[k], win_r.at[k], -offset).start()
        sent = waiter(whole, win_s.at[k], win_r.at[k])
        pending.append(sent)
        return sent

    tok_window = to_window(
        tok_all, lambda w: tok_near.at[w], tok_near.at[0 : n_win - 1], 0, UP_WINDOW
    )
    wo_window = to_window(
        wo_hbm,
        lambda w: wo_v.at[:, w * out_wide : (w + 1) * out_wide],
        wo_v.at[:, 0 : (n_win - 1) * out_wide],
        1,
        UP_WINDOW,
    )

    got_state.wait()
    for copy in got_small:
        copy.wait()
    far_sent.wait_recv()
    sums = rs1[own].astype(f32)
    for i in range(count):
        sums += rs1_far[i].astype(f32)

    rows = heads * seq
    query_sum, key_sum = sums[:rows, :head], sums[rows:, :head]
    value_sum, extra = sums[:rows, head:], sums[rows:, head:]
    which = lax.broadcasted_iota(jnp.int32, (rows, head), 0) // seq
    lane = lax.broadcasted_iota(jnp.int32, (rows, head), 1)
    beta_sum = jnp.sum(
        jnp.where(lane == t * heads + which, extra, 0.0), axis=1, keepdims=True
    )
    decay_sum = jnp.sum(
        jnp.where(lane == n_heads + t * heads + which, extra, 0.0), axis=1, keepdims=True
    )
    square_sum = lanes_of(extra, 2 * n_heads)
    first = lax.rsqrt(square_sum / width + epsilon)
    query_pre, key_pre, value_pre = first * query_sum, first * key_sum, first * value_sum
    query = query_pre * lax.rsqrt(jnp.sum(query_pre * query_pre, axis=1, keepdims=True) + epsilon)
    key = key_pre * lax.rsqrt(jnp.sum(key_pre * key_pre, axis=1, keepdims=True) + epsilon)
    beta = jax.nn.sigmoid(first * beta_sum)
    which1 = lax.broadcasted_iota(jnp.int32, (rows, 1), 0) // seq
    a_logs, dt_biases = alog_v[...].reshape(1, heads), dt_v[...].reshape(1, heads)
    a_log = jnp.zeros((rows, 1), f32)
    dt_bias = jnp.zeros((rows, 1), f32)
    for h in range(heads):
        a_log = jnp.where(which1 == h, a_logs[:, h : h + 1], a_log)
        dt_bias = jnp.where(which1 == h, dt_biases[:, h : h + 1], dt_bias)
    logit = first * decay_sum + dt_bias
    softplus = jnp.maximum(logit, 0.0) + jnp.log1p(jnp.exp(-jnp.abs(logit)))
    decay = jnp.exp(-jnp.exp(a_log) * softplus)
    query_t, key_t = query.T, key.T
    key_reads, query_reads = [], []
    for k in range(rows):
        matrix = state_v[k % seq, k // seq]
        key_reads.append(jnp.sum(matrix * key_t[:, k : k + 1], axis=0, keepdims=True))
        query_reads.append(jnp.sum(matrix * query_t[:, k : k + 1], axis=0, keepdims=True))
    key_read = jnp.concatenate(key_reads, axis=0)
    query_read = jnp.concatenate(query_reads, axis=0)
    fresh = beta * (value_pre - decay * key_read)
    meeting = jnp.sum(query * key, axis=1, keepdims=True)
    reading = decay * query_read + meeting * fresh
    normed = (
        reading
        * lax.rsqrt(jnp.mean(reading * reading, axis=1, keepdims=True) + epsilon)
        * hgain_v[...]
    )

    ag2_src[...] = normed.astype(bf16)
    to_far(distant, lambda i: ag2_src, ag2, ag2_s, ag2_r, 1)
    for k in range(rows):
        matrix = state_v[k % seq, k // seq]
        state_out[k % seq, k // seq] = (
            decay[k : k + 1] * matrix + key_t[:, k : k + 1] * fresh[k : k + 1]
        )
    to_far(close, lambda i: ag2_src, ag2, ag2_s, ag2_r, 1)
    ag2_sent = far_waiter(ag2, ag2_s, ag2_r)
    wu_window = to_window(
        wu_hbm,
        lambda w: wu_v.at[w * block : (w + 1) * block],
        wu_v.at[0 : (n_win - 1) * block],
        2,
        UP_WINDOW,
    )
    wdn_window = to_window(
        wdn_hbm,
        lambda w: wdn_v.at[w * block : (w + 1) * block],
        wdn_v.at[0 : (n_win - 1) * block],
        3,
        DOWN_WINDOW,
    )

    def iota(shape, dim):
        return lax.broadcasted_iota(jnp.int32, shape, dim)

    def owner_row(slot, r):
        half = ex.half
        reach = jnp.where(slot < half, 2 + 4 * slot, 4 * half - 2 - 4 * slot)
        return (z - reach + n_kv) % n_kv * seq + r

    per_w = count * seq
    shape = (n_win * all_rows, all_rows)
    lane = iota(shape, 1)
    lane_owner = owner_row(lane % per_w // seq, lane % seq)
    window_pick = (
        (lane // per_w == iota(shape, 0) // all_rows) & (lane_owner == iota(shape, 0) % all_rows)
    ).astype(bf16)
    shape = (per_w, all_rows)
    place_rows = (owner_row(iota(shape, 0) // seq, iota(shape, 0) % seq) == iota(shape, 1)).astype(
        bf16
    )
    head_picks = []
    shape = (per_w, count * kinds)
    for h in range(heads):
        r0, c1 = iota(shape, 0), iota(shape, 1)
        head_picks.append(
            (
                (c1 // kinds == r0 // seq) & (c1 % seq == r0 % seq) & (c1 // seq % heads == h)
            ).astype(bf16)
        )
    shape = (count * parts * seq, all_rows)
    r0, c1 = iota(shape, 0), iota(shape, 1)
    spread_rows = (
        (r0 // (parts * seq) == c1 % per_w // seq) & (r0 % seq == c1 % seq)
    ).astype(bf16)
    shape = (per_w, count * parts * seq)
    r0, c1 = iota(shape, 0), iota(shape, 1)
    part_picks = [
        (
            (c1 // (parts * seq) == r0 // seq) & (c1 % seq == r0 % seq) & (c1 // seq % parts == j)
        ).astype(bf16)
        for j in range(parts)
    ]
    tok_window.wait_recv()
    token_parts = []
    mixer_gain = jnp.zeros((block, all_rows), f32)
    lane = iota((block, all_rows), 1)
    for w, offset in enumerate(UP_WINDOW):
        source = tok_near.at[w] if offset else tok_all
        token_parts.append(source[0:n_tp].astype(f32).reshape(block, all_rows).astype(bf16))
        column = column_of(source[n_tp].astype(f32)[0:1, 0:block])
        mixer_gain = jnp.where(lane // per_w == w, column, mixer_gain)
    token_w = nn(jnp.concatenate(token_parts, axis=1), window_pick)
    for copy in got_weights:
        copy.wait()
    ag2_sent.wait_recv()
    wo_window.wait_recv()
    everyone = ag2[...].astype(f32).reshape(count * kinds, head).astype(bf16)
    for h in range(heads):
        picked = nn(head_picks[h], everyone).astype(bf16)
        for w in range(n_win):
            at = w * out_wide + h * head
            diag[w * per_w : (w + 1) * per_w, at : at + head] = picked
    att[t] = nt(wo_v[...], diag[...]).astype(bf16)
    att_sent = to_tp(att, att_s, att_r)
    pending.append(att_sent)
    att_sent.wait_recv()
    wu_window.wait_recv()

    attended = att[0].astype(f32)
    for k in range(1, n_tp):
        attended += att[k].astype(f32)
    middle_b = (token_w + attended).astype(bf16)
    middle = middle_b.astype(f32)
    sq_src[...] = jnp.sum(middle * middle, axis=0, keepdims=True)
    to_far(ex.farthest_first, lambda i: sq_src, sq_far, sq_s, sq_r, -1)
    sq_sent = far_waiter(sq_far, sq_s, sq_r)
    scaled = jnp.concatenate([middle * mixer_gain] * n_win, axis=0)
    shape = scaled.shape
    scaled = jnp.where(iota(shape, 1) // per_w == iota(shape, 0) // block, scaled, 0.0)
    left = nt(spread_rows, scaled.astype(bf16))
    part = iota(left.shape, 0) // seq % parts
    product = jnp.zeros((left.shape[0], wide), f32)
    for j in range(parts):
        product += nn(
            jnp.where(part == j, left, 0.0).astype(bf16), wu_v[:, j * wide : (j + 1) * wide]
        )
    rs3[...] = product.astype(bf16).reshape(rs3.shape)
    to_far(distant, lambda i: rs3.at[i], rs3_far, rs3_s, rs3_r, -1)
    for w, offset in enumerate(UP_WINDOW):
        placed = nt(middle_b, window_pick[w * all_rows : (w + 1) * all_rows]).astype(bf16)
        mid_src[w] = placed.reshape(n_tp, mine, all_rows)
        if not offset:
            mid[w] = mid_src[w, t]
    to_far(close, lambda i: rs3.at[i], rs3_far, rs3_s, rs3_r, -1)
    rs3_sent = far_waiter(rs3_far, rs3_s, rs3_r)
    for w, offset in enumerate(UP_WINDOW):
        if offset:
            ex.copy(mid_src.at[w, t], mid.at[w], mid_s, mid_r, offset).start()
    mid_sent = waiter(mid.at[0 : n_win - 1], mid_s, mid_r)
    pending.append(mid_sent)
    sq_sent.wait_recv()
    lane = iota((1, all_rows), 1)
    squares = jnp.zeros((1, all_rows), f32)
    for i in range(count):
        squares += jnp.where(lane % per_w // seq == i, sq_far[i], 0.0)
    shape = (parts * seq, all_rows)
    squares = jnp.sum(
        jnp.where(iota(shape, 1) % seq == iota(shape, 0) % seq, squares, 0.0),
        axis=1,
        keepdims=True,
    )
    second = lax.rsqrt(squares / width + epsilon)
    up = jnp.zeros((parts * seq, wide), f32)
    rs3_sent.wait_recv()
    for i in range(count):
        up += rs3_far[i].astype(f32)
    ag4_src[...] = jnp.square(jnp.maximum(second * up, 0.0)).astype(bf16)

    to_far(distant, lambda i: ag4_src, ag4, ag4_s, ag4_r, 1)
    wdn_window.wait_recv()
    mid_sent.wait_recv()
    middle = mid[0].astype(f32)
    for w in range(1, n_win):
        middle += mid[w].astype(f32)
    to_far(close, lambda i: ag4_src, ag4, ag4_s, ag4_r, 1)
    ag4_sent = far_waiter(ag4, ag4_s, ag4_r)
    ag4_sent.wait_recv()
    everyone = ag4[...].reshape(count * parts * seq, wide)
    picked = jnp.concatenate(
        [nn(part_picks[j], everyone).astype(bf16) for j in range(parts)], axis=1
    )
    lowered_part = nt(wdn_v[...], picked).astype(bf16)
    fin_src[...] = nn(lowered_part, place_rows).astype(bf16).reshape(fin_src.shape)
    for w, offset in sorted(enumerate(DOWN_WINDOW), key=lambda pair: -abs(pair[1])):
        row = lax.rem(z + offset + n_kv, n_kv)
        for k in sorted(range(n_tp), key=lambda k: -min(k, n_tp - k)):
            if offset == 0 and k == 0:
                fin[w * n_tp + t] = fin_src[w * n_tp + t]
                continue
            peer = lax.rem(t + k, n_tp)
            pltpu.make_async_remote_copy(
                src_ref=fin_src.at[w * n_tp + peer],
                dst_ref=fin.at[w * n_tp + t],
                send_sem=fin_s,
                recv_sem=fin_r,
                device_id=(g, row, peer),
                device_id_type=MESH,
            ).start()
    fin_sent = waiter(fin.at[0 : n_win * n_tp - 1], fin_s, fin_r)
    pending.append(fin_sent)
    fin_sent.wait_recv()
    lowered = jnp.sum(fin[...].astype(f32), axis=0)
    out_ref[...] = (middle + lowered).astype(bf16)
    for copy in pending:
        copy.wait_send()


def solution(mesh):
    n_kv, n_tp = mesh.shape["kv"], mesh.shape["tp"]

    def local(
        tokens,
        state,
        norm_gain,
        w_query,
        w_key,
        w_value,
        w_beta,
        w_decay,
        a_log,
        dt_bias,
        head_gain,
        w_out,
        mixer_gain,
        w_up,
        w_down,
    ):
        seq, heads, head = state.shape[:3]
        rows, mine = tokens.shape
        block = w_query.shape[0]
        parts = w_up.shape[1] // (2 * head)
        wide = w_up.shape[1] // parts
        count = n_kv // 4
        dims = (n_kv, n_tp, seq, heads, block * n_kv)
        vmem, hbm = (
            pl.BlockSpec(memory_space=pltpu.VMEM),
            pl.BlockSpec(memory_space=pltpu.HBM),
        )
        dma = pltpu.SemaphoreType.DMA
        blocks = (parts * seq, wide)
        near = (3 * count - 1,)
        n_win = len(UP_WINDOW)
        scratch = [
            pltpu.VMEM((n_tp + 1, mine, rows), bf16),
            pltpu.VMEM((n_win, n_tp + 1, mine, rows), bf16),
            pltpu.VMEM(state.shape, f32),
            pltpu.VMEM((2 * heads * block, 2 * head), bf16),
            pltpu.VMEM((2, w_beta.shape[1], head), bf16),
            pltpu.VMEM((block, n_win * heads * head), bf16),
            pltpu.VMEM((n_win * block, w_up.shape[1]), bf16),
            pltpu.VMEM((n_win * block, w_down.shape[0]), bf16),
            pltpu.VMEM((n_kv, *blocks), bf16),
            pltpu.VMEM((*near, *blocks), bf16),
            pltpu.VMEM((count, *blocks), bf16),
            pltpu.VMEM((count, *blocks), bf16),
            pltpu.VMEM((heads * seq, head), bf16),
            pltpu.VMEM((count, heads * seq, head), bf16),
            pltpu.VMEM((rows, n_win * heads * head), bf16),
            pltpu.VMEM((n_tp, block, rows), bf16),
            pltpu.VMEM((n_win, n_tp, mine, rows), bf16),
            pltpu.VMEM((n_win, mine, rows), bf16),
            pltpu.VMEM((count, *blocks), bf16),
            pltpu.VMEM((count, *blocks), bf16),
            pltpu.VMEM((1, rows), f32),
            pltpu.VMEM((count, 1, rows), f32),
            pltpu.VMEM(blocks, bf16),
            pltpu.VMEM((count, *blocks), bf16),
            pltpu.VMEM((n_win * n_tp, mine, rows), bf16),
            pltpu.VMEM((n_win * n_tp, mine, rows), bf16),
            pltpu.VMEM(norm_gain.shape, bf16),
            pltpu.VMEM(mixer_gain.shape, bf16),
            pltpu.VMEM((1, head), f32),
            pltpu.VMEM(a_log.shape, f32),
            pltpu.VMEM(dt_bias.shape, f32),
            dma((13,)),
            dma,
            dma,
            dma((2,)),
            dma((2,)),
            dma,
            dma,
            dma((4,)),
            dma((4,)),
            *[dma] * 14,
            pltpu.SemaphoreType.REGULAR,
            pltpu.SemaphoreType.REGULAR,
        ]
        mixed_t, new_state = pl.pallas_call(
            functools.partial(kernel, dims),
            out_shape=(
                jax.ShapeDtypeStruct((mine, rows), bf16),
                jax.ShapeDtypeStruct(state.shape, f32),
            ),
            in_specs=[hbm] * 15,
            out_specs=(vmem, vmem),
            scratch_shapes=scratch,
            compiler_params=pltpu.CompilerParams(collective_id=0, has_side_effects=True, vmem_limit_bytes=32 * 2**20),
        )(
            *[
                pltpu.with_memory_space_constraint(x, pltpu.HBM)
                for x in (
                    tokens.T,
                    state,
                    norm_gain,
                    w_query,
                    w_key,
                    w_value,
                    w_beta.T,
                    w_decay.T,
                    a_log,
                    dt_bias,
                    head_gain.reshape(1, head),
                    w_out.T,
                    mixer_gain,
                    w_up,
                    w_down.T,
                )
            ]
        )
        return mixed_t.T, new_state

    return jax.shard_map(
        local,
        mesh=mesh,
        in_specs=(
            P("grp", ("kv", "tp")),
            P(("grp", "kv"), "tp", None, None),
            P("kv"),
            P("kv", "tp"),
            P("kv", "tp"),
            P("kv", "tp"),
            P(),
            P(),
            P("tp"),
            P("tp"),
            P(),
            P("tp", "kv"),
            P("kv"),
            P("kv", "tp"),
            P("tp", "kv"),
        ),
        out_specs=(P("grp", ("kv", "tp")), P(("grp", "kv"), "tp", None, None)),
        check_vma=False,
    )
```

```python
import functools

import jax
import jax.numpy as jnp
from jax import lax
from jax.experimental import pallas as pl
from jax.experimental.pallas import tpu as pltpu
from jax.sharding import PartitionSpec as P

MESH = pl.DeviceIdType.MESH
epsilon = 1e-06
f32 = jnp.float32
bf16 = jnp.bfloat16


def nn(a, b):
    return jnp.dot(a, b, preferred_element_type=f32)


def nt(a, b):
    return lax.dot_general(a, b, (((1,), (1,)), ((), ())), preferred_element_type=f32)


def exact_nn(a, onehot):
    high = a.astype(bf16)
    low = (a - high.astype(f32)).astype(bf16)
    return nn(high, onehot) + nn(low, onehot)


def lanes_of(x, lane):
    at = lax.broadcasted_iota(jnp.int32, x.shape, 1)
    return jnp.sum(jnp.where(at == lane, x, 0.0), axis=1, keepdims=True)


def column_of(row):
    n = row.shape[1]
    eye = lax.broadcasted_iota(jnp.int32, (n, n), 0) == lax.broadcasted_iota(
        jnp.int32, (n, n), 1
    )
    return jnp.sum(jnp.where(eye, row, 0.0), axis=1, keepdims=True)


UP_WINDOW = (-1, 0, 1, 2)
DOWN_WINDOW = (-2, -1, 0, 1)


def reach_of(i, n_kv, where=jnp.where):
    q, top = n_kv // 16, n_kv // 2 - 2
    return where(i < q, top - 4 * i, where(i < 2 * q, -2 - 4 * i, top + 4 * q - 4 * i))


class Exchange:
    def __init__(self, n_kv, g, z, t):
        self.n_kv, self.g, self.z, self.t = n_kv, g, z, t
        self.count = n_kv // 4
        self.reach = [
            reach_of(i, n_kv, lambda c, x, y: x if c else y) for i in range(self.count)
        ]
        self.farthest_first = sorted(range(self.count), key=lambda i: -abs(self.reach[i]))
        self.own = 3 * self.count + n_kv // 8 - 1

    def device(self, offset):
        return (self.g, lax.rem(self.z + offset + self.n_kv, self.n_kv), self.t)

    def near_runs(self):
        q = self.n_kv // 16
        farther = [(3, 0, q, 2), (3, q, q - 1, -2), (0, 0, 2 * q, 1), (1, 0, 2 * q, -1)]
        closer = [
            (3, 2 * q, q, 2),
            (3, 3 * q, q, -2),
            (0, 2 * q, 2 * q, 1),
            (1, 2 * q, 2 * q, -1),
        ]
        return farther, closer

    def copy(self, src, dst, send, recv, offset):
        return pltpu.make_async_remote_copy(
            src_ref=src,
            dst_ref=dst,
            send_sem=send,
            recv_sem=recv,
            device_id=self.device(offset),
            device_id_type=MESH,
        )


def placing(per_slot, n_kv, seq, z):
    count = n_kv // 4
    shape = (n_kv * per_slot, n_kv * seq)
    m = lax.broadcasted_iota(jnp.int32, shape, 0)
    slot = m // per_slot
    i = slot % count
    group = slot // count
    reach = reach_of(i, n_kv)
    side = jnp.where(reach > 0, 2, -2)
    step = jnp.where(group == 0, 1, jnp.where(group == 1, -1, jnp.where(group == 2, 0, side)))
    offset = jnp.where(slot == 3 * count + n_kv // 8 - 1, 0, reach + step)
    owner = (z - offset + n_kv) % n_kv
    row = owner * seq + m % seq
    return (row == lax.broadcasted_iota(jnp.int32, shape, 1)).astype(bf16)


def kernel(
    dims,
    tok_ref,
    state_hbm,
    gain_ref,
    wq_hbm,
    wk_hbm,
    wv_hbm,
    wb_hbm,
    wd_hbm,
    alog_ref,
    dt_ref,
    hgain_ref,
    wo_hbm,
    mgain_ref,
    wu_hbm,
    wdn_hbm,
    out_ref,
    state_out,
    tok_all,
    tok_near,
    state_v,
    rhs1,
    wext,
    wo_v,
    wu_v,
    wdn_v,
    rs1,
    rs1_near,
    rs1_far_src,
    rs1_far,
    ag2_src,
    ag2,
    diag,
    att,
    mid_src,
    mid,
    rs3,
    rs3_far,
    sq_src,
    sq_far,
    ag4_src,
    ag4,
    fin_src,
    fin,
    gain_v,
    mgain_v,
    hgain_v,
    alog_v,
    dt_v,
    loc,
    tok_s,
    tok_r,
    rs1_ns,
    rs1_nr,
    rs1_fs,
    rs1_fr,
    win_s,
    win_r,
    ag2_s,
    ag2_r,
    att_s,
    att_r,
    rs3_s,
    rs3_r,
    sq_s,
    sq_r,
    mid_s,
    mid_r,
    ag4_s,
    ag4_r,
    fin_s,
    fin_r,
    sem_a,
    sem_b,
):
    n_kv, n_tp, seq, heads, width = dims
    g, z, t = lax.axis_index("grp"), lax.axis_index("kv"), lax.axis_index("tp")
    ex = Exchange(n_kv, g, z, t)
    count = ex.count
    mine = tok_ref.shape[0]
    block = n_tp * mine
    all_rows = tok_ref.shape[1]
    head = hgain_v.shape[1]
    own = ex.own

    def tp_peer(k):
        return (g, z, lax.rem(t + k, n_tp))

    barrier = pltpu.get_barrier_semaphore()
    for k in range(1, n_tp):
        pl.semaphore_signal(barrier, inc=1, device_id=tp_peer(k), device_id_type=MESH)
    for offset in (1, -1, 2, -2, 4, -4):
        pl.semaphore_signal(barrier, inc=1, device_id=ex.device(offset), device_id_type=MESH)

    def waiter(ref, send, recv):
        return pltpu.make_async_remote_copy(
            src_ref=ref,
            dst_ref=ref,
            send_sem=send,
            recv_sem=recv,
            device_id=tp_peer(1),
            device_id_type=MESH,
        )

    def fetch(src, dst, k):
        copy = pltpu.make_async_copy(src, dst, loc.at[k])
        copy.start()
        return copy

    got_tok = fetch(tok_ref, tok_all.at[t], 0)
    got_mgain = fetch(mgain_ref, mgain_v, 1)
    got_gain = fetch(gain_ref, gain_v, 2)
    lanes = wext.shape[2]
    at = pl.multiple_of((z * block // lanes) * lanes, lanes)
    got_ext = [
        fetch(wb_hbm.at[:, pl.ds(at, lanes)], wext.at[0], 3),
        fetch(wd_hbm.at[:, pl.ds(at, lanes)], wext.at[1], 4),
    ]
    for i, w in enumerate((wq_hbm, wk_hbm)):
        for h in range(heads):
            at = (i * heads + h) * block
            fetch(w.at[:, h * head : (h + 1) * head], rhs1.at[at : at + block, 0:head], 5)
    for h in range(heads):
        fetch(
            wv_hbm.at[:, h * head : (h + 1) * head],
            rhs1.at[h * block : (h + 1) * block, head : 2 * head],
            5,
        )
    whole = rhs1.at[0 : 3 * heads * block // 2]
    got_rhs1 = pltpu.make_async_copy(whole, whole, loc.at[5])
    got_small = [
        fetch(hgain_ref, hgain_v, 6),
        fetch(alog_ref, alog_v, 7),
        fetch(dt_ref, dt_v, 8),
    ]
    got_state = fetch(state_hbm, state_v, 9)
    parts = wu_v.shape[1] // (2 * head)
    wide = 2 * head
    kinds = heads * seq
    n_win = len(UP_WINDOW)
    out_wide = heads * head
    here_up, here_down = UP_WINDOW.index(0), DOWN_WINDOW.index(0)
    got_weights = [
        fetch(wo_hbm, wo_v.at[:, here_up * out_wide : (here_up + 1) * out_wide], 10),
        fetch(wu_hbm, wu_v.at[here_up * block : (here_up + 1) * block], 11),
        fetch(wdn_hbm, wdn_v.at[here_down * block : (here_down + 1) * block], 12),
    ]

    rhs1[heads * block :, head:] = jnp.zeros((heads * block, head), bf16)
    diag[...] = jnp.zeros(diag.shape, bf16)
    spread16 = placing(parts * seq, n_kv, seq, z)
    part_of_row = (
        lax.broadcasted_iota(jnp.int32, (n_kv * parts * seq, parts * block), 0) // seq
    ) % parts
    part_mask = part_of_row == (
        lax.broadcasted_iota(jnp.int32, (n_kv * parts * seq, parts * block), 1) // block
    )
    got_mgain.wait()
    gain_row = mgain_v[...].astype(f32).reshape(1, block)
    gain_row = jnp.concatenate([gain_row, jnp.zeros((1, all_rows - block), f32)], axis=1)
    tok_all[n_tp] = jnp.broadcast_to(gain_row, (mine, all_rows)).astype(bf16)
    got_gain.wait()
    gain = column_of(gain_v[...].astype(f32).reshape(1, block))
    got_tok.wait()

    pl.semaphore_wait(barrier, n_tp - 1 + 6)
    for offset in (4, -4):
        pl.semaphore_signal(sem_a, inc=1, device_id=ex.device(offset), device_id_type=MESH)

    def to_tp(dst, send, recv):
        for k in sorted(range(1, n_tp), key=lambda k: -min(k, n_tp - k)):
            peer = lax.rem(t + k, n_tp)
            pltpu.make_async_remote_copy(
                src_ref=dst.at[t],
                dst_ref=dst.at[t],
                send_sem=send,
                recv_sem=recv,
                device_id=(g, z, peer),
                device_id_type=MESH,
            ).start()
        return waiter(dst.at[0 : n_tp - 1], send, recv)

    pending = []
    tok_sent = to_tp(tok_all, tok_s, tok_r)
    pending.append(tok_sent)
    got_rhs1.wait()
    for copy in got_ext:
        copy.wait()
    odd = lax.rem(z, lanes // block) if lanes // block > 1 else 0
    pieces = []
    for i in range(2):
        piece = wext[i][:, 0:block]
        for k in range(1, lanes // block):
            piece = jnp.where(odd == k, wext[i][:, k * block : (k + 1) * block], piece)
        pieces.append(piece)
    n_heads = pieces[0].shape[0]
    wext_t = jnp.concatenate(
        pieces + [jnp.zeros((head - 2 * n_heads, block), bf16)], axis=0
    )
    at_row = lax.broadcasted_iota(jnp.int32, (head, block), 0)
    square_t = (at_row == 2 * n_heads).astype(bf16)
    ext_t = jnp.concatenate([wext_t, square_t], axis=1)

    tok_sent.wait_recv()
    pl.semaphore_wait(sem_a, 2)
    for offset in (8, -8):
        pl.semaphore_signal(sem_b, inc=1, device_id=ex.device(offset), device_id_type=MESH)

    def spread(x_t):
        stacked = jnp.concatenate([x_t] * parts, axis=0)
        rows = nt(spread16, stacked)
        return jnp.where(part_mask, rows, 0.0).astype(bf16)

    tok_t = tok_all[0:n_tp].astype(f32).reshape(block, all_rows)
    scaled_t = (tok_t * gain).astype(bf16)
    left = spread(scaled_t)
    both = jnp.concatenate([scaled_t, (tok_t * tok_t).astype(bf16)], axis=0)
    left2 = nt(spread16, both)
    left2 = jnp.where(part_of_row[:, 0 : 2 * block] >= heads, left2, 0.0).astype(bf16)
    product = nn(left, rhs1[...])
    extra = nt(left2, ext_t)
    product = jnp.concatenate([product[:, :head], product[:, head:] + extra], axis=1)
    rs1[...] = product.astype(bf16).reshape(rs1.shape)

    def to_far(chosen, src_of, dst, send, recv, sign):
        for i in chosen:
            ex.copy(src_of(i), dst.at[i], send, recv, sign * ex.reach[i]).start()

    def far_waiter(dst, send, recv):
        sent = waiter(dst, send, recv)
        pending.append(sent)
        return sent

    distant, close = ex.farthest_first[:count // 2], ex.farthest_first[count // 2 :]

    near_sent = []
    for part, runs in enumerate(ex.near_runs()):
        for group, first, blocks, step in runs:
            at, to = group * count + first, min(group, 2) * count + first
            ex.copy(
                rs1.at[at : at + blocks],
                rs1_near.at[to : to + blocks],
                rs1_ns.at[part],
                rs1_nr.at[part],
                -step,
            ).start()
        blocks = sum(run[2] for run in runs)
        near_sent.append(waiter(rs1.at[0:blocks], rs1_ns.at[part], rs1_nr.at[part]))
    pending += near_sent

    def near_sums(chosen):
        for i in chosen:
            total = rs1[2 * count + i].astype(f32)
            for k in range(3):
                if k < 2 or 3 * count + i != own:
                    total += rs1_near[k * count + i].astype(f32)
            rs1_far_src[i] = total.astype(bf16)

    near_sent[0].wait_recv()
    near_sums(distant)
    pl.semaphore_wait(sem_b, 2)
    to_far(distant, lambda i: rs1_far_src.at[i], rs1_far, rs1_fs, rs1_fr, -1)
    near_sent[1].wait_recv()
    near_sums(close)
    to_far(close, lambda i: rs1_far_src.at[i], rs1_far, rs1_fs, rs1_fr, -1)
    far_sent = far_waiter(rs1_far, rs1_fs, rs1_fr)

    def to_window(src, dst_of, whole, k, offsets):
        for w, offset in enumerate(offsets):
            if offset:
                ex.copy(src, dst_of(w), win_s.at[k], win_r.at[k], -offset).start()
        sent = waiter(whole, win_s.at[k], win_r.at[k])
        pending.append(sent)
        return sent

    tok_window = to_window(
        tok_all, lambda w: tok_near.at[w], tok_near.at[0 : n_win - 1], 0, UP_WINDOW
    )
    wo_window = to_window(
        wo_hbm,
        lambda w: wo_v.at[:, w * out_wide : (w + 1) * out_wide],
        wo_v.at[:, 0 : (n_win - 1) * out_wide],
        1,
        UP_WINDOW,
    )

    got_state.wait()
    for copy in got_small:
        copy.wait()
    far_sent.wait_recv()
    sums = rs1[own].astype(f32)
    for i in range(count):
        sums += rs1_far[i].astype(f32)

    rows = heads * seq
    query_sum, key_sum = sums[:rows, :head], sums[rows:, :head]
    value_sum, extra = sums[:rows, head:], sums[rows:, head:]
    which = lax.broadcasted_iota(jnp.int32, (rows, head), 0) // seq
    lane = lax.broadcasted_iota(jnp.int32, (rows, head), 1)
    beta_sum = jnp.sum(
        jnp.where(lane == t * heads + which, extra, 0.0), axis=1, keepdims=True
    )
    decay_sum = jnp.sum(
        jnp.where(lane == n_heads + t * heads + which, extra, 0.0), axis=1, keepdims=True
    )
    square_sum = lanes_of(extra, 2 * n_heads)
    first = lax.rsqrt(square_sum / width + epsilon)
    query_pre, key_pre, value_pre = first * query_sum, first * key_sum, first * value_sum
    query = query_pre * lax.rsqrt(jnp.sum(query_pre * query_pre, axis=1, keepdims=True) + epsilon)
    key = key_pre * lax.rsqrt(jnp.sum(key_pre * key_pre, axis=1, keepdims=True) + epsilon)
    beta = jax.nn.sigmoid(first * beta_sum)
    which1 = lax.broadcasted_iota(jnp.int32, (rows, 1), 0) // seq
    a_logs, dt_biases = alog_v[...].reshape(1, heads), dt_v[...].reshape(1, heads)
    a_log = jnp.zeros((rows, 1), f32)
    dt_bias = jnp.zeros((rows, 1), f32)
    for h in range(heads):
        a_log = jnp.where(which1 == h, a_logs[:, h : h + 1], a_log)
        dt_bias = jnp.where(which1 == h, dt_biases[:, h : h + 1], dt_bias)
    logit = first * decay_sum + dt_bias
    softplus = jnp.maximum(logit, 0.0) + jnp.log1p(jnp.exp(-jnp.abs(logit)))
    decay = jnp.exp(-jnp.exp(a_log) * softplus)
    query_t, key_t = query.T, key.T
    key_reads, query_reads = [], []
    for k in range(rows):
        matrix = state_v[k % seq, k // seq]
        key_reads.append(jnp.sum(matrix * key_t[:, k : k + 1], axis=0, keepdims=True))
        query_reads.append(jnp.sum(matrix * query_t[:, k : k + 1], axis=0, keepdims=True))
    key_read = jnp.concatenate(key_reads, axis=0)
    query_read = jnp.concatenate(query_reads, axis=0)
    fresh = beta * (value_pre - decay * key_read)
    meeting = jnp.sum(query * key, axis=1, keepdims=True)
    reading = decay * query_read + meeting * fresh
    normed = (
        reading
        * lax.rsqrt(jnp.mean(reading * reading, axis=1, keepdims=True) + epsilon)
        * hgain_v[...]
    )

    ag2_src[...] = normed.astype(bf16)
    to_far(distant, lambda i: ag2_src, ag2, ag2_s, ag2_r, 1)
    for k in range(rows):
        matrix = state_v[k % seq, k // seq]
        state_out[k % seq, k // seq] = (
            decay[k : k + 1] * matrix + key_t[:, k : k + 1] * fresh[k : k + 1]
        )
    to_far(close, lambda i: ag2_src, ag2, ag2_s, ag2_r, 1)
    ag2_sent = far_waiter(ag2, ag2_s, ag2_r)
    wu_window = to_window(
        wu_hbm,
        lambda w: wu_v.at[w * block : (w + 1) * block],
        wu_v.at[0 : (n_win - 1) * block],
        2,
        UP_WINDOW,
    )
    wdn_window = to_window(
        wdn_hbm,
        lambda w: wdn_v.at[w * block : (w + 1) * block],
        wdn_v.at[0 : (n_win - 1) * block],
        3,
        DOWN_WINDOW,
    )

    def iota(shape, dim):
        return lax.broadcasted_iota(jnp.int32, shape, dim)

    def owner_row(slot, r):
        return (z - reach_of(slot, n_kv) + n_kv) % n_kv * seq + r

    per_w = count * seq
    shape = (n_win * all_rows, all_rows)
    lane = iota(shape, 1)
    lane_owner = owner_row(lane % per_w // seq, lane % seq)
    window_pick = (
        (lane // per_w == iota(shape, 0) // all_rows) & (lane_owner == iota(shape, 0) % all_rows)
    ).astype(bf16)
    shape = (per_w, all_rows)
    place_rows = (owner_row(iota(shape, 0) // seq, iota(shape, 0) % seq) == iota(shape, 1)).astype(
        bf16
    )
    head_picks = []
    shape = (per_w, count * kinds)
    for h in range(heads):
        r0, c1 = iota(shape, 0), iota(shape, 1)
        head_picks.append(
            (
                (c1 // kinds == r0 // seq) & (c1 % seq == r0 % seq) & (c1 // seq % heads == h)
            ).astype(bf16)
        )
    shape = (count * parts * seq, all_rows)
    r0, c1 = iota(shape, 0), iota(shape, 1)
    spread_rows = (
        (r0 // (parts * seq) == c1 % per_w // seq) & (r0 % seq == c1 % seq)
    ).astype(bf16)
    shape = (per_w, count * parts * seq)
    r0, c1 = iota(shape, 0), iota(shape, 1)
    part_picks = [
        (
            (c1 // (parts * seq) == r0 // seq) & (c1 % seq == r0 % seq) & (c1 // seq % parts == j)
        ).astype(bf16)
        for j in range(parts)
    ]
    tok_window.wait_recv()
    token_parts = []
    mixer_gain = jnp.zeros((block, all_rows), f32)
    lane = iota((block, all_rows), 1)
    for w, offset in enumerate(UP_WINDOW):
        source = tok_near.at[w] if offset else tok_all
        token_parts.append(source[0:n_tp].astype(f32).reshape(block, all_rows).astype(bf16))
        column = column_of(source[n_tp].astype(f32)[0:1, 0:block])
        mixer_gain = jnp.where(lane // per_w == w, column, mixer_gain)
    token_w = nn(jnp.concatenate(token_parts, axis=1), window_pick)
    for copy in got_weights:
        copy.wait()
    ag2_sent.wait_recv()
    wo_window.wait_recv()
    everyone = ag2[...].astype(f32).reshape(count * kinds, head).astype(bf16)
    for h in range(heads):
        picked = nn(head_picks[h], everyone).astype(bf16)
        for w in range(n_win):
            at = w * out_wide + h * head
            diag[w * per_w : (w + 1) * per_w, at : at + head] = picked
    att[t] = nt(wo_v[...], diag[...]).astype(bf16)
    att_sent = to_tp(att, att_s, att_r)
    pending.append(att_sent)
    att_sent.wait_recv()
    wu_window.wait_recv()

    attended = att[0].astype(f32)
    for k in range(1, n_tp):
        attended += att[k].astype(f32)
    middle_b = (token_w + attended).astype(bf16)
    middle = middle_b.astype(f32)
    sq_src[...] = jnp.sum(middle * middle, axis=0, keepdims=True)
    to_far(ex.farthest_first, lambda i: sq_src, sq_far, sq_s, sq_r, -1)
    sq_sent = far_waiter(sq_far, sq_s, sq_r)
    scaled = jnp.concatenate([middle * mixer_gain] * n_win, axis=0)
    shape = scaled.shape
    scaled = jnp.where(iota(shape, 1) // per_w == iota(shape, 0) // block, scaled, 0.0)
    left = nt(spread_rows, scaled.astype(bf16))
    part = iota(left.shape, 0) // seq % parts
    product = jnp.zeros((left.shape[0], wide), f32)
    for j in range(parts):
        product += nn(
            jnp.where(part == j, left, 0.0).astype(bf16), wu_v[:, j * wide : (j + 1) * wide]
        )
    rs3[...] = product.astype(bf16).reshape(rs3.shape)
    to_far(distant, lambda i: rs3.at[i], rs3_far, rs3_s, rs3_r, -1)
    for w, offset in enumerate(UP_WINDOW):
        placed = nt(middle_b, window_pick[w * all_rows : (w + 1) * all_rows]).astype(bf16)
        mid_src[w] = placed.reshape(n_tp, mine, all_rows)
        if not offset:
            mid[w] = mid_src[w, t]
    to_far(close, lambda i: rs3.at[i], rs3_far, rs3_s, rs3_r, -1)
    rs3_sent = far_waiter(rs3_far, rs3_s, rs3_r)
    for w, offset in enumerate(UP_WINDOW):
        if offset:
            ex.copy(mid_src.at[w, t], mid.at[w], mid_s, mid_r, offset).start()
    mid_sent = waiter(mid.at[0 : n_win - 1], mid_s, mid_r)
    pending.append(mid_sent)
    sq_sent.wait_recv()
    lane = iota((1, all_rows), 1)
    squares = jnp.zeros((1, all_rows), f32)
    for i in range(count):
        squares += jnp.where(lane % per_w // seq == i, sq_far[i], 0.0)
    shape = (parts * seq, all_rows)
    squares = jnp.sum(
        jnp.where(iota(shape, 1) % seq == iota(shape, 0) % seq, squares, 0.0),
        axis=1,
        keepdims=True,
    )
    second = lax.rsqrt(squares / width + epsilon)
    up = jnp.zeros((parts * seq, wide), f32)
    rs3_sent.wait_recv()
    for i in range(count):
        up += rs3_far[i].astype(f32)
    ag4_src[...] = jnp.square(jnp.maximum(second * up, 0.0)).astype(bf16)

    to_far(distant, lambda i: ag4_src, ag4, ag4_s, ag4_r, 1)
    wdn_window.wait_recv()
    mid_sent.wait_recv()
    middle = mid[0].astype(f32)
    for w in range(1, n_win):
        middle += mid[w].astype(f32)
    to_far(close, lambda i: ag4_src, ag4, ag4_s, ag4_r, 1)
    ag4_sent = far_waiter(ag4, ag4_s, ag4_r)
    ag4_sent.wait_recv()
    everyone = ag4[...].reshape(count * parts * seq, wide)
    picked = jnp.concatenate(
        [nn(part_picks[j], everyone).astype(bf16) for j in range(parts)], axis=1
    )
    lowered_part = nt(wdn_v[...], picked).astype(bf16)
    fin_src[...] = nn(lowered_part, place_rows).astype(bf16).reshape(fin_src.shape)
    for w, offset in sorted(enumerate(DOWN_WINDOW), key=lambda pair: -abs(pair[1])):
        row = lax.rem(z + offset + n_kv, n_kv)
        for k in sorted(range(n_tp), key=lambda k: -min(k, n_tp - k)):
            if offset == 0 and k == 0:
                fin[w * n_tp + t] = fin_src[w * n_tp + t]
                continue
            peer = lax.rem(t + k, n_tp)
            pltpu.make_async_remote_copy(
                src_ref=fin_src.at[w * n_tp + peer],
                dst_ref=fin.at[w * n_tp + t],
                send_sem=fin_s,
                recv_sem=fin_r,
                device_id=(g, row, peer),
                device_id_type=MESH,
            ).start()
    fin_sent = waiter(fin.at[0 : n_win * n_tp - 1], fin_s, fin_r)
    pending.append(fin_sent)
    fin_sent.wait_recv()
    lowered = jnp.sum(fin[...].astype(f32), axis=0)
    out_ref[...] = (middle + lowered).astype(bf16)
    for copy in pending:
        copy.wait_send()


def solution(mesh):
    n_kv, n_tp = mesh.shape["kv"], mesh.shape["tp"]

    def local(
        tokens,
        state,
        norm_gain,
        w_query,
        w_key,
        w_value,
        w_beta,
        w_decay,
        a_log,
        dt_bias,
        head_gain,
        w_out,
        mixer_gain,
        w_up,
        w_down,
    ):
        seq, heads, head = state.shape[:3]
        rows, mine = tokens.shape
        block = w_query.shape[0]
        parts = w_up.shape[1] // (2 * head)
        wide = w_up.shape[1] // parts
        count = n_kv // 4
        dims = (n_kv, n_tp, seq, heads, block * n_kv)
        vmem, hbm = (
            pl.BlockSpec(memory_space=pltpu.VMEM),
            pl.BlockSpec(memory_space=pltpu.HBM),
        )
        dma = pltpu.SemaphoreType.DMA
        blocks = (parts * seq, wide)
        n_win = len(UP_WINDOW)
        scratch = [
            pltpu.VMEM((n_tp + 1, mine, rows), bf16),
            pltpu.VMEM((n_win, n_tp + 1, mine, rows), bf16),
            pltpu.VMEM(state.shape, f32),
            pltpu.VMEM((2 * heads * block, 2 * head), bf16),
            pltpu.VMEM((2, w_beta.shape[1], head), bf16),
            pltpu.VMEM((block, n_win * heads * head), bf16),
            pltpu.VMEM((n_win * block, w_up.shape[1]), bf16),
            pltpu.VMEM((n_win * block, w_down.shape[0]), bf16),
            pltpu.VMEM((n_kv, *blocks), bf16),
            pltpu.VMEM((3 * count, *blocks), bf16),
            pltpu.VMEM((count, *blocks), bf16),
            pltpu.VMEM((count, *blocks), bf16),
            pltpu.VMEM((heads * seq, head), bf16),
            pltpu.VMEM((count, heads * seq, head), bf16),
            pltpu.VMEM((rows, n_win * heads * head), bf16),
            pltpu.VMEM((n_tp, block, rows), bf16),
            pltpu.VMEM((n_win, n_tp, mine, rows), bf16),
            pltpu.VMEM((n_win, mine, rows), bf16),
            pltpu.VMEM((count, *blocks), bf16),
            pltpu.VMEM((count, *blocks), bf16),
            pltpu.VMEM((1, rows), f32),
            pltpu.VMEM((count, 1, rows), f32),
            pltpu.VMEM(blocks, bf16),
            pltpu.VMEM((count, *blocks), bf16),
            pltpu.VMEM((n_win * n_tp, mine, rows), bf16),
            pltpu.VMEM((n_win * n_tp, mine, rows), bf16),
            pltpu.VMEM(norm_gain.shape, bf16),
            pltpu.VMEM(mixer_gain.shape, bf16),
            pltpu.VMEM((1, head), f32),
            pltpu.VMEM(a_log.shape, f32),
            pltpu.VMEM(dt_bias.shape, f32),
            dma((13,)),
            dma,
            dma,
            dma((2,)),
            dma((2,)),
            dma,
            dma,
            dma((4,)),
            dma((4,)),
            *[dma] * 14,
            pltpu.SemaphoreType.REGULAR,
            pltpu.SemaphoreType.REGULAR,
        ]
        mixed_t, new_state = pl.pallas_call(
            functools.partial(kernel, dims),
            out_shape=(
                jax.ShapeDtypeStruct((mine, rows), bf16),
                jax.ShapeDtypeStruct(state.shape, f32),
            ),
            in_specs=[hbm] * 15,
            out_specs=(vmem, vmem),
            scratch_shapes=scratch,
            compiler_params=pltpu.CompilerParams(collective_id=0, has_side_effects=True, vmem_limit_bytes=32 * 2**20),
        )(
            *[
                pltpu.with_memory_space_constraint(x, pltpu.HBM)
                for x in (
                    tokens.T,
                    state,
                    norm_gain,
                    w_query,
                    w_key,
                    w_value,
                    w_beta.T,
                    w_decay.T,
                    a_log,
                    dt_bias,
                    head_gain.reshape(1, head),
                    w_out.T,
                    mixer_gain,
                    w_up,
                    w_down.T,
                )
            ]
        )
        return mixed_t.T, new_state

    return jax.shard_map(
        local,
        mesh=mesh,
        in_specs=(
            P("grp", ("kv", "tp")),
            P(("grp", "kv"), "tp", None, None),
            P("kv"),
            P("kv", "tp"),
            P("kv", "tp"),
            P("kv", "tp"),
            P(),
            P(),
            P("tp"),
            P("tp"),
            P(),
            P("tp", "kv"),
            P("kv"),
            P("kv", "tp"),
            P("tp", "kv"),
        ),
        out_specs=(P("grp", ("kv", "tp")), P(("grp", "kv"), "tp", None, None)),
        check_vma=False,
    )
```

```python
import functools

import jax
import jax.numpy as jnp
from jax import lax
from jax.experimental import pallas as pl
from jax.experimental.pallas import tpu as pltpu
from jax.sharding import PartitionSpec as P

MESH = pl.DeviceIdType.MESH
epsilon = 1e-06
f32 = jnp.float32
bf16 = jnp.bfloat16


def nn(a, b):
    return jnp.dot(a, b, preferred_element_type=f32)


def nt(a, b):
    return lax.dot_general(a, b, (((1,), (1,)), ((), ())), preferred_element_type=f32)


def exact_nn(a, onehot):
    high = a.astype(bf16)
    low = (a - high.astype(f32)).astype(bf16)
    return nn(high, onehot) + nn(low, onehot)


def lanes_of(x, lane):
    at = lax.broadcasted_iota(jnp.int32, x.shape, 1)
    return jnp.sum(jnp.where(at == lane, x, 0.0), axis=1, keepdims=True)


def column_of(row):
    n = row.shape[1]
    eye = lax.broadcasted_iota(jnp.int32, (n, n), 0) == lax.broadcasted_iota(
        jnp.int32, (n, n), 1
    )
    return jnp.sum(jnp.where(eye, row, 0.0), axis=1, keepdims=True)


UP_WINDOW = (-1, 0, 1, 2)
DOWN_WINDOW = (-2, -1, 0, 1)


def reach_of(i, n_kv, where=jnp.where):
    q, top = n_kv // 16, n_kv // 2 - 2
    return where(i < q, top - 4 * i, where(i < 2 * q, -2 - 4 * i, top + 4 * q - 4 * i))


class Exchange:
    def __init__(self, n_kv, g, z, t):
        self.n_kv, self.g, self.z, self.t = n_kv, g, z, t
        self.count = n_kv // 4
        self.reach = [
            reach_of(i, n_kv, lambda c, x, y: x if c else y) for i in range(self.count)
        ]
        self.farthest_first = sorted(range(self.count), key=lambda i: -abs(self.reach[i]))
        self.own = 3 * self.count + n_kv // 8 - 1

    def device(self, offset):
        return (self.g, lax.rem(self.z + offset + self.n_kv, self.n_kv), self.t)

    def near_runs(self):
        q = self.n_kv // 16
        farther = [(3, 0, q, 2), (3, q, q - 1, -2), (0, 0, 2 * q, 1), (1, 0, 2 * q, -1)]
        closer = [
            (3, 2 * q, q, 2),
            (3, 3 * q, q, -2),
            (0, 2 * q, 2 * q, 1),
            (1, 2 * q, 2 * q, -1),
        ]
        return farther, closer

    def copy(self, src, dst, send, recv, offset):
        return pltpu.make_async_remote_copy(
            src_ref=src,
            dst_ref=dst,
            send_sem=send,
            recv_sem=recv,
            device_id=self.device(offset),
            device_id_type=MESH,
        )


def placing(per_slot, n_kv, seq, z):
    count = n_kv // 4
    shape = (n_kv * per_slot, n_kv * seq)
    m = lax.broadcasted_iota(jnp.int32, shape, 0)
    slot = m // per_slot
    i = slot % count
    group = slot // count
    reach = reach_of(i, n_kv)
    side = jnp.where(reach > 0, 2, -2)
    step = jnp.where(group == 0, 1, jnp.where(group == 1, -1, jnp.where(group == 2, 0, side)))
    offset = jnp.where(slot == 3 * count + n_kv // 8 - 1, 0, reach + step)
    owner = (z - offset + n_kv) % n_kv
    row = owner * seq + m % seq
    return (row == lax.broadcasted_iota(jnp.int32, shape, 1)).astype(bf16)


def kernel(
    dims,
    tok_ref,
    state_hbm,
    gain_ref,
    wq_hbm,
    wk_hbm,
    wv_hbm,
    wb_hbm,
    wd_hbm,
    alog_ref,
    dt_ref,
    hgain_ref,
    wo_hbm,
    mgain_ref,
    wu_hbm,
    wdn_hbm,
    out_ref,
    state_out,
    tok_all,
    tok_near,
    state_v,
    rhs1,
    wext,
    wo_v,
    wu_v,
    wdn_v,
    rs1,
    rs1_near,
    rs1_far_src,
    rs1_far,
    ag2_src,
    ag2,
    diag,
    att,
    mid_src,
    mid,
    rs3,
    rs3_far,
    sq_src,
    sq_far,
    ag4_src,
    ag4,
    fin_src,
    fin,
    gain_v,
    mgain_v,
    hgain_v,
    alog_v,
    dt_v,
    loc,
    tok_s,
    tok_r,
    rs1_ns,
    rs1_nr,
    rs1_fs,
    rs1_fr,
    win_s,
    win_r,
    ag2_s,
    ag2_r,
    att_s,
    att_r,
    rs3_s,
    rs3_r,
    sq_s,
    sq_r,
    mid_s,
    mid_r,
    ag4_s,
    ag4_r,
    fin_s,
    fin_r,
    sem_a,
    sem_b,
):
    n_kv, n_tp, seq, heads, width = dims
    g, z, t = lax.axis_index("grp"), lax.axis_index("kv"), lax.axis_index("tp")
    ex = Exchange(n_kv, g, z, t)
    count = ex.count
    mine = tok_ref.shape[0]
    block = n_tp * mine
    all_rows = tok_ref.shape[1]
    head = hgain_v.shape[1]
    own = ex.own

    def tp_peer(k):
        return (g, z, lax.rem(t + k, n_tp))

    barrier = pltpu.get_barrier_semaphore()
    for k in range(1, n_tp):
        pl.semaphore_signal(barrier, inc=1, device_id=tp_peer(k), device_id_type=MESH)
    for offset in (1, -1, 2, -2, 4, -4):
        pl.semaphore_signal(barrier, inc=1, device_id=ex.device(offset), device_id_type=MESH)

    def waiter(ref, send, recv):
        return pltpu.make_async_remote_copy(
            src_ref=ref,
            dst_ref=ref,
            send_sem=send,
            recv_sem=recv,
            device_id=tp_peer(1),
            device_id_type=MESH,
        )

    def fetch(src, dst, k):
        copy = pltpu.make_async_copy(src, dst, loc.at[k])
        copy.start()
        return copy

    got_tok = fetch(tok_ref, tok_all.at[t], 0)
    got_mgain = fetch(mgain_ref, mgain_v, 1)
    got_gain = fetch(gain_ref, gain_v, 2)
    lanes = wext.shape[2]
    at = pl.multiple_of((z * block // lanes) * lanes, lanes)
    got_ext = [
        fetch(wb_hbm.at[:, pl.ds(at, lanes)], wext.at[0], 3),
        fetch(wd_hbm.at[:, pl.ds(at, lanes)], wext.at[1], 4),
    ]
    for i, w in enumerate((wq_hbm, wk_hbm)):
        for h in range(heads):
            at = (i * heads + h) * block
            fetch(w.at[:, h * head : (h + 1) * head], rhs1.at[at : at + block, 0:head], 5)
    for h in range(heads):
        fetch(
            wv_hbm.at[:, h * head : (h + 1) * head],
            rhs1.at[h * block : (h + 1) * block, head : 2 * head],
            5,
        )
    whole = rhs1.at[0 : 3 * heads * block // 2]
    got_rhs1 = pltpu.make_async_copy(whole, whole, loc.at[5])
    got_small = [
        fetch(hgain_ref, hgain_v, 6),
        fetch(alog_ref, alog_v, 7),
        fetch(dt_ref, dt_v, 8),
    ]
    got_state = fetch(state_hbm, state_v, 9)
    parts = wu_v.shape[1] // (2 * head)
    wide = 2 * head
    kinds = heads * seq
    n_win = len(UP_WINDOW)
    out_wide = heads * head
    here_up, here_down = UP_WINDOW.index(0), DOWN_WINDOW.index(0)
    got_weights = [
        fetch(wo_hbm, wo_v.at[:, here_up * out_wide : (here_up + 1) * out_wide], 10),
        fetch(wu_hbm, wu_v.at[here_up * block : (here_up + 1) * block], 11),
        fetch(wdn_hbm, wdn_v.at[here_down * block : (here_down + 1) * block], 12),
    ]

    rhs1[heads * block :, head:] = jnp.zeros((heads * block, head), bf16)
    diag[...] = jnp.zeros(diag.shape, bf16)
    spread16 = placing(parts * seq, n_kv, seq, z)
    part_of_row = (
        lax.broadcasted_iota(jnp.int32, (n_kv * parts * seq, parts * block), 0) // seq
    ) % parts
    part_mask = part_of_row == (
        lax.broadcasted_iota(jnp.int32, (n_kv * parts * seq, parts * block), 1) // block
    )
    got_mgain.wait()
    gain_row = mgain_v[...].astype(f32).reshape(1, block)
    gain_row = jnp.concatenate([gain_row, jnp.zeros((1, all_rows - block), f32)], axis=1)
    tok_all[n_tp] = jnp.broadcast_to(gain_row, (mine, all_rows)).astype(bf16)
    got_gain.wait()
    gain = column_of(gain_v[...].astype(f32).reshape(1, block))
    got_tok.wait()

    pl.semaphore_wait(barrier, n_tp - 1 + 6)
    for offset in (4, -4):
        pl.semaphore_signal(sem_a, inc=1, device_id=ex.device(offset), device_id_type=MESH)

    def to_tp(dst, send, recv):
        for k in sorted(range(1, n_tp), key=lambda k: -min(k, n_tp - k)):
            peer = lax.rem(t + k, n_tp)
            pltpu.make_async_remote_copy(
                src_ref=dst.at[t],
                dst_ref=dst.at[t],
                send_sem=send,
                recv_sem=recv,
                device_id=(g, z, peer),
                device_id_type=MESH,
            ).start()
        return waiter(dst.at[0 : n_tp - 1], send, recv)

    pending = []
    tok_sent = to_tp(tok_all, tok_s, tok_r)
    pending.append(tok_sent)
    got_rhs1.wait()
    for copy in got_ext:
        copy.wait()
    odd = lax.rem(z, lanes // block) if lanes // block > 1 else 0
    pieces = []
    for i in range(2):
        piece = wext[i][:, 0:block]
        for k in range(1, lanes // block):
            piece = jnp.where(odd == k, wext[i][:, k * block : (k + 1) * block], piece)
        pieces.append(piece)
    n_heads = pieces[0].shape[0]
    wext_t = jnp.concatenate(
        pieces + [jnp.zeros((head - 2 * n_heads, block), bf16)], axis=0
    )
    at_row = lax.broadcasted_iota(jnp.int32, (head, block), 0)
    square_t = (at_row == 2 * n_heads).astype(bf16)
    ext_t = jnp.concatenate([wext_t, square_t], axis=1)

    tok_sent.wait_recv()
    pl.semaphore_wait(sem_a, 2)
    for offset in (8, -8):
        pl.semaphore_signal(sem_b, inc=1, device_id=ex.device(offset), device_id_type=MESH)

    def spread(x_t):
        stacked = jnp.concatenate([x_t] * parts, axis=0)
        rows = nt(spread16, stacked)
        return jnp.where(part_mask, rows, 0.0).astype(bf16)

    tok_t = tok_all[0:n_tp].astype(f32).reshape(block, all_rows)
    scaled_t = (tok_t * gain).astype(bf16)
    left = spread(scaled_t)
    both = jnp.concatenate([scaled_t, (tok_t * tok_t).astype(bf16)], axis=0)
    left2 = nt(spread16, both)
    left2 = jnp.where(part_of_row[:, 0 : 2 * block] >= heads, left2, 0.0).astype(bf16)
    product = nn(left, rhs1[...])
    extra = nt(left2, ext_t)
    product = jnp.concatenate([product[:, :head], product[:, head:] + extra], axis=1)
    rs1[...] = product.astype(bf16).reshape(rs1.shape)

    def to_far(chosen, src_of, dst, send, recv, sign):
        for i in chosen:
            ex.copy(src_of(i), dst.at[i], send, recv, sign * ex.reach[i]).start()

    def far_waiter(dst, send, recv):
        sent = waiter(dst, send, recv)
        pending.append(sent)
        return sent

    distant, close = ex.farthest_first[:count // 2], ex.farthest_first[count // 2 :]

    near_sent = []
    for part, runs in enumerate(ex.near_runs()):
        for group, first, blocks, step in runs:
            at, to = group * count + first, min(group, 2) * count + first
            ex.copy(
                rs1.at[at : at + blocks],
                rs1_near.at[to : to + blocks],
                rs1_ns.at[part],
                rs1_nr.at[part],
                -step,
            ).start()
        blocks = sum(run[2] for run in runs)
        near_sent.append(waiter(rs1.at[0:blocks], rs1_ns.at[part], rs1_nr.at[part]))
    pending += near_sent

    def near_sums(chosen):
        for i in chosen:
            total = rs1[2 * count + i].astype(f32)
            for k in range(3):
                if k < 2 or 3 * count + i != own:
                    total += rs1_near[k * count + i].astype(f32)
            rs1_far_src[i] = total.astype(bf16)

    near_sent[0].wait_recv()
    near_sums(distant)
    pl.semaphore_wait(sem_b, 2)
    to_far(distant, lambda i: rs1_far_src.at[i], rs1_far, rs1_fs, rs1_fr, -1)
    near_sent[1].wait_recv()
    near_sums(close)
    to_far(close, lambda i: rs1_far_src.at[i], rs1_far, rs1_fs, rs1_fr, -1)
    far_sent = far_waiter(rs1_far, rs1_fs, rs1_fr)

    def to_window(src, dst_of, whole, k, offsets):
        for w, offset in enumerate(offsets):
            if offset:
                ex.copy(src, dst_of(w), win_s.at[k], win_r.at[k], -offset).start()
        sent = waiter(whole, win_s.at[k], win_r.at[k])
        pending.append(sent)
        return sent

    tok_window = to_window(
        tok_all, lambda w: tok_near.at[w], tok_near.at[0 : n_win - 1], 0, UP_WINDOW
    )
    wo_window = to_window(
        wo_hbm,
        lambda w: wo_v.at[:, w * out_wide : (w + 1) * out_wide],
        wo_v.at[:, 0 : (n_win - 1) * out_wide],
        1,
        UP_WINDOW,
    )

    got_state.wait()
    for copy in got_small:
        copy.wait()
    far_sent.wait_recv()
    sums = rs1[own].astype(f32)
    for i in range(count):
        sums += rs1_far[i].astype(f32)

    rows = heads * seq
    query_sum, key_sum = sums[:rows, :head], sums[rows:, :head]
    value_sum, extra = sums[:rows, head:], sums[rows:, head:]
    which = lax.broadcasted_iota(jnp.int32, (rows, head), 0) // seq
    lane = lax.broadcasted_iota(jnp.int32, (rows, head), 1)
    beta_sum = jnp.sum(
        jnp.where(lane == t * heads + which, extra, 0.0), axis=1, keepdims=True
    )
    decay_sum = jnp.sum(
        jnp.where(lane == n_heads + t * heads + which, extra, 0.0), axis=1, keepdims=True
    )
    square_sum = lanes_of(extra, 2 * n_heads)
    first = lax.rsqrt(square_sum / width + epsilon)
    query_pre, key_pre, value_pre = first * query_sum, first * key_sum, first * value_sum
    query = query_pre * lax.rsqrt(jnp.sum(query_pre * query_pre, axis=1, keepdims=True) + epsilon)
    key = key_pre * lax.rsqrt(jnp.sum(key_pre * key_pre, axis=1, keepdims=True) + epsilon)
    beta = jax.nn.sigmoid(first * beta_sum)
    which1 = lax.broadcasted_iota(jnp.int32, (rows, 1), 0) // seq
    a_logs, dt_biases = alog_v[...].reshape(1, heads), dt_v[...].reshape(1, heads)
    a_log = jnp.zeros((rows, 1), f32)
    dt_bias = jnp.zeros((rows, 1), f32)
    for h in range(heads):
        a_log = jnp.where(which1 == h, a_logs[:, h : h + 1], a_log)
        dt_bias = jnp.where(which1 == h, dt_biases[:, h : h + 1], dt_bias)
    logit = first * decay_sum + dt_bias
    softplus = jnp.maximum(logit, 0.0) + jnp.log1p(jnp.exp(-jnp.abs(logit)))
    decay = jnp.exp(-jnp.exp(a_log) * softplus)
    query_t, key_t = query.T, key.T
    key_reads, query_reads = [], []
    for k in range(rows):
        matrix = state_v[k % seq, k // seq]
        key_reads.append(jnp.sum(matrix * key_t[:, k : k + 1], axis=0, keepdims=True))
        query_reads.append(jnp.sum(matrix * query_t[:, k : k + 1], axis=0, keepdims=True))
    key_read = jnp.concatenate(key_reads, axis=0)
    query_read = jnp.concatenate(query_reads, axis=0)
    fresh = beta * (value_pre - decay * key_read)
    meeting = jnp.sum(query * key, axis=1, keepdims=True)
    reading = decay * query_read + meeting * fresh
    normed = (
        reading
        * lax.rsqrt(jnp.mean(reading * reading, axis=1, keepdims=True) + epsilon)
        * hgain_v[...]
    )

    ag2_src[...] = normed.astype(bf16)
    to_far(distant, lambda i: ag2_src, ag2, ag2_s, ag2_r, 1)
    for k in range(rows):
        matrix = state_v[k % seq, k // seq]
        state_out[k % seq, k // seq] = (
            decay[k : k + 1] * matrix + key_t[:, k : k + 1] * fresh[k : k + 1]
        )
    to_far(close, lambda i: ag2_src, ag2, ag2_s, ag2_r, 1)
    ag2_sent = far_waiter(ag2, ag2_s, ag2_r)
    wu_window = to_window(
        wu_hbm,
        lambda w: wu_v.at[w * block : (w + 1) * block],
        wu_v.at[0 : (n_win - 1) * block],
        2,
        UP_WINDOW,
    )
    wdn_window = to_window(
        wdn_hbm,
        lambda w: wdn_v.at[w * block : (w + 1) * block],
        wdn_v.at[0 : (n_win - 1) * block],
        3,
        DOWN_WINDOW,
    )

    def iota(shape, dim):
        return lax.broadcasted_iota(jnp.int32, shape, dim)

    def owner_row(slot, r):
        return (z - reach_of(slot, n_kv) + n_kv) % n_kv * seq + r

    per_w = count * seq
    shape = (n_win * all_rows, all_rows)
    lane = iota(shape, 1)
    lane_owner = owner_row(lane % per_w // seq, lane % seq)
    window_pick = (
        (lane // per_w == iota(shape, 0) // all_rows) & (lane_owner == iota(shape, 0) % all_rows)
    ).astype(bf16)
    shape = (per_w, all_rows)
    place_rows = (owner_row(iota(shape, 0) // seq, iota(shape, 0) % seq) == iota(shape, 1)).astype(
        bf16
    )
    head_picks = []
    shape = (per_w, count * kinds)
    for h in range(heads):
        r0, c1 = iota(shape, 0), iota(shape, 1)
        head_picks.append(
            (
                (c1 // kinds == r0 // seq) & (c1 % seq == r0 % seq) & (c1 // seq % heads == h)
            ).astype(bf16)
        )
    shape = (count * parts * seq, all_rows)
    r0, c1 = iota(shape, 0), iota(shape, 1)
    spread_rows = (
        (r0 // (parts * seq) == c1 % per_w // seq) & (r0 % seq == c1 % seq)
    ).astype(bf16)
    shape = (per_w, count * parts * seq)
    r0, c1 = iota(shape, 0), iota(shape, 1)
    part_picks = [
        (
            (c1 // (parts * seq) == r0 // seq) & (c1 % seq == r0 % seq) & (c1 // seq % parts == j)
        ).astype(bf16)
        for j in range(parts)
    ]
    tok_window.wait_recv()
    token_parts = []
    mixer_gain = jnp.zeros((block, all_rows), f32)
    lane = iota((block, all_rows), 1)
    for w, offset in enumerate(UP_WINDOW):
        source = tok_near.at[w] if offset else tok_all
        token_parts.append(source[0:n_tp].astype(f32).reshape(block, all_rows).astype(bf16))
        column = column_of(source[n_tp].astype(f32)[0:1, 0:block])
        mixer_gain = jnp.where(lane // per_w == w, column, mixer_gain)
    token_w = nn(jnp.concatenate(token_parts, axis=1), window_pick)
    for copy in got_weights:
        copy.wait()
    ag2_sent.wait_recv()
    wo_window.wait_recv()
    everyone = ag2[...].astype(f32).reshape(count * kinds, head).astype(bf16)
    for h in range(heads):
        picked = nn(head_picks[h], everyone).astype(bf16)
        for w in range(n_win):
            at = w * out_wide + h * head
            diag[w * per_w : (w + 1) * per_w, at : at + head] = picked
    att[t] = nt(wo_v[...], diag[...]).astype(bf16)
    att_sent = to_tp(att, att_s, att_r)
    pending.append(att_sent)
    att_sent.wait_recv()
    wu_window.wait_recv()

    attended = att[0].astype(f32)
    for k in range(1, n_tp):
        attended += att[k].astype(f32)
    middle_b = (token_w + attended).astype(bf16)
    middle = middle_b.astype(f32)
    sq_src[...] = jnp.sum(middle * middle, axis=0, keepdims=True)
    to_far(ex.farthest_first, lambda i: sq_src, sq_far, sq_s, sq_r, -1)
    sq_sent = far_waiter(sq_far, sq_s, sq_r)
    scaled = jnp.concatenate([middle * mixer_gain] * n_win, axis=0)
    shape = scaled.shape
    scaled = jnp.where(iota(shape, 1) // per_w == iota(shape, 0) // block, scaled, 0.0)
    left = nt(spread_rows, scaled.astype(bf16))
    part = iota(left.shape, 0) // seq % parts
    product = jnp.zeros((left.shape[0], wide), f32)
    for j in range(parts):
        product += nn(
            jnp.where(part == j, left, 0.0).astype(bf16), wu_v[:, j * wide : (j + 1) * wide]
        )
    rs3[...] = product.astype(bf16).reshape(rs3.shape)
    to_far(distant, lambda i: rs3.at[i], rs3_far, rs3_s, rs3_r, -1)
    for w, offset in enumerate(UP_WINDOW):
        placed = nt(middle_b, window_pick[w * all_rows : (w + 1) * all_rows]).astype(bf16)
        mid_src[w] = placed.reshape(n_tp, mine, all_rows)
        if not offset:
            mid[w] = mid_src[w, t]
    to_far(close, lambda i: rs3.at[i], rs3_far, rs3_s, rs3_r, -1)
    rs3_sent = far_waiter(rs3_far, rs3_s, rs3_r)
    for w, offset in enumerate(UP_WINDOW):
        if offset:
            ex.copy(mid_src.at[w, t], mid.at[w], mid_s, mid_r, offset).start()
    mid_sent = waiter(mid.at[0 : n_win - 1], mid_s, mid_r)
    pending.append(mid_sent)
    sq_sent.wait_recv()
    lane = iota((1, all_rows), 1)
    squares = jnp.zeros((1, all_rows), f32)
    for i in range(count):
        squares += jnp.where(lane % per_w // seq == i, sq_far[i], 0.0)
    shape = (parts * seq, all_rows)
    squares = jnp.sum(
        jnp.where(iota(shape, 1) % seq == iota(shape, 0) % seq, squares, 0.0),
        axis=1,
        keepdims=True,
    )
    second = lax.rsqrt(squares / width + epsilon)
    up = jnp.zeros((parts * seq, wide), f32)
    rs3_sent.wait_recv()
    for i in range(count):
        up += rs3_far[i].astype(f32)
    ag4_src[...] = jnp.square(jnp.maximum(second * up, 0.0)).astype(bf16)

    to_far(distant, lambda i: ag4_src, ag4, ag4_s, ag4_r, 1)
    wdn_window.wait_recv()
    mid_sent.wait_recv()
    middle = mid[0].astype(f32)
    for w in range(1, n_win):
        middle += mid[w].astype(f32)
    to_far(close, lambda i: ag4_src, ag4, ag4_s, ag4_r, 1)
    ag4_sent = far_waiter(ag4, ag4_s, ag4_r)
    ag4_sent.wait_recv()
    everyone = ag4[...].reshape(count * parts * seq, wide)
    picked = jnp.concatenate(
        [nn(part_picks[j], everyone).astype(bf16) for j in range(parts)], axis=1
    )
    lowered_part = nt(wdn_v[...], picked).astype(bf16)
    fin_src[...] = nn(lowered_part, place_rows).astype(bf16).reshape(fin_src.shape)
    for w, offset in sorted(enumerate(DOWN_WINDOW), key=lambda pair: -abs(pair[1])):
        row = lax.rem(z + offset + n_kv, n_kv)
        for k in sorted(range(n_tp), key=lambda k: -min(k, n_tp - k)):
            if offset == 0 and k == 0:
                fin[w * n_tp + t] = fin_src[w * n_tp + t]
                continue
            peer = lax.rem(t + k, n_tp)
            pltpu.make_async_remote_copy(
                src_ref=fin_src.at[w * n_tp + peer],
                dst_ref=fin.at[w * n_tp + t],
                send_sem=fin_s,
                recv_sem=fin_r,
                device_id=(g, row, peer),
                device_id_type=MESH,
            ).start()
    fin_sent = waiter(fin.at[0 : n_win * n_tp - 1], fin_s, fin_r)
    pending.append(fin_sent)
    fin_sent.wait_recv()
    lowered = jnp.sum(fin[...].astype(f32), axis=0)
    out_ref[...] = (middle + lowered).astype(bf16)
    for copy in pending:
        copy.wait_send()


def write_out(mixed_ref, state_ref, mixed_out, state_out, sems):
    copies = [
        pltpu.make_async_copy(state_ref, state_out, sems.at[0]),
        pltpu.make_async_copy(mixed_ref, mixed_out, sems.at[1]),
    ]
    for copy in copies:
        copy.start()
    for copy in copies:
        copy.wait()


def solution(mesh):
    n_kv, n_tp = mesh.shape["kv"], mesh.shape["tp"]

    def local(
        tokens,
        state,
        norm_gain,
        w_query,
        w_key,
        w_value,
        w_beta,
        w_decay,
        a_log,
        dt_bias,
        head_gain,
        w_out,
        mixer_gain,
        w_up,
        w_down,
    ):
        seq, heads, head = state.shape[:3]
        rows, mine = tokens.shape
        block = w_query.shape[0]
        parts = w_up.shape[1] // (2 * head)
        wide = w_up.shape[1] // parts
        count = n_kv // 4
        dims = (n_kv, n_tp, seq, heads, block * n_kv)
        vmem, hbm = (
            pl.BlockSpec(memory_space=pltpu.VMEM),
            pl.BlockSpec(memory_space=pltpu.HBM),
        )
        dma = pltpu.SemaphoreType.DMA
        blocks = (parts * seq, wide)
        n_win = len(UP_WINDOW)
        scratch = [
            pltpu.VMEM((n_tp + 1, mine, rows), bf16),
            pltpu.VMEM((n_win, n_tp + 1, mine, rows), bf16),
            pltpu.VMEM(state.shape, f32),
            pltpu.VMEM((2 * heads * block, 2 * head), bf16),
            pltpu.VMEM((2, w_beta.shape[1], head), bf16),
            pltpu.VMEM((block, n_win * heads * head), bf16),
            pltpu.VMEM((n_win * block, w_up.shape[1]), bf16),
            pltpu.VMEM((n_win * block, w_down.shape[0]), bf16),
            pltpu.VMEM((n_kv, *blocks), bf16),
            pltpu.VMEM((3 * count, *blocks), bf16),
            pltpu.VMEM((count, *blocks), bf16),
            pltpu.VMEM((count, *blocks), bf16),
            pltpu.VMEM((heads * seq, head), bf16),
            pltpu.VMEM((count, heads * seq, head), bf16),
            pltpu.VMEM((rows, n_win * heads * head), bf16),
            pltpu.VMEM((n_tp, block, rows), bf16),
            pltpu.VMEM((n_win, n_tp, mine, rows), bf16),
            pltpu.VMEM((n_win, mine, rows), bf16),
            pltpu.VMEM((count, *blocks), bf16),
            pltpu.VMEM((count, *blocks), bf16),
            pltpu.VMEM((1, rows), f32),
            pltpu.VMEM((count, 1, rows), f32),
            pltpu.VMEM(blocks, bf16),
            pltpu.VMEM((count, *blocks), bf16),
            pltpu.VMEM((n_win * n_tp, mine, rows), bf16),
            pltpu.VMEM((n_win * n_tp, mine, rows), bf16),
            pltpu.VMEM(norm_gain.shape, bf16),
            pltpu.VMEM(mixer_gain.shape, bf16),
            pltpu.VMEM((1, head), f32),
            pltpu.VMEM(a_log.shape, f32),
            pltpu.VMEM(dt_bias.shape, f32),
            dma((13,)),
            dma,
            dma,
            dma((2,)),
            dma((2,)),
            dma,
            dma,
            dma((4,)),
            dma((4,)),
            *[dma] * 14,
            pltpu.SemaphoreType.REGULAR,
            pltpu.SemaphoreType.REGULAR,
        ]
        mixed_t, new_state = pl.pallas_call(
            functools.partial(kernel, dims),
            out_shape=(
                jax.ShapeDtypeStruct((mine, rows), bf16),
                jax.ShapeDtypeStruct(state.shape, f32),
            ),
            in_specs=[hbm] * 15,
            out_specs=(vmem, vmem),
            scratch_shapes=scratch,
            compiler_params=pltpu.CompilerParams(collective_id=0, has_side_effects=True, vmem_limit_bytes=32 * 2**20),
        )(
            *[
                pltpu.with_memory_space_constraint(x, pltpu.HBM)
                for x in (
                    tokens.T,
                    state,
                    norm_gain,
                    w_query,
                    w_key,
                    w_value,
                    w_beta.T,
                    w_decay.T,
                    a_log,
                    dt_bias,
                    head_gain.reshape(1, head),
                    w_out.T,
                    mixer_gain,
                    w_up,
                    w_down.T,
                )
            ]
        )
        mixed_t, new_state = pl.pallas_call(
            write_out,
            out_shape=(
                jax.ShapeDtypeStruct((mine, rows), bf16),
                jax.ShapeDtypeStruct(state.shape, f32),
            ),
            in_specs=[vmem, vmem],
            out_specs=(hbm, hbm),
            scratch_shapes=[dma((2,))],
            compiler_params=pltpu.CompilerParams(vmem_limit_bytes=2**20),
        )(mixed_t, new_state)
        return mixed_t.T, new_state

    return jax.shard_map(
        local,
        mesh=mesh,
        in_specs=(
            P("grp", ("kv", "tp")),
            P(("grp", "kv"), "tp", None, None),
            P("kv"),
            P("kv", "tp"),
            P("kv", "tp"),
            P("kv", "tp"),
            P(),
            P(),
            P("tp"),
            P("tp"),
            P(),
            P("tp", "kv"),
            P("kv"),
            P("kv", "tp"),
            P("tp", "kv"),
        ),
        out_specs=(P("grp", ("kv", "tp")), P(("grp", "kv"), "tp", None, None)),
        check_vma=False,
    )
```
